256 devices in a mesh: grp: 2 (over y), sp: 32 (over z, core), tp: 4 (over x).
Axes of the slice: x: 4, y: 2, z: 16, core: 2. Of those that a mesh axis runs over, the one named last changes fastest.
The devices are a block of a 4x16x16 slice.
Arguments:
- conv_value: bfloat16 [32768, 1024], P(('grp', 'sp'), 'tp'), parts along dimension 0, may hold values from -6 to 6
- conv_gate: bfloat16 [32768, 1024], P(('grp', 'sp'), 'tp'), parts along dimension 0, may hold values from -6 to 6
- kernel: bfloat16 [31, 1024], P(None, 'tp'), may hold values from -4 to 4
- conv_bias: float32 [1024], P('tp'), may hold values from -3 to 3
- ln_gain: float32 [1024], P('tp'), may hold values from 0.1 to 1.9
- ln_bias: float32 [1024], P('tp'), may hold values from -3 to 3
- out_gain: float32 [1024], P('tp'), may hold values from 0.1 to 1.9
- out_weight: bfloat16 [1024, 2048], replicated, may hold values from -0.1875 to 0.1875
- residual: bfloat16 [32768, 2048], P(('grp', 'sp', 'tp')), parts along dimension 0, may hold values from -6 to 6
- moe_gain: float32 [2048], replicated, may hold values from 0.1 to 1.9
- expert_ids: int32 [32768, 2], P(('grp', 'sp', 'tp')), parts along dimension 0, may hold values from 0 to 127, as said below
- expert_weights: float32 [32768, 2], P(('grp', 'sp', 'tp')), parts along dimension 0, may hold values from 0.1 to 0.7
- w_gate: bfloat16 [128, 2048, 512], P(('sp', 'tp')), may hold values from -0.125 to 0.125
- w_up: bfloat16 [128, 2048, 512], P(('sp', 'tp')), may hold values from -0.125 to 0.125
- w_down: bfloat16 [128, 512, 2048], P(('sp', 'tp')), may hold values from -0.25 to 0.25
Outputs:
- layer_out: bfloat16 [32768, 2048], P(('grp', 'sp', 'tp')), parts along dimension 0
The draws below stay inside these ranges and needn't reach their ends.
There are 2 independent parts, one for each index of `grp`. The reference program is written for one: setup_inputs(seed, part) draws one part's arguments, and reference() takes and returns one part's arrays. A program takes and returns all parts, laid end to end along the dimension named above; an argument that names none is the same for every part. Nothing has to cross between parts.
Inputs may be any that keep to these rules, and one draw needn't show every extreme that they name: `expert_ids`: each row names two different experts of one group (group = expert number // 32). Among the 128 rows of one device (aligned blocks of 128 rows) no expert is named more than 4 times, and in every such block some expert is named exactly 4 times.
All inputs are finite; a program needn't handle non-finite values.
Results may differ from the reference program's by a relative error of at most 0.0095.
Values may be sent and summed in bfloat16 or wider, within the bound.
A program may use at most 64 MiB of HBM per device.

```python
import jax
import jax.numpy as jnp
from jax import lax

D = 2048
CONV_CH = 1024
KERNEL = 31
HID = 512
ROWS = 128
TOKENS = 16384
EXPERTS = 128
EPG = 32
CAP = 4


def draw_kernel(key, part):
    key_base, key_jitter = jax.random.split(jax.random.fold_in(key, 11))
    ramp = jnp.exp(jnp.log(0.3) + jnp.log(10.0) * jnp.arange(CONV_CH, dtype=jnp.float32) / CONV_CH)
    jitter = jnp.exp(jax.random.uniform(key_jitter, (CONV_CH,), jnp.float32, -0.35, 0.35))
    base = jnp.clip(jax.random.normal(key_base, (KERNEL, CONV_CH), jnp.float32), -4.0, 4.0)
    return (base * ramp * jitter / jnp.sqrt(jnp.float32(KERNEL))).astype(jnp.bfloat16)


def draw_expert_ids(key, part):
    group_size = min(ROWS, EXPERTS // 2)
    rounds = TOKENS // group_size
    busiest = jax.random.randint(jax.random.fold_in(key, 21), (), 0, EXPERTS)
    round_keys = jax.random.split(jax.random.fold_in(key, 22), rounds)
    numbers = jnp.arange(EXPERTS, dtype=jnp.int32)

    def one_round(round_key):
        key_shift, key_order, key_mix, key_swap = jax.random.split(round_key, 4)
        shift_by = jax.random.randint(key_shift, (), 1, EPG)
        pre_image = busiest // EPG * EPG + (busiest % EPG - shift_by) % EPG
        scores = jax.random.permutation(key_order, EXPERTS).astype(jnp.int32)
        forced = (numbers == busiest) | (numbers == pre_image)
        scores = jnp.where(forced, scores + EXPERTS, scores)
        _, chosen = lax.top_k(scores, group_size)
        chosen = jax.random.permutation(key_mix, chosen.astype(jnp.int32))
        second = chosen // EPG * EPG + (chosen % EPG + shift_by) % EPG
        swapped = jax.random.randint(key_swap, (group_size,), 0, 2)
        first_col = jnp.where(swapped == 1, second, chosen)
        second_col = jnp.where(swapped == 1, chosen, second)
        return jnp.stack([first_col, second_col], axis=1).astype(jnp.int32)
    return jax.vmap(one_round)(round_keys).reshape(TOKENS, 2).astype(jnp.int32)


def block_levels(own_key, extent, shards, low, largest):
    def one(dim, shards_of):
        steps = jax.random.uniform(jax.random.fold_in(jax.random.fold_in(own_key, 6), dim), (shards_of,), jnp.float32, low / len(shards), largest / len(shards))
        return jnp.repeat(jnp.exp(steps), extent[dim] // shards_of).reshape((-1,) + (1,) * (len(extent) - dim - 1))

    level = one(*shards[0])
    for cut in shards[1:]:
        level = level * one(*cut)
    return level


def noise(stream_key, extent, scale, bound, shards=(), kind=jnp.bfloat16):
    array = scale * jax.random.normal(stream_key, extent, jnp.float32)
    if shards:
        array = array * block_levels(stream_key, extent, shards, -0.22, 0.18)
    return jnp.clip(array, -bound, bound).astype(kind)


def setup_inputs(seed: int = 0, part: int = 0) -> dict:
    keys = jax.random.split(jax.random.key(seed), 16)
    own_keys = jax.random.split(jax.random.fold_in(keys[15], part), 16)
    conv_value = noise(own_keys[0], (TOKENS, CONV_CH), 1.0, 6.0, ((0, 32), (1, 4)))
    conv_gate = noise(own_keys[1], (TOKENS, CONV_CH), 1.0, 6.0, ((0, 32), (1, 4)))
    kernel = draw_kernel(jax.random.fold_in(keys[15], 71), part)
    conv_bias = noise(keys[3], (CONV_CH,), 0.5, 3.0, ((0, 4),), jnp.float32)
    ln_gain = jnp.clip(1.0 + 0.18 * jax.random.normal(keys[4], (CONV_CH,), jnp.float32), 0.1, 1.9)
    ln_bias = noise(keys[5], (CONV_CH,), 0.5, 3.0, ((0, 4),), jnp.float32)
    out_gain = jnp.clip(1.0 + 0.18 * jax.random.normal(keys[6], (CONV_CH,), jnp.float32), 0.1, 1.9)
    out_weight = noise(keys[7], (CONV_CH, D), CONV_CH ** -0.5, 0.1875)
    residual = noise(own_keys[8], (TOKENS, D), 1.0, 6.0, ((0, 128),))
    moe_gain = jnp.clip(1.0 + 0.18 * jax.random.normal(keys[9], (D,), jnp.float32), 0.1, 1.9)
    expert_ids = draw_expert_ids(jax.random.fold_in(jax.random.fold_in(keys[15], part), 71), part)
    expert_weights = jnp.clip(0.1 + 0.59999999 * jax.random.uniform(own_keys[11], (TOKENS, 2), jnp.float32) ** block_levels(own_keys[11], (TOKENS, 2), ((0, 128),), -0.2, 0.2), 0.1, 0.7)
    w_gate = noise(keys[12], (EXPERTS, D, HID), D ** -0.5, 0.125, ((0, 128),))
    w_up = noise(keys[13], (EXPERTS, D, HID), D ** -0.5, 0.125, ((0, 128),))
    w_down = noise(keys[14], (EXPERTS, HID, D), HID ** -0.5, 0.25, ((0, 128),))
    return dict(conv_value=conv_value, conv_gate=conv_gate, kernel=kernel, conv_bias=conv_bias, ln_gain=ln_gain, ln_bias=ln_bias, out_gain=out_gain, out_weight=out_weight, residual=residual, moe_gain=moe_gain, expert_ids=expert_ids, expert_weights=expert_weights, w_gate=w_gate, w_up=w_up, w_down=w_down)


EPSILON = 1e-06

def reference(conv_value, conv_gate, kernel, conv_bias, ln_gain, ln_bias, out_gain, out_weight, residual, moe_gain, expert_ids, expert_weights, w_gate, w_up, w_down):
    gated = (conv_value.astype(jnp.float32) * jax.nn.sigmoid(conv_gate.astype(jnp.float32))).astype(jnp.bfloat16)
    padded = jnp.concatenate([jnp.zeros((KERNEL - 1, CONV_CH), gated.dtype), gated], axis=0)
    convolved = jnp.zeros((TOKENS, CONV_CH), jnp.float32) + conv_bias
    for offset in range(KERNEL):
        convolved = convolved + padded[offset:offset + TOKENS].astype(jnp.float32) * kernel[offset].astype(jnp.float32)
    average = lax.optimization_barrier(jnp.mean(convolved, axis=1, keepdims=True))
    spread = lax.optimization_barrier(jnp.mean(convolved * convolved, axis=1, keepdims=True)) - average * average
    swished = jax.nn.silu((convolved - average) * lax.rsqrt(spread + EPSILON) * ln_gain + ln_bias)
    energy = lax.optimization_barrier(jnp.mean(swished * swished, axis=1, keepdims=True))
    branch = (swished * lax.rsqrt(energy + EPSILON) * out_gain).astype(jnp.bfloat16)
    projected = jnp.dot(branch, out_weight, preferred_element_type=jnp.float32)
    hidden = (residual.astype(jnp.float32) + projected).astype(jnp.bfloat16)
    widened = hidden.astype(jnp.float32)
    normed = (widened * lax.rsqrt(lax.optimization_barrier(jnp.mean(widened * widened, axis=1, keepdims=True)) + EPSILON) * moe_gain).astype(jnp.bfloat16)
    flat_ids = expert_ids.reshape(-1).astype(jnp.int32)
    onehot = (flat_ids[:, None] == jnp.arange(EXPERTS, dtype=jnp.int32)[None, :]).astype(jnp.int32)
    slot_rank = lax.optimization_barrier(jnp.sum((jnp.cumsum(onehot, axis=0) - 1) * onehot, axis=1)).astype(jnp.int32)
    capacity = TOKENS // ROWS * CAP
    position = flat_ids * capacity + slot_rank
    token_index = (jnp.arange(2 * TOKENS, dtype=jnp.int32) // 2).astype(jnp.int32)
    table = jnp.full((EXPERTS * capacity,), TOKENS, jnp.int32).at[position].set(token_index).reshape(EXPERTS, capacity)
    weight_table = jnp.zeros((EXPERTS * capacity,), jnp.float32).at[position].set(expert_weights.reshape(-1).astype(jnp.float32)).reshape(EXPERTS, capacity)
    source_rows = jnp.concatenate([normed, jnp.zeros((1, D), normed.dtype)], axis=0)

    def one_expert(total, pieces):
        rows_index, row_weights, gate_w, up_w, down_w = pieces
        taken = source_rows[rows_index]
        gate_part = jnp.dot(taken, gate_w, preferred_element_type=jnp.float32)
        up_part = jnp.dot(taken, up_w, preferred_element_type=jnp.float32)
        active = (jax.nn.silu(gate_part) * up_part).astype(jnp.bfloat16)
        result = jnp.dot(active, down_w, preferred_element_type=jnp.float32).astype(jnp.bfloat16)
        return (total.at[rows_index].add(row_weights[:, None] * result.astype(jnp.float32)), None)
    start_total = jnp.zeros((TOKENS + 1, D), jnp.float32)
    combined, _ = lax.scan(one_expert, start_total, (table, weight_table, w_gate, w_up, w_down))
    return (widened + combined[:TOKENS]).astype(jnp.bfloat16)
```

```python
import functools

import jax
import jax.numpy as jnp
from jax import lax
from jax.experimental import pallas as pl
from jax.experimental.pallas import tpu as pltpu
from jax.sharding import PartitionSpec as P

EPSILON = 1e-06
MESH = pl.DeviceIdType.MESH
F32 = jnp.float32
BF16 = jnp.bfloat16

SPAN = 4
PLANES = 16
GROUPS = 4
HOPS = 9
SEATS = 8
DEPTH = 4
UNIT = 32
BLOCKS = 3 + 2 * (HOPS - 1)


def first_block(hop):
    return 0 if hop == 1 else 3 + 2 * (hop - 2)


def kinds_at(hop):
    found = []
    for rel in (2, 1, 0):
        if rel == 2 and hop > 1:
            continue
        if any(static_valid(on, hop, rel) for on in range(SPAN)):
            found.append(rel)
    return found


def static_valid(on, hop, rel):
    start = (on - hop) % SPAN
    kind = (start + hop) // SPAN + rel
    return kind <= 1 or (kind == 2 and start >= 2)


def valid(on, hop, rel):
    start = lax.rem(on + 12 - hop, SPAN)
    kind = lax.div(start + hop, SPAN) + rel
    return (kind <= 1) | ((kind == 2) & (start >= 2))


def iota(shape, dim):
    return lax.broadcasted_iota(jnp.int32, shape, dim)


def ranks(col, row):
    size = col.shape[0]
    out = {}
    e1c, e2c = col[:, 0:1], col[:, 1:2]
    e1r, e2r = row[0:1, :], row[1:2, :]
    gc, gr = e1c >> 5, e1r >> 5
    o1c, o2c = (e1c >> 3) & 3, (e2c >> 3) & 3
    o1r, o2r = (e1r >> 3) & 3, (e2r >> 3) & 3
    mxc, mnc = jnp.maximum(o1c, o2c), jnp.minimum(o1c, o2c)
    mxr, mnr = jnp.maximum(o1r, o2r), jnp.minimum(o1r, o2r)
    sub = iota((size, size), 0)
    lane = iota((size, size), 1)
    same = gc == gr
    for name, kc, kr in (("P", 3 - mxc, 3 - mxr), ("M", mnc, mnr)):
        kc = kc * size + iota((size, 1), 0)
        kr = kr * size + iota((1, size), 1)
        out[name + "r"] = jnp.sum((same & (kc < kr)).astype(F32), axis=0, keepdims=True).astype(jnp.int32)
        out[name + "c"] = jnp.sum((same & (kr < kc)).astype(F32), axis=1, keepdims=True).astype(jnp.int32)
    out.update(gc=gc, gr=gr, mxc=mxc, mnc=mnc, sub=sub, lane=lane)
    return out


def route_body(col_ref, row_ref, wcol_ref, meta_ref):
    col, row = col_ref[...], row_ref[...]
    size = col.shape[0]
    zed = lax.div(lax.axis_index("sp"), 2)
    zo, g0 = lax.rem(zed, SPAN), lax.div(zed, SPAN)
    r = ranks(col, row)
    e1c, e2c = col[:, 0:1], col[:, 1:2]
    e1r, e2r = row[0:1, :], row[1:2, :]
    earlier = r["lane"] < r["sub"]
    place = []
    for e in (e1c, e2c):
        hit = ((e == e1r) | (e == e2r)) & earlier
        place.append(jnp.sum(hit.astype(F32), axis=1, keepdims=True).astype(jnp.int32))
    group = r["gc"]
    ahead = group - g0
    ahead = jnp.where(ahead < 0, ahead + GROUPS, ahead)
    far_up = jnp.where(zo >= 2, 1, 0)
    lanes = iota((size, 128), 1)
    for plane in range(PLANES):
        slot_row = jnp.full((1, 128), -1.0, F32)
        weight_row = jnp.zeros((1, 128), F32)
        for k, e in enumerate((e1c, e2c)):
            po = plane % SPAN
            own_up = jnp.where(po >= zo, 1, 0)
            up = jnp.where(ahead == 0, own_up, jnp.where(ahead == 1, 1, jnp.where(ahead == 2, far_up, 0)))
            slot = jnp.where(up == 1, r["Pc"], r["Mc"]).astype(F32)
            lane = jnp.where((e >> 3) == plane, (e & 7) * 16 + place[k], -1)
            hit = lane == lanes
            slot_row = slot_row + jnp.sum(jnp.where(hit, slot + 1.0, 0.0), axis=0, keepdims=True)
            weight_row = weight_row + jnp.sum(jnp.where(hit, wcol_ref[:, k : k + 1], 0.0), axis=0, keepdims=True)
        meta_ref[plane] = jnp.concatenate([slot_row, weight_row, jnp.zeros((6, 128), F32)], axis=0)


def moe_body(
    hidden_ref, normed_ref, col_ref, row_ref, meta_ref, wg_hbm, wu_hbm, wd_hbm, out_ref,
    wg, wu, wd, own, came, back, part, xs, xr, rb, yr,
    wsem, fsend, frecv, bsend, brecv, xsend, xrecv, ysend, yrecv,
):
    sp, tp = lax.axis_index("sp"), lax.axis_index("tp")
    zed, core = lax.div(sp, 2), lax.rem(sp, 2)
    zo, g0 = lax.rem(zed, SPAN), lax.div(zed, SPAN)
    seat = core * 4 + tp
    off = (zo, SPAN - 1 - zo)
    last = tuple(jnp.where(o == SPAN - 1, 1, 0) for o in off)
    following = tuple(lax.rem(o + 1, SPAN) for o in off)
    ring_to = ({"sp": lax.rem(zed + 1, PLANES) * 2 + core}, {"sp": lax.rem(zed + PLANES - 1, PLANES) * 2 + core})
    ring_from = (ring_to[1], ring_to[0])

    def seat_device(s):
        return {"sp": zed * 2 + lax.div(s, 4), "tp": lax.rem(s, 4)}

    weights = [
        pltpu.make_async_copy(wg_hbm.at[0], wg, wsem.at[0]),
        pltpu.make_async_copy(wu_hbm.at[0], wu, wsem.at[1]),
        pltpu.make_async_copy(wd_hbm.at[0], wd, wsem.at[2]),
    ]
    for w in weights:
        w.start()

    for d in (0, 1):
        for i in range(3):
            back[d, i] = jnp.zeros(back.shape[2:], BF16)

        @pl.when(off[d] == SPAN - 1)
        def _():
            for hop in range(1, HOPS + 1):
                came[d, first_block(hop), 1] = jnp.zeros(came.shape[3:], BF16)

    barrier = pltpu.get_barrier_semaphore()
    for to in ring_to:
        pl.semaphore_signal(barrier, inc=1, device_id=to, device_id_type=MESH)
    for k in range(1, SEATS):
        pl.semaphore_signal(barrier, inc=1, device_id=seat_device(lax.rem(seat + k, SEATS)), device_id_type=MESH)
    pl.semaphore_wait(barrier, SEATS + 1)

    r = ranks(col_ref[...], row_ref[...])
    normed = normed_ref[...]
    tokens = normed.shape[0]
    for d, name in ((0, "P"), (1, "M")):
        slot = r["gr"] * 64 + r[name + "r"]
        onehot = jnp.where(iota((GROUPS * 64, tokens), 0) == slot, 1.0, 0.0).astype(BF16)
        rows = jnp.dot(onehot, normed, preferred_element_type=F32).astype(BF16)
        own[d] = rows.reshape(own.shape[1:])

    def forward(d, src, hop, index, unit):
        return pltpu.make_async_remote_copy(
            src_ref=src, dst_ref=came.at[d, index, unit],
            send_sem=fsend.at[d, index, unit], recv_sem=frecv.at[d, index, unit],
            device_id=ring_to[d], device_id_type=MESH,
        )

    def backward(d, src, index, unit):
        return pltpu.make_async_remote_copy(
            src_ref=src, dst_ref=back.at[d, index, unit],
            send_sem=bsend.at[d, index, unit], recv_sem=brecv.at[d, index, unit],
            device_id=ring_from[d], device_id_type=MESH,
        )

    def first_hop(act):
        for rel in kinds_at(1):
            for unit in (0, 1):
                for d in (0, 1):
                    kind = rel + last[d]
                    group = lax.rem(g0 + kind, GROUPS) if d == 0 else lax.rem(g0 + GROUPS - kind, GROUPS)
                    fine = valid(following[d], 1, rel)
                    if unit == 1 and rel == 0:
                        fine = fine & (following[d] < SPAN - 1)

                    @pl.when(fine)
                    def _():
                        act(forward(d, own.at[d, group, unit], 1, rel, unit), d, rel, unit)

    first_hop(lambda copy, *_: copy.start())

    def arrivals(hop, act):
        for rel in kinds_at(hop):
            for unit in (0, 1):
                for d in (0, 1):
                    fine = valid(off[d], hop, rel)
                    if unit == 1 and rel == 0:
                        fine = fine & (off[d] < SPAN - 1)

                    @pl.when(fine)
                    def _():
                        act(d, rel, unit)

    def goes_on(d, hop, rel, unit):
        there = rel - last[d]
        ok = there >= 0
        if unit == 1:
            ok = ok & ((there > 0) | (following[d] < SPAN - 1))
        return ok, first_block(hop + 1) + jnp.maximum(there, 0)

    def relay(hop):
        def act(d, rel, unit):
            index = first_block(hop) + rel
            forward(d, came.at[d, index, unit], hop, index, unit).wait_recv()
            if hop < HOPS:
                ok, there = goes_on(d, hop, rel, unit)

                @pl.when(ok)
                def _():
                    forward(d, came.at[d, index, unit], hop + 1, there, unit).start()

        arrivals(hop, act)

    def up_if(flag, a, b):
        return (jnp.where(flag, a[0], b[0]), jnp.where(flag, first_block(a[1]), first_block(b[1])),
                jnp.where(flag, zed - a[1], zed + b[1]))

    def fixed(d, hop):
        return (d, first_block(hop), zed - hop if d == 0 else zed + hop)

    batches = [[fixed(0, h), fixed(1, h), fixed(0, h + 1), fixed(1, h + 1)] for h in (1, 3, 5)]
    batches.append([
        None,
        up_if(zo != 0, (0, 7), (1, 9)),
        up_if(zo >= 2, (0, 8), (1, 8)),
        up_if(zo == 3, (0, 9), (1, 7)),
    ])

    def where_part(d, hop):
        if hop <= 6:
            return (hop - 1) // 2, ((hop - 1) % 2) * 2 + d
        return 3, {(0, 7): 1, (1, 9): 1, (0, 8): 2, (1, 8): 2, (1, 7): 3, (0, 9): 3}[(d, hop)]

    def selectors(b):
        slots, loads = [], []
        for k, source in enumerate(batches[b]):
            whose = zed if source is None else lax.rem(source[2] + PLANES, PLANES)
            meta = meta_ref[whose]
            if k:
                meta = pltpu.roll(meta, 4 * k, 1)
            slots.append(iota((64, 128), 0).astype(F32) == meta[0:1])
            loads.append(meta[1:2])
        return slots, loads

    def spread(b):
        slots, _ = selectors(b)
        pick = jnp.concatenate([jnp.where(s, 1.0, 0.0) for s in slots], axis=0)
        pick = jnp.transpose(pick, (1, 0)).astype(BF16)
        blocks = []
        for source in batches[b]:
            ref = own.at[0, g0] if source is None else came.at[source[0], source[1]]
            blocks.append(ref[...].reshape(64, ref.shape[-1]))
        rows = jnp.dot(pick, jnp.concatenate(blocks, axis=0), preferred_element_type=F32)
        xs[b] = rows.astype(BF16).reshape(xs.shape[1:])
        pltpu.make_async_copy(xs.at[b, seat], xr.at[b, seat], xrecv.at[b]).start()
        for k in range(1, SEATS):
            spread_copy(b, k).start()

    def spread_copy(b, k):
        to = lax.rem(seat + k, SEATS)
        return pltpu.make_async_remote_copy(
            src_ref=xs.at[b, to], dst_ref=xr.at[b, seat], send_sem=xsend.at[b, k], recv_sem=xrecv.at[b],
            device_id=seat_device(to), device_id_type=MESH,
        )

    def return_copy(b, k):
        to = lax.rem(seat + k, SEATS)
        return pltpu.make_async_remote_copy(
            src_ref=rb.at[b, to], dst_ref=yr.at[b, seat], send_sem=ysend.at[b, k], recv_sem=yrecv.at[b],
            device_id=seat_device(to), device_id_type=MESH,
        )

    def expert(b):
        pltpu.make_async_copy(xs.at[b], xr.at[b], xrecv.at[b]).wait()
        rows = xr[b].reshape(SEATS * 16, xr.shape[-1])
        gate = jnp.dot(rows, wg[...], preferred_element_type=F32)
        up = jnp.dot(rows, wu[...], preferred_element_type=F32)
        active = (jax.nn.silu(gate) * up).astype(BF16)
        result = jnp.dot(active, wd[...], preferred_element_type=F32).astype(BF16)
        rb[b] = result.reshape(rb.shape[1:])
        pltpu.make_async_copy(rb.at[b, seat], yr.at[b, seat], yrecv.at[b]).start()
        for k in range(1, SEATS):
            return_copy(b, k).start()

    def combine(b):
        slots, loads = selectors(b)
        pltpu.make_async_copy(rb.at[b], yr.at[b], yrecv.at[b]).wait()
        rows = yr[b].reshape(SEATS * 16, yr.shape[-1])
        scale = jnp.concatenate([jnp.where(s, w, 0.0) for s, w in zip(slots, loads)], axis=0)
        high = scale.astype(BF16)
        low = (scale - high.astype(F32)).astype(BF16)
        total = jnp.dot(high, rows, preferred_element_type=F32) + jnp.dot(low, rows, preferred_element_type=F32)
        part[b] = total.astype(BF16).reshape(part.shape[1:])

    relay(1)
    relay(2)
    spread(0)
    relay(3)
    relay(4)
    spread(1)
    for w in weights:
        w.wait()
    expert(0)
    relay(5)
    relay(6)
    spread(2)
    expert(1)
    combine(0)
    relay(7)
    relay(8)
    relay(9)
    spread(3)
    expert(2)
    combine(1)
    expert(3)
    combine(2)
    combine(3)

    def hand_back(hop):
        for rel in reversed(kinds_at(hop)):
            for unit in (0, 1):
                for d in (0, 1):
                    fine = valid(off[d], hop, rel)
                    if unit == 1 and rel == 0:
                        fine = fine & (off[d] < SPAN - 1)
                    index = first_block(hop) + rel
                    b, k = where_part(d, hop) if rel == 0 else (0, 0)

                    @pl.when(fine)
                    def _():
                        if rel == 0:
                            if hop < HOPS:
                                later = first_block(hop + 1)

                                @pl.when(off[d] < SPAN - 1 - unit)
                                def _():
                                    backward(d, back.at[d, later, unit], later, unit).wait_recv()
                                    part[b, k, unit] = (
                                        part[b, k, unit].astype(F32) + back[d, later, unit].astype(F32)
                                    ).astype(BF16)

                            backward(d, part.at[b, k, unit], index, unit).start()
                        else:
                            later = first_block(hop + 1) + rel - last[d]
                            backward(d, back.at[d, later, unit], later, unit).wait_recv()
                            backward(d, back.at[d, later, unit], index, unit).start()

    for hop in range(HOPS, 0, -1):
        hand_back(hop)

    first_hop(lambda copy, d, rel, unit: backward(d, back.at[d, rel, unit], rel, unit).wait_recv())
    group, up_rank, down_rank = r["gc"], r["Pc"], r["Mc"]
    lanes = iota((tokens, 64), 1)
    far = jnp.where(zo >= 2, 0, 1)
    far_rank = jnp.where(zo >= 2, up_rank, down_rank)
    plan = [
        ((group == g0) & (r["mxc"] > zo), up_rank, back.at[0, 0]),
        ((group == g0) & (r["mnc"] < zo), down_rank, back.at[1, 0]),
        (group == lax.rem(g0 + 1, GROUPS), up_rank, back.at[0, 1 - last[0]]),
        (group == lax.rem(g0 + GROUPS - 1, GROUPS), down_rank, back.at[1, 1 - last[1]]),
        (group == lax.rem(g0 + 2, GROUPS), far_rank, back.at[far, 2 - jnp.where(zo >= 2, last[0], last[1])]),
        (group == g0, up_rank, part.at[3, 0]),
    ]
    pick = [jnp.where((jnp.where(mask, rank, -1) == lanes), 1.0, 0.0) for mask, rank, _ in plan]
    pick = jnp.concatenate(pick, axis=1).astype(BF16)
    blocks = jnp.concatenate([ref[...].reshape(64, ref.shape[-1]) for _, _, ref in plan], axis=0)
    total = jnp.dot(pick, blocks, preferred_element_type=F32)
    out_ref[...] = (hidden_ref[...].astype(F32) + total).astype(BF16)

    first_hop(lambda copy, *_: copy.wait_send())
    for hop in range(1, HOPS + 1):
        def done(d, rel, unit):
            index = first_block(hop) + rel
            if hop < HOPS:
                ok, there = goes_on(d, hop, rel, unit)

                @pl.when(ok)
                def _():
                    forward(d, came.at[d, index, unit], hop + 1, there, unit).wait_send()

            backward(d, back.at[d, index, unit], index, unit).wait_send()

        arrivals(hop, done)
    for b in range(len(batches)):
        for k in range(1, SEATS):
            spread_copy(b, k).wait_send()
            return_copy(b, k).wait_send()


def route(ids, loads):
    size = ids.shape[0]
    return pl.pallas_call(
        route_body,
        out_shape=jax.ShapeDtypeStruct((PLANES, 8, 128), F32),
        in_specs=[pl.BlockSpec(memory_space=pltpu.VMEM)] * 3,
        out_specs=pl.BlockSpec(memory_space=pltpu.VMEM),
    )(ids, ids.T, loads)


def experts_kernel(hidden, normed, ids, meta, w_gate, w_up, w_down):
    rows, width = normed.shape
    inner = w_gate.shape[2]
    vmem = pl.BlockSpec(memory_space=pltpu.VMEM)
    far = pl.BlockSpec(memory_space=pl.ANY)
    seats = pltpu.VMEM((4, SEATS, 16, width), BF16)
    dma = pltpu.SemaphoreType.DMA
    return pl.pallas_call(
        moe_body,
        out_shape=jax.ShapeDtypeStruct((rows, width), BF16),
        in_specs=[vmem] * 5 + [far] * 3,
        out_specs=vmem,
        scratch_shapes=[
            pltpu.VMEM((width, inner), BF16),
            pltpu.VMEM((width, inner), BF16),
            pltpu.VMEM((inner, width), BF16),
            pltpu.VMEM((2, GROUPS, 2, UNIT, width), BF16),
            pltpu.VMEM((2, BLOCKS, 2, UNIT, width), BF16),
            pltpu.VMEM((2, BLOCKS, 2, UNIT, width), BF16),
            pltpu.VMEM((4, 4, 2, UNIT, width), BF16),
            seats, seats, seats, seats,
            dma((3,)),
            dma((2, BLOCKS, 2)), dma((2, BLOCKS, 2)), dma((2, BLOCKS, 2)), dma((2, BLOCKS, 2)),
            dma((4, SEATS)), dma((4,)), dma((4, SEATS)), dma((4,)),
        ],
        compiler_params=pltpu.CompilerParams(
            collective_id=1, has_side_effects=True, vmem_limit_bytes=60 << 20
        ),
    )(hidden, normed, ids, ids.T, meta, w_gate, w_up, w_down)


def passed_along(block, axis, distance):
    devices = range(lax.axis_size(axis))
    route = [(i - distance, i) for i in devices if i - distance in devices]
    return lax.ppermute(block, axis, route)


def copy_for_each(shard, axis):
    size = lax.axis_size(axis)
    return lax.all_to_all(
        jnp.broadcast_to(shard[None], (size, *shard.shape)), axis, 0, 0, tiled=True
    )


def of_everyone(shard, axis):
    return copy_for_each(shard, axis).sum(axis=0)


def together(arrays, axis):
    ends = [0]
    for a in arrays:
        ends.append(ends[-1] + a.size)
    subtotal = of_everyone(jnp.concatenate([a.ravel() for a in arrays]), axis)
    return tuple((subtotal[b:e].reshape(a.shape) for a, b, e in zip(arrays, ends, ends[1:])))


def per_device(
    conv_value,
    conv_gate,
    kernel,
    conv_bias,
    ln_gain,
    ln_bias,
    out_gain,
    out_weight,
    residual,
    moe_gain,
    expert_ids,
    expert_weights,
    w_gate,
    w_up,
    w_down,
):
    tok_rows, channels = conv_value.shape
    reach_rows = kernel.shape[0] - 1
    full_channels = channels * lax.axis_size("tp")
    gated = (conv_value.astype(jnp.float32) * jax.nn.sigmoid(conv_gate.astype(jnp.float32))).astype(
        jnp.bfloat16
    )
    before = passed_along(gated[tok_rows - reach_rows :], "sp", 1)
    padded = jnp.concatenate([before, gated], axis=0)
    convolved = jnp.zeros((tok_rows, channels), jnp.float32) + conv_bias
    for offset in range(reach_rows + 1):
        convolved = convolved + padded[offset : offset + tok_rows].astype(jnp.float32) * kernel[
            offset
        ].astype(jnp.float32)
    totals = together((jnp.sum(convolved, axis=1), jnp.sum(convolved * convolved, axis=1)), "tp")
    average = (totals[0] / full_channels)[:, None]
    spread = (totals[1] / full_channels)[:, None] - average * average
    swished = jax.nn.silu((convolved - average) * lax.rsqrt(spread + EPSILON) * ln_gain + ln_bias)
    energy = of_everyone(jnp.sum(swished * swished, axis=1), "tp")
    branch = (swished * lax.rsqrt(energy / full_channels + EPSILON)[:, None] * out_gain).astype(
        jnp.bfloat16
    )
    row_count = tok_rows // lax.axis_size("tp")
    regrouped = lax.all_to_all(branch, "tp", split_axis=0, concat_axis=1, tiled=True)
    projected = jnp.dot(regrouped, out_weight, preferred_element_type=jnp.float32)
    hidden = (residual.astype(jnp.float32) + projected).astype(jnp.bfloat16)
    widened = hidden.astype(jnp.float32)
    normed = (
        widened * lax.rsqrt(jnp.mean(widened * widened, axis=1, keepdims=True) + EPSILON) * moe_gain
    ).astype(jnp.bfloat16)
    meta = route(expert_ids, expert_weights)
    cores = jnp.repeat(meta, 2, axis=0)
    shared = lax.all_to_all(cores, "sp", split_axis=0, concat_axis=0, tiled=True)
    mine = lax.dynamic_index_in_dim(
        shared.reshape(PLANES, 2, *meta.shape[1:]), lax.axis_index("sp") % 2, axis=1, keepdims=False
    )
    return experts_kernel(hidden, normed, expert_ids, mine, w_gate, w_up, w_down)


def solution(mesh):
    in_specs = (
        P(("grp", "sp"), "tp"),
        P(("grp", "sp"), "tp"),
        P(None, "tp"),
        P("tp"),
        P("tp"),
        P("tp"),
        P("tp"),
        P(),
        P(("grp", "sp", "tp"), None),
        P(),
        P(("grp", "sp", "tp"), None),
        P(("grp", "sp", "tp"), None),
        P(("sp", "tp"), None, None),
        P(("sp", "tp"), None, None),
        P(("sp", "tp"), None, None),
    )
    out_specs = P(("grp", "sp", "tp"), None)
    return jax.shard_map(
        per_device, mesh=mesh, in_specs=in_specs, out_specs=out_specs, check_vma=False
    )
```

```python
import jax
import jax.numpy as jnp
from jax import lax
from jax.experimental import pallas as pl
from jax.experimental.pallas import tpu as pltpu
from jax.sharding import PartitionSpec as P

EPSILON = 1e-06
MESH = pl.DeviceIdType.MESH
F32 = jnp.float32
BF16 = jnp.bfloat16

SPAN = 4
PLANES = 16
GROUPS = 4
HOPS = 9
SEATS = 8
UNIT = 32
BLOCKS = 3 + 2 * (HOPS - 1)


def first_block(hop):
    return 0 if hop == 1 else 3 + 2 * (hop - 2)


def kinds_at(hop):
    found = []
    for rel in (2, 1, 0):
        if rel == 2 and hop > 1:
            continue
        if any(static_valid(on, hop, rel) for on in range(SPAN)):
            found.append(rel)
    return found


def static_valid(on, hop, rel):
    start = (on - hop) % SPAN
    kind = (start + hop) // SPAN + rel
    return kind <= 1 or (kind == 2 and start >= 2)


def valid(on, hop, rel):
    start = lax.rem(on + 12 - hop, SPAN)
    kind = lax.div(start + hop, SPAN) + rel
    return (kind <= 1) | ((kind == 2) & (start >= 2))


def iota(shape, dim):
    return lax.broadcasted_iota(jnp.int32, shape, dim)


def ranks(col, row):
    size = col.shape[0]
    out = {}
    e1c, e2c = col[:, 0:1], col[:, 1:2]
    e1r, e2r = row[0:1, :], row[1:2, :]
    gc, gr = e1c >> 5, e1r >> 5
    o1c, o2c = (e1c >> 3) & 3, (e2c >> 3) & 3
    o1r, o2r = (e1r >> 3) & 3, (e2r >> 3) & 3
    mxc, mnc = jnp.maximum(o1c, o2c), jnp.minimum(o1c, o2c)
    mxr, mnr = jnp.maximum(o1r, o2r), jnp.minimum(o1r, o2r)
    sub = iota((size, size), 0)
    lane = iota((size, size), 1)
    same = gc == gr
    for name, kc, kr in (("P", 3 - mxc, 3 - mxr), ("M", mnc, mnr)):
        kc = kc * size + iota((size, 1), 0)
        kr = kr * size + iota((1, size), 1)
        out[name + "r"] = jnp.sum((same & (kc < kr)).astype(F32), axis=0, keepdims=True).astype(jnp.int32)
        out[name + "c"] = jnp.sum((same & (kr < kc)).astype(F32), axis=1, keepdims=True).astype(jnp.int32)
    out.update(gc=gc, gr=gr, mxc=mxc, mnc=mnc, sub=sub, lane=lane)
    return out


def route_body(col_ref, row_ref, wcol_ref, meta_ref, zed):
    col, row = col_ref[...], row_ref[...]
    size = col.shape[0]
    zo, g0 = lax.rem(zed, SPAN), lax.div(zed, SPAN)
    r = ranks(col, row)
    e1c, e2c = col[:, 0:1], col[:, 1:2]
    e1r, e2r = row[0:1, :], row[1:2, :]
    earlier = r["lane"] < r["sub"]
    place = []
    for e in (e1c, e2c):
        hit = ((e == e1r) | (e == e2r)) & earlier
        place.append(jnp.sum(hit.astype(F32), axis=1, keepdims=True).astype(jnp.int32))
    group = r["gc"]
    ahead = group - g0
    ahead = jnp.where(ahead < 0, ahead + GROUPS, ahead)
    far_up = jnp.where(zo >= 2, 1, 0)
    lanes = iota((size, 128), 1)
    for plane in range(PLANES):
        slot_row = jnp.full((1, 128), -1.0, F32)
        weight_row = jnp.zeros((1, 128), F32)
        for k, e in enumerate((e1c, e2c)):
            po = plane % SPAN
            own_up = jnp.where(po >= zo, 1, 0)
            up = jnp.where(ahead == 0, own_up, jnp.where(ahead == 1, 1, jnp.where(ahead == 2, far_up, 0)))
            slot = jnp.where(up == 1, r["Pc"], r["Mc"]).astype(F32)
            lane = jnp.where((e >> 3) == plane, (e & 7) * 16 + place[k], -1)
            hit = lane == lanes
            slot_row = slot_row + jnp.sum(jnp.where(hit, slot + 1.0, 0.0), axis=0, keepdims=True)
            weight_row = weight_row + jnp.sum(jnp.where(hit, wcol_ref[:, k : k + 1], 0.0), axis=0, keepdims=True)
        meta_ref[plane] = jnp.concatenate([slot_row, weight_row, jnp.zeros((6, 128), F32)], axis=0)


def moe_body(
    hidden_ref, normed_ref, col_ref, row_ref, meta_ref, wg_hbm, wu_hbm, wd_hbm, out_ref,
    wg, wu, wd, own, came, back, part, xs, xr, rb, yr,
    wsem, fsend, frecv, bsend, brecv, xsend, xrecv, ysend, yrecv,
):
    sp, tp = lax.axis_index("sp"), lax.axis_index("tp")
    zed, core = lax.div(sp, 2), lax.rem(sp, 2)
    zo, g0 = lax.rem(zed, SPAN), lax.div(zed, SPAN)
    seat = core * 4 + tp
    off = (zo, SPAN - 1 - zo)
    last = tuple(jnp.where(o == SPAN - 1, 1, 0) for o in off)
    following = tuple(lax.rem(o + 1, SPAN) for o in off)
    ring_to = ({"sp": lax.rem(zed + 1, PLANES) * 2 + core}, {"sp": lax.rem(zed + PLANES - 1, PLANES) * 2 + core})
    ring_from = (ring_to[1], ring_to[0])

    def seat_device(s):
        return {"sp": zed * 2 + lax.div(s, 4), "tp": lax.rem(s, 4)}

    weights = [
        pltpu.make_async_copy(wg_hbm.at[0], wg, wsem.at[0]),
        pltpu.make_async_copy(wu_hbm.at[0], wu, wsem.at[1]),
        pltpu.make_async_copy(wd_hbm.at[0], wd, wsem.at[2]),
    ]
    for w in weights:
        w.start()

    for d in (0, 1):
        for i in range(3):
            back[d, i] = jnp.zeros(back.shape[2:], BF16)

        @pl.when(off[d] == SPAN - 1)
        def _():
            for hop in range(1, HOPS + 1):
                came[d, first_block(hop), 1] = jnp.zeros(came.shape[3:], BF16)

    barrier = pltpu.get_barrier_semaphore()
    for to in ring_to:
        pl.semaphore_signal(barrier, inc=1, device_id=to, device_id_type=MESH)
    for k in range(1, SEATS):
        pl.semaphore_signal(barrier, inc=1, device_id=seat_device(lax.rem(seat + k, SEATS)), device_id_type=MESH)
    pl.semaphore_wait(barrier, SEATS + 1)

    r = ranks(col_ref[...], row_ref[...])
    normed = normed_ref[...]
    tokens = normed.shape[0]
    for d, name in ((0, "P"), (1, "M")):
        slot = r["gr"] * 64 + r[name + "r"]
        onehot = jnp.where(iota((GROUPS * 64, tokens), 0) == slot, 1.0, 0.0).astype(BF16)
        rows = jnp.dot(onehot, normed, preferred_element_type=F32).astype(BF16)
        own[d] = rows.reshape(own.shape[1:])

    def forward(d, src, hop, index, unit):
        return pltpu.make_async_remote_copy(
            src_ref=src, dst_ref=came.at[d, index, unit],
            send_sem=fsend.at[d, index, unit], recv_sem=frecv.at[d, index, unit],
            device_id=ring_to[d], device_id_type=MESH,
        )

    def backward(d, src, index, unit):
        return pltpu.make_async_remote_copy(
            src_ref=src, dst_ref=back.at[d, index, unit],
            send_sem=bsend.at[d, index, unit], recv_sem=brecv.at[d, index, unit],
            device_id=ring_from[d], device_id_type=MESH,
        )

    def first_hop(act):
        for rel in kinds_at(1):
            for unit in (0, 1):
                for d in (0, 1):
                    kind = rel + last[d]
                    group = lax.rem(g0 + kind, GROUPS) if d == 0 else lax.rem(g0 + GROUPS - kind, GROUPS)
                    fine = valid(following[d], 1, rel)
                    if unit == 1 and rel == 0:
                        fine = fine & (following[d] < SPAN - 1)

                    @pl.when(fine)
                    def _():
                        act(forward(d, own.at[d, group, unit], 1, rel, unit), d, rel, unit)

    first_hop(lambda copy, *_: copy.start())

    def arrivals(hop, act):
        for rel in kinds_at(hop):
            for unit in (0, 1):
                for d in (0, 1):
                    fine = valid(off[d], hop, rel)
                    if unit == 1 and rel == 0:
                        fine = fine & (off[d] < SPAN - 1)

                    @pl.when(fine)
                    def _():
                        act(d, rel, unit)

    def goes_on(d, hop, rel, unit):
        there = rel - last[d]
        ok = there >= 0
        if unit == 1:
            ok = ok & ((there > 0) | (following[d] < SPAN - 1))
        return ok, first_block(hop + 1) + jnp.maximum(there, 0)

    def relay(hop):
        def act(d, rel, unit):
            index = first_block(hop) + rel
            forward(d, came.at[d, index, unit], hop, index, unit).wait_recv()
            if hop < HOPS:
                ok, there = goes_on(d, hop, rel, unit)

                @pl.when(ok)
                def _():
                    forward(d, came.at[d, index, unit], hop + 1, there, unit).start()

        arrivals(hop, act)

    def up_if(flag, a, b):
        return (jnp.where(flag, a[0], b[0]), jnp.where(flag, first_block(a[1]), first_block(b[1])),
                jnp.where(flag, zed - a[1], zed + b[1]))

    def fixed(d, hop):
        return (d, first_block(hop), zed - hop if d == 0 else zed + hop)

    batches = [[fixed(0, h), fixed(1, h), fixed(0, h + 1), fixed(1, h + 1)] for h in (1, 3, 5)]
    batches.append([
        None,
        up_if(zo != 0, (0, 7), (1, 9)),
        up_if(zo >= 2, (0, 8), (1, 8)),
        up_if(zo == 3, (0, 9), (1, 7)),
    ])

    def where_part(d, hop):
        if hop <= 6:
            return (hop - 1) // 2, ((hop - 1) % 2) * 2 + d
        return 3, {(0, 7): 1, (1, 9): 1, (0, 8): 2, (1, 8): 2, (1, 7): 3, (0, 9): 3}[(d, hop)]

    def selectors(b):
        slots, loads = [], []
        for k, source in enumerate(batches[b]):
            whose = zed if source is None else lax.rem(source[2] + PLANES, PLANES)
            meta = meta_ref[whose]
            if k:
                meta = pltpu.roll(meta, 4 * k, 1)
            slots.append(iota((64, 128), 0).astype(F32) == meta[0:1])
            loads.append(meta[1:2])
        return slots, loads

    def spread(b):
        slots, _ = selectors(b)
        pick = jnp.concatenate([jnp.where(s, 1.0, 0.0) for s in slots], axis=0)
        pick = jnp.transpose(pick, (1, 0)).astype(BF16)
        blocks = []
        for source in batches[b]:
            ref = own.at[0, g0] if source is None else came.at[source[0], source[1]]
            blocks.append(ref[...].reshape(64, ref.shape[-1]))
        rows = jnp.dot(pick, jnp.concatenate(blocks, axis=0), preferred_element_type=F32)
        xs[b] = rows.astype(BF16).reshape(xs.shape[1:])
        pltpu.make_async_copy(xs.at[b, seat], xr.at[b, seat], xrecv.at[b]).start()
        for k in range(1, SEATS):
            spread_copy(b, k).start()

    def spread_copy(b, k):
        to = lax.rem(seat + k, SEATS)
        return pltpu.make_async_remote_copy(
            src_ref=xs.at[b, to], dst_ref=xr.at[b, seat], send_sem=xsend.at[b, k], recv_sem=xrecv.at[b],
            device_id=seat_device(to), device_id_type=MESH,
        )

    def return_copy(b, k):
        to = lax.rem(seat + k, SEATS)
        return pltpu.make_async_remote_copy(
            src_ref=rb.at[b, to], dst_ref=yr.at[b, seat], send_sem=ysend.at[b, k], recv_sem=yrecv.at[b],
            device_id=seat_device(to), device_id_type=MESH,
        )

    def expert(b):
        pltpu.make_async_copy(xs.at[b], xr.at[b], xrecv.at[b]).wait()
        rows = xr[b].reshape(SEATS * 16, xr.shape[-1])
        gate = jnp.dot(rows, wg[...], preferred_element_type=F32)
        up = jnp.dot(rows, wu[...], preferred_element_type=F32)
        active = (jax.nn.silu(gate) * up).astype(BF16)
        result = jnp.dot(active, wd[...], preferred_element_type=F32).astype(BF16)
        rb[b] = result.reshape(rb.shape[1:])
        pltpu.make_async_copy(rb.at[b, seat], yr.at[b, seat], yrecv.at[b]).start()
        for k in range(1, SEATS):
            return_copy(b, k).start()

    def combine(b):
        slots, loads = selectors(b)
        pltpu.make_async_copy(rb.at[b], yr.at[b], yrecv.at[b]).wait()
        rows = yr[b].reshape(SEATS * 16, yr.shape[-1])
        scale = jnp.concatenate([jnp.where(s, w, 0.0) for s, w in zip(slots, loads)], axis=0)
        high = scale.astype(BF16)
        low = (scale - high.astype(F32)).astype(BF16)
        total = jnp.dot(high, rows, preferred_element_type=F32) + jnp.dot(low, rows, preferred_element_type=F32)
        part[b] = total.astype(BF16).reshape(part.shape[1:])

    relay(1)
    relay(2)
    spread(0)
    relay(3)
    relay(4)
    spread(1)
    for w in weights:
        w.wait()
    expert(0)
    relay(5)
    relay(6)
    spread(2)
    expert(1)
    combine(0)
    relay(7)
    relay(8)
    relay(9)
    spread(3)
    expert(2)
    combine(1)
    expert(3)
    combine(2)
    combine(3)

    def hand_back(hop):
        for rel in reversed(kinds_at(hop)):
            for unit in (0, 1):
                for d in (0, 1):
                    fine = valid(off[d], hop, rel)
                    if unit == 1 and rel == 0:
                        fine = fine & (off[d] < SPAN - 1)
                    index = first_block(hop) + rel
                    b, k = where_part(d, hop) if rel == 0 else (0, 0)

                    @pl.when(fine)
                    def _():
                        if rel == 0:
                            if hop < HOPS:
                                later = first_block(hop + 1)

                                @pl.when(off[d] < SPAN - 1 - unit)
                                def _():
                                    backward(d, back.at[d, later, unit], later, unit).wait_recv()
                                    part[b, k, unit] = (
                                        part[b, k, unit].astype(F32) + back[d, later, unit].astype(F32)
                                    ).astype(BF16)

                            backward(d, part.at[b, k, unit], index, unit).start()
                        else:
                            later = first_block(hop + 1) + rel - last[d]
                            backward(d, back.at[d, later, unit], later, unit).wait_recv()
                            backward(d, back.at[d, later, unit], index, unit).start()

    for hop in range(HOPS, 0, -1):
        hand_back(hop)

    first_hop(lambda copy, d, rel, unit: backward(d, back.at[d, rel, unit], rel, unit).wait_recv())
    group, up_rank, down_rank = r["gc"], r["Pc"], r["Mc"]
    lanes = iota((tokens, 64), 1)
    far = jnp.where(zo >= 2, 0, 1)
    far_rank = jnp.where(zo >= 2, up_rank, down_rank)
    plan = [
        ((group == g0) & (r["mxc"] > zo), up_rank, back.at[0, 0]),
        ((group == g0) & (r["mnc"] < zo), down_rank, back.at[1, 0]),
        (group == lax.rem(g0 + 1, GROUPS), up_rank, back.at[0, 1 - last[0]]),
        (group == lax.rem(g0 + GROUPS - 1, GROUPS), down_rank, back.at[1, 1 - last[1]]),
        (group == lax.rem(g0 + 2, GROUPS), far_rank, back.at[far, 2 - jnp.where(zo >= 2, last[0], last[1])]),
        (group == g0, up_rank, part.at[3, 0]),
    ]
    pick = [jnp.where((jnp.where(mask, rank, -1) == lanes), 1.0, 0.0) for mask, rank, _ in plan]
    pick = jnp.concatenate(pick, axis=1).astype(BF16)
    blocks = jnp.concatenate([ref[...].reshape(64, ref.shape[-1]) for _, _, ref in plan], axis=0)
    total = jnp.dot(pick, blocks, preferred_element_type=F32)
    out_ref[...] = (hidden_ref[...].astype(F32) + total).astype(BF16)

    first_hop(lambda copy, *_: copy.wait_send())
    for hop in range(1, HOPS + 1):
        def done(d, rel, unit):
            index = first_block(hop) + rel
            if hop < HOPS:
                ok, there = goes_on(d, hop, rel, unit)

                @pl.when(ok)
                def _():
                    forward(d, came.at[d, index, unit], hop + 1, there, unit).wait_send()

            backward(d, back.at[d, index, unit], index, unit).wait_send()

        arrivals(hop, done)
    for b in range(len(batches)):
        for k in range(1, SEATS):
            spread_copy(b, k).wait_send()
            return_copy(b, k).wait_send()


def experts_kernel(hidden, normed, ids, meta, w_gate, w_up, w_down):
    rows, width = normed.shape
    inner = w_gate.shape[2]
    vmem = pl.BlockSpec(memory_space=pltpu.VMEM)
    far = pl.BlockSpec(memory_space=pl.ANY)
    seats = pltpu.VMEM((4, SEATS, 16, width), BF16)
    dma = pltpu.SemaphoreType.DMA
    return pl.pallas_call(
        moe_body,
        out_shape=jax.ShapeDtypeStruct((rows, width), BF16),
        in_specs=[vmem] * 5 + [far] * 3,
        out_specs=vmem,
        scratch_shapes=[
            pltpu.VMEM((width, inner), BF16),
            pltpu.VMEM((width, inner), BF16),
            pltpu.VMEM((inner, width), BF16),
            pltpu.VMEM((2, GROUPS, 2, UNIT, width), BF16),
            pltpu.VMEM((2, BLOCKS, 2, UNIT, width), BF16),
            pltpu.VMEM((2, BLOCKS, 2, UNIT, width), BF16),
            pltpu.VMEM((4, 4, 2, UNIT, width), BF16),
            seats, seats, seats, seats,
            dma((3,)),
            dma((2, BLOCKS, 2)), dma((2, BLOCKS, 2)), dma((2, BLOCKS, 2)), dma((2, BLOCKS, 2)),
            dma((4, SEATS)), dma((4,)), dma((4, SEATS)), dma((4,)),
        ],
        compiler_params=pltpu.CompilerParams(
            collective_id=1, has_side_effects=True, vmem_limit_bytes=60 << 20
        ),
    )(hidden, normed, ids, ids.T, meta, w_gate, w_up, w_down)


def front_body(
    value_ref, gate_ref, taps_ref, vec_ref, gain_ref, col_ref, row_ref, load_ref, weight_hbm, residual_hbm,
    hidden_ref, normed_ref, meta_ref,
    weight, residual, gated, grown, packs, conv, tables,
    lsem, gsend, grecv, hsend, hrecv, psend, precv, tsend, trecv,
):
    sp, tp = lax.axis_index("sp"), lax.axis_index("tp")
    steps, teams = lax.axis_size("sp"), lax.axis_size("tp")
    zed, core = lax.div(sp, 2), lax.rem(sp, 2)
    rows = hidden_ref.shape[0]
    pieces = rows // UNIT
    channels = value_ref.shape[1]

    def team(k):
        return lax.rem(tp + k, teams)

    def column(k):
        return lax.rem(zed + k, PLANES) * 2 + core

    barrier = pltpu.get_barrier_semaphore()
    for k in range(1, teams):
        pl.semaphore_signal(barrier, inc=1, device_id={"tp": team(k)}, device_id_type=MESH)

    @pl.when((sp > 0) & (tp == 0))
    def _():
        for k in range(teams):
            pl.semaphore_signal(barrier, inc=1, device_id={"sp": sp - 1, "tp": k}, device_id_type=MESH)

    for k in range(1, PLANES):
        pl.semaphore_signal(barrier, inc=1, device_id={"sp": column(k)}, device_id_type=MESH)

    fetch_weight = pltpu.make_async_copy(weight_hbm, weight, lsem.at[0])
    fetch_residual = pltpu.make_async_copy(residual_hbm, residual, lsem.at[1])
    fetch_weight.start()
    fetch_residual.start()

    passed = (value_ref[...].astype(F32) * jax.nn.sigmoid(gate_ref[...].astype(F32))).astype(BF16)
    gated[...] = passed.reshape(gated.shape)
    packs[tp, 0 : taps_ref.shape[0]] = taps_ref[...].astype(F32)
    packs[tp, 32:40] = vec_ref[...]

    @pl.when((sp == 0) & (tp == 0))
    def _():
        grown[:, 0] = jnp.zeros((teams, UNIT, channels), BF16)

    route_body(col_ref, row_ref, load_ref, tables, zed)
    pl.semaphore_wait(barrier, teams + PLANES - 2 + jnp.where(sp < steps - 1, 1, 0))

    def whole(to, k):
        return pltpu.make_async_remote_copy(
            src_ref=gated.at[pl.ds(jnp.maximum(to * pieces - 1, 0), pieces + 1)], dst_ref=grown.at[tp],
            send_sem=gsend.at[k], recv_sem=grecv.at[tp], device_id={"tp": to}, device_id_type=MESH,
        )

    def short(to, k):
        return pltpu.make_async_remote_copy(
            src_ref=gated.at[pl.ds(0, pieces)], dst_ref=grown.at[tp, pl.ds(1, pieces)],
            send_sem=gsend.at[k], recv_sem=grecv.at[tp], device_id={"tp": to}, device_id_type=MESH,
        )

    def got(source, first):
        size = pieces if first else pieces + 1
        return pltpu.make_async_remote_copy(
            src_ref=gated.at[pl.ds(0, size)], dst_ref=grown.at[source, pl.ds(1 if first else 0, size)],
            send_sem=gsend.at[0], recv_sem=grecv.at[source], device_id={"tp": source}, device_id_type=MESH,
        )

    def pack_copy(k):
        return pltpu.make_async_remote_copy(
            src_ref=packs.at[tp], dst_ref=packs.at[tp], send_sem=psend.at[k], recv_sem=precv.at[tp],
            device_id={"tp": team(k)}, device_id_type=MESH,
        )

    def halo(source):
        return pltpu.make_async_remote_copy(
            src_ref=gated.at[gated.shape[0] - 1], dst_ref=grown.at[source, 0],
            send_sem=hsend.at[0], recv_sem=hrecv.at[source],
            device_id={"sp": lax.rem(sp + 1, steps), "tp": 0}, device_id_type=MESH,
        )

    def table_copy(k):
        return pltpu.make_async_remote_copy(
            src_ref=tables.at[column(k)  // 2], dst_ref=meta_land(k), send_sem=tsend.at[k], recv_sem=trecv.at[k],
            device_id={"sp": column(k)}, device_id_type=MESH,
        )

    def meta_land(k):
        return tables.at[PLANES + k]

    for k in (2, 1, 3):
        pack_copy(k).start()
        for test, copy in ((team(k) == 0, short), (team(k) > 0, whole)):

            @pl.when(test)
            def _():
                copy(team(k), k).start()

    @pl.when(sp < steps - 1)
    def _():
        halo(tp).start()

    for k in range(1, PLANES):
        table_copy(k).start()

    for test, size in ((tp == 0, 0), (tp > 0, 1)):

        @pl.when(test)
        def _():
            low = jnp.maximum(tp * pieces - 1, 0) if size else 0
            grown[tp, 1 - size : pieces + 1] = gated[pl.ds(low, pieces + size)]

    def wait_part(k):
        source = team(k)
        if k:
            for test, first in ((tp == 0, True), (tp > 0, False)):

                @pl.when(test)
                def _():
                    got(source, first).wait_recv()

            pltpu.make_async_remote_copy(
                src_ref=packs.at[tp], dst_ref=packs.at[source], send_sem=psend.at[k], recv_sem=precv.at[source],
                device_id={"tp": source}, device_id_type=MESH,
            ).wait_recv()

        @pl.when((tp == 0) & (sp > 0))
        def _():
            halo(source).wait_recv()

    reach = taps_ref.shape[0] - 1
    shift0 = UNIT - reach
    for k in (0, 1, 3, 2):
        wait_part(k)
        source = team(k)
        for half in range(channels // 128):
            lanes = pl.ds(half * 128, 128)
            x = grown[source, :, :, lanes].reshape((pieces + 1) * UNIT, 128).astype(F32)
            total = jnp.broadcast_to(packs[source, 32:33, lanes], (rows, 128))
            for r in range(8):
                span = rows if r == 0 else rows + 8
                acc = None
                for q in range(0, (UNIT - r) // 8 + 1):
                    tap = 8 * q + r - shift0
                    if not 0 <= tap <= reach:
                        continue
                    term = x[8 * q : 8 * q + span] * packs[source, tap : tap + 1, lanes]
                    acc = term if acc is None else acc + term
                total = total + (acc if r == 0 else acc[r : r + rows])
            conv[source, :, lanes] = total

    full = channels * teams
    parts = [conv[s] for s in range(teams)]
    average = sum(jnp.sum(p, axis=1, keepdims=True) for p in parts) / full
    spread = sum(jnp.sum(p * p, axis=1, keepdims=True) for p in parts) / full - average * average
    scale = lax.rsqrt(spread + EPSILON)
    energy = jnp.zeros((rows, 1), F32)
    for s in range(teams):
        v = jax.nn.silu((conv[s] - average) * scale * packs[s, 33:34] + packs[s, 34:35])
        conv[s] = v
        energy = energy + jnp.sum(v * v, axis=1, keepdims=True)
    scale = lax.rsqrt(energy / full + EPSILON)
    branch = jnp.concatenate([(conv[s] * scale * packs[s, 35:36]).astype(BF16) for s in range(teams)], axis=1)
    fetch_weight.wait()
    fetch_residual.wait()
    projected = jnp.dot(branch, weight[...], preferred_element_type=F32)
    hidden = (residual[...].astype(F32) + projected).astype(BF16)
    hidden_ref[...] = hidden
    wide = hidden.astype(F32)
    scale = lax.rsqrt(jnp.mean(wide * wide, axis=1, keepdims=True) + EPSILON)
    normed_ref[...] = (wide * scale * gain_ref[...]).astype(BF16)

    meta_ref[zed] = tables[zed]
    for k in range(1, PLANES):
        table_copy(k).wait_recv()
        meta_ref[lax.rem(zed + PLANES - k, PLANES)] = tables[PLANES + k]

    for k in range(1, teams):
        pack_copy(k).wait_send()
        for test, copy in ((team(k) == 0, short), (team(k) > 0, whole)):

            @pl.when(test)
            def _():
                copy(team(k), k).wait_send()

    @pl.when(sp < steps - 1)
    def _():
        halo(tp).wait_send()

    for k in range(1, PLANES):
        table_copy(k).wait_send()


def front_kernel(value, gate, taps, vectors, moe_gain, ids, loads, out_weight, residual):
    rows, width = residual.shape
    tok_rows, channels = value.shape
    teams = lax.axis_size("tp")
    vmem = pl.BlockSpec(memory_space=pltpu.VMEM)
    far = pl.BlockSpec(memory_space=pl.ANY)
    dma = pltpu.SemaphoreType.DMA
    return pl.pallas_call(
        front_body,
        out_shape=(
            jax.ShapeDtypeStruct((rows, width), BF16),
            jax.ShapeDtypeStruct((rows, width), BF16),
            jax.ShapeDtypeStruct((PLANES, 8, 128), F32),
        ),
        in_specs=[vmem] * 8 + [far] * 2,
        out_specs=[vmem] * 3,
        scratch_shapes=[
            pltpu.VMEM(out_weight.shape, BF16),
            pltpu.VMEM((rows, width), BF16),
            pltpu.VMEM((tok_rows // UNIT, UNIT, channels), BF16),
            pltpu.VMEM((teams, rows // UNIT + 1, UNIT, channels), BF16),
            pltpu.VMEM((teams, 40, channels), F32),
            pltpu.VMEM((teams, rows, channels), F32),
            pltpu.VMEM((2 * PLANES, 8, 128), F32),
            dma((2,)), dma((teams,)), dma((teams,)), dma((1,)), dma((teams,)), dma((teams,)), dma((teams,)),
            dma((PLANES,)), dma((PLANES,)),
        ],
        compiler_params=pltpu.CompilerParams(
            collective_id=2, has_side_effects=True, vmem_limit_bytes=40 << 20
        ),
    )(value, gate, taps, vectors, moe_gain, ids, ids.T, loads, out_weight, residual)


def per_device(
    conv_value,
    conv_gate,
    kernel,
    conv_bias,
    ln_gain,
    ln_bias,
    out_gain,
    out_weight,
    residual,
    moe_gain,
    expert_ids,
    expert_weights,
    w_gate,
    w_up,
    w_down,
):
    nothing = jnp.zeros((4, conv_bias.shape[0]), jnp.float32)
    vectors = jnp.concatenate([jnp.stack([conv_bias, ln_gain, ln_bias, out_gain]), nothing], axis=0)
    hidden, normed, meta = front_kernel(
        conv_value, conv_gate, kernel, vectors, moe_gain[None], expert_ids, expert_weights, out_weight, residual
    )
    return experts_kernel(hidden, normed, expert_ids, meta, w_gate, w_up, w_down)


def solution(mesh):
    in_specs = (
        P(("grp", "sp"), "tp"),
        P(("grp", "sp"), "tp"),
        P(None, "tp"),
        P("tp"),
        P("tp"),
        P("tp"),
        P("tp"),
        P(),
        P(("grp", "sp", "tp"), None),
        P(),
        P(("grp", "sp", "tp"), None),
        P(("grp", "sp", "tp"), None),
        P(("sp", "tp"), None, None),
        P(("sp", "tp"), None, None),
        P(("sp", "tp"), None, None),
    )
    out_specs = P(("grp", "sp", "tp"), None)
    return jax.shard_map(
        per_device, mesh=mesh, in_specs=in_specs, out_specs=out_specs, check_vma=False
    )
```

```python
import functools

import jax
import jax.numpy as jnp
from jax import lax
from jax.experimental import pallas as pl
from jax.experimental.pallas import tpu as pltpu
from jax.sharding import PartitionSpec as P

EPSILON = 1e-06
MESH = pl.DeviceIdType.MESH
F32 = jnp.float32
BF16 = jnp.bfloat16

SPAN = 4
PLANES = 16
GROUPS = 4
HOPS = 9
SEATS = 8
UNIT = 32
NARROW, WIDE = 48, 64
BLOCKS = 3 + 2 * (HOPS - 1)


def first_block(hop):
    return 0 if hop == 1 else 3 + 2 * (hop - 2)


def kinds_at(hop):
    found = []
    for rel in (2, 1, 0):
        if rel == 2 and hop > 1:
            continue
        if any(static_valid(on, hop, rel) for on in range(SPAN)):
            found.append(rel)
    return found


def static_valid(on, hop, rel):
    start = (on - hop) % SPAN
    kind = (start + hop) // SPAN + rel
    return kind <= 1 or (kind == 2 and start >= 2)


def valid(on, hop, rel):
    start = lax.rem(on + 12 - hop, SPAN)
    kind = lax.div(start + hop, SPAN) + rel
    return (kind <= 1) | ((kind == 2) & (start >= 2))


def iota(shape, dim):
    return lax.broadcasted_iota(jnp.int32, shape, dim)


def ranks(col, row):
    size = col.shape[0]
    out = {}
    e1c, e2c = col[:, 0:1], col[:, 1:2]
    e1r, e2r = row[0:1, :], row[1:2, :]
    gc, gr = e1c >> 5, e1r >> 5
    o1c, o2c = (e1c >> 3) & 3, (e2c >> 3) & 3
    o1r, o2r = (e1r >> 3) & 3, (e2r >> 3) & 3
    mxc, mnc = jnp.maximum(o1c, o2c), jnp.minimum(o1c, o2c)
    mxr, mnr = jnp.maximum(o1r, o2r), jnp.minimum(o1r, o2r)
    sub = iota((size, size), 0)
    lane = iota((size, size), 1)
    same = gc == gr
    for name, kc, kr in (("P", 3 - mxc, 3 - mxr), ("M", mnc, mnr)):
        kc = kc * size + iota((size, 1), 0)
        kr = kr * size + iota((1, size), 1)
        out[name + "r"] = jnp.sum((same & (kc < kr)).astype(F32), axis=0, keepdims=True).astype(jnp.int32)
        out[name + "c"] = jnp.sum((same & (kr < kc)).astype(F32), axis=1, keepdims=True).astype(jnp.int32)
    out.update(gc=gc, gr=gr, mxc=mxc, mnc=mnc, sub=sub, lane=lane)
    return out


def route_tables(row, loads, meta_ref, zed):
    size = row.shape[1]
    cols = columns_of(row, loads)
    col = cols[:, 0:2].astype(jnp.int32)
    zo, g0 = lax.rem(zed, SPAN), lax.div(zed, SPAN)
    r = ranks(col, row)
    e1c, e2c = col[:, 0:1], col[:, 1:2]
    e1r, e2r = row[0:1, :], row[1:2, :]
    earlier = r["lane"] < r["sub"]
    place = []
    for e in (e1c, e2c):
        hit = ((e == e1r) | (e == e2r)) & earlier
        place.append(jnp.sum(hit.astype(F32), axis=1, keepdims=True).astype(jnp.int32))
    group = r["gc"]
    ahead = group - g0
    ahead = jnp.where(ahead < 0, ahead + GROUPS, ahead)
    far_up = jnp.where(zo >= 2, 1, 0)
    lanes = iota((size, 128), 1)
    for plane in range(PLANES):
        slot_row = jnp.full((1, 128), -1.0, F32)
        weight_row = jnp.zeros((1, 128), F32)
        for k, e in enumerate((e1c, e2c)):
            po = plane % SPAN
            own_up = jnp.where(po >= zo, 1, 0)
            up = jnp.where(ahead == 0, own_up, jnp.where(ahead == 1, 1, jnp.where(ahead == 2, far_up, 0)))
            slot = jnp.where(up == 1, r["Pc"], r["Mc"]).astype(F32)
            lane = jnp.where((e >> 3) == plane, (e & 7) * 16 + place[k], -1)
            hit = lane == lanes
            slot_row = slot_row + jnp.sum(jnp.where(hit, slot + 1.0, 0.0), axis=0, keepdims=True)
            weight_row = weight_row + jnp.sum(jnp.where(hit, cols[:, 2 + k : 3 + k], 0.0), axis=0, keepdims=True)
        meta_ref[plane] = jnp.concatenate([slot_row, weight_row, jnp.zeros((6, 128), F32)], axis=0)
    return jnp.broadcast_to(jnp.where(r["Pr"] >= NARROW, 1.0, 0.0), (8, size))


def columns_of(*rows):
    stack = jnp.concatenate([r.astype(F32) for r in rows], axis=0)
    stack = jnp.concatenate([stack, jnp.zeros((8 - stack.shape[0], stack.shape[1]), F32)], axis=0)
    return jnp.transpose(stack, (1, 0))


def moe_body(
    cap, normed_hbm, row_hbm, meta_hbm, wg_hbm, wu_hbm, wd_hbm, out_ref,
    normed_ref, row_ref, meta_ref, wg, wu, wd, own, came, back, part, xs, xr, rb, yr,
    isem, wsem, fsend, frecv, bsend, brecv, xsend, xrecv, ysend, yrecv,
):
    sp, tp = lax.axis_index("sp"), lax.axis_index("tp")
    zed, core = lax.div(sp, 2), lax.rem(sp, 2)
    zo, g0 = lax.rem(zed, SPAN), lax.div(zed, SPAN)
    seat = core * 4 + tp
    off = (zo, SPAN - 1 - zo)
    last = tuple(jnp.where(o == SPAN - 1, 1, 0) for o in off)
    following = tuple(lax.rem(o + 1, SPAN) for o in off)
    ring_to = ({"sp": lax.rem(zed + 1, PLANES) * 2 + core}, {"sp": lax.rem(zed + PLANES - 1, PLANES) * 2 + core})
    ring_from = (ring_to[1], ring_to[0])

    def seat_device(s):
        return {"sp": zed * 2 + lax.div(s, 4), "tp": lax.rem(s, 4)}

    small = [
        pltpu.make_async_copy(row_hbm, row_ref, isem.at[0]),
        pltpu.make_async_copy(normed_hbm, normed_ref, isem.at[1]),
        pltpu.make_async_copy(meta_hbm, meta_ref, isem.at[2]),
    ]
    for w in small:
        w.start()
    pieces = (pl.ds(0, UNIT), pl.ds(UNIT, cap - UNIT))
    weights = [
        pltpu.make_async_copy(wg_hbm.at[0], wg, wsem.at[0]),
        pltpu.make_async_copy(wu_hbm.at[0], wu, wsem.at[1]),
        pltpu.make_async_copy(wd_hbm.at[0], wd, wsem.at[2]),
    ]
    for w in weights:
        w.start()

    for d in (0, 1):
        for i in range(3):
            back[d, i] = jnp.zeros(back.shape[2:], BF16)

        @pl.when(off[d] == SPAN - 1)
        def _():
            for hop in range(1, HOPS + 1):
                came[d, first_block(hop), UNIT:cap] = jnp.zeros((cap - UNIT, came.shape[3]), BF16)

    barrier = pltpu.get_barrier_semaphore()
    for to in ring_to:
        pl.semaphore_signal(barrier, inc=1, device_id=to, device_id_type=MESH)
    for k in range(1, SEATS):
        pl.semaphore_signal(barrier, inc=1, device_id=seat_device(lax.rem(seat + k, SEATS)), device_id_type=MESH)

    small[0].wait()
    row = row_ref[...]
    tokens = row.shape[1]
    r = ranks(columns_of(row)[:, 0:2].astype(jnp.int32), row)
    small[1].wait()
    normed = normed_ref[...]
    for d, name in ((0, "P"), (1, "M")):
        slot = r["gr"] * cap + r[name + "r"]
        onehot = jnp.where(iota((GROUPS * cap, tokens), 0) == slot, 1.0, 0.0).astype(BF16)
        rows = jnp.dot(onehot, normed, preferred_element_type=F32).astype(BF16)
        own[d] = rows.reshape(own.shape[1:])
    pl.semaphore_wait(barrier, SEATS + 1)

    def forward(d, src, hop, index, unit):
        return pltpu.make_async_remote_copy(
            src_ref=src, dst_ref=came.at[d, index, pieces[unit]],
            send_sem=fsend.at[d, index, unit], recv_sem=frecv.at[d, index, unit],
            device_id=ring_to[d], device_id_type=MESH,
        )

    def backward(d, src, index, unit):
        return pltpu.make_async_remote_copy(
            src_ref=src, dst_ref=back.at[d, index, pieces[unit]],
            send_sem=bsend.at[d, index, unit], recv_sem=brecv.at[d, index, unit],
            device_id=ring_from[d], device_id_type=MESH,
        )

    def first_hop(act):
        for rel in kinds_at(1):
            for unit in (0, 1):
                for d in (0, 1):
                    kind = rel + last[d]
                    group = lax.rem(g0 + kind, GROUPS) if d == 0 else lax.rem(g0 + GROUPS - kind, GROUPS)
                    fine = valid(following[d], 1, rel)
                    if unit == 1 and rel == 0:
                        fine = fine & (following[d] < SPAN - 1)

                    @pl.when(fine)
                    def _():
                        act(forward(d, own.at[d, group, pieces[unit]], 1, rel, unit), d, rel, unit)

    first_hop(lambda copy, *_: copy.start())

    def arrivals(hop, act):
        for rel in kinds_at(hop):
            for unit in (0, 1):
                for d in (0, 1):
                    fine = valid(off[d], hop, rel)
                    if unit == 1 and rel == 0:
                        fine = fine & (off[d] < SPAN - 1)

                    @pl.when(fine)
                    def _():
                        act(d, rel, unit)

    def goes_on(d, hop, rel, unit):
        there = rel - last[d]
        ok = there >= 0
        if unit == 1:
            ok = ok & ((there > 0) | (following[d] < SPAN - 1))
        return ok, first_block(hop + 1) + jnp.maximum(there, 0)

    def relay(hop):
        def act(d, rel, unit):
            index = first_block(hop) + rel
            forward(d, came.at[d, index, pieces[unit]], hop, index, unit).wait_recv()
            if hop < HOPS:
                ok, there = goes_on(d, hop, rel, unit)

                @pl.when(ok)
                def _():
                    forward(d, came.at[d, index, pieces[unit]], hop + 1, there, unit).start()

        arrivals(hop, act)

    def up_if(flag, a, b):
        return (jnp.where(flag, a[0], b[0]), jnp.where(flag, first_block(a[1]), first_block(b[1])),
                jnp.where(flag, zed - a[1], zed + b[1]))

    def fixed(d, hop):
        return (d, first_block(hop), zed - hop if d == 0 else zed + hop)

    batches = [[fixed(0, h), fixed(1, h), fixed(0, h + 1), fixed(1, h + 1)] for h in (1, 3, 5)]
    batches.append([
        None,
        up_if(zo != 0, (0, 7), (1, 9)),
        up_if(zo >= 2, (0, 8), (1, 8)),
        up_if(zo == 3, (0, 9), (1, 7)),
    ])

    def where_part(d, hop):
        if hop <= 6:
            return (hop - 1) // 2, ((hop - 1) % 2) * 2 + d
        return 3, {(0, 7): 1, (1, 9): 1, (0, 8): 2, (1, 8): 2, (1, 7): 3, (0, 9): 3}[(d, hop)]

    def selectors(b):
        slots, loads = [], []
        for k, source in enumerate(batches[b]):
            whose = zed if source is None else lax.rem(source[2] + PLANES, PLANES)
            meta = meta_ref[whose]
            if k:
                meta = pltpu.roll(meta, 4 * k, 1)
            slots.append(iota((cap, 128), 0).astype(F32) == meta[0:1])
            loads.append(meta[1:2])
        return slots, loads

    def spread(b):
        slots, _ = selectors(b)
        pick = jnp.concatenate([jnp.where(s, 1.0, 0.0) for s in slots], axis=0)
        pick = jnp.transpose(pick, (1, 0)).astype(BF16)
        blocks = []
        for source in batches[b]:
            ref = own.at[0, g0] if source is None else came.at[source[0], source[1]]
            blocks.append(ref[...])
        rows = jnp.dot(pick, jnp.concatenate(blocks, axis=0), preferred_element_type=F32)
        xs[b] = rows.astype(BF16).reshape(xs.shape[1:])
        pltpu.make_async_copy(xs.at[b, seat], xr.at[b, seat], xrecv.at[b]).start()
        for k in range(1, SEATS):
            spread_copy(b, k).start()

    def spread_copy(b, k):
        to = lax.rem(seat + k, SEATS)
        return pltpu.make_async_remote_copy(
            src_ref=xs.at[b, to], dst_ref=xr.at[b, seat], send_sem=xsend.at[b, k], recv_sem=xrecv.at[b],
            device_id=seat_device(to), device_id_type=MESH,
        )

    def return_copy(b, k):
        to = lax.rem(seat + k, SEATS)
        return pltpu.make_async_remote_copy(
            src_ref=rb.at[b, to], dst_ref=yr.at[b, seat], send_sem=ysend.at[b, k], recv_sem=yrecv.at[b],
            device_id=seat_device(to), device_id_type=MESH,
        )

    def expert(b):
        pltpu.make_async_copy(xs.at[b], xr.at[b], xrecv.at[b]).wait()
        rows = xr[b].reshape(SEATS * 16, xr.shape[-1])
        gate = jnp.dot(rows, wg[...], preferred_element_type=F32)
        up = jnp.dot(rows, wu[...], preferred_element_type=F32)
        active = (jax.nn.silu(gate) * up).astype(BF16)
        result = jnp.dot(active, wd[...], preferred_element_type=F32).astype(BF16)
        rb[b] = result.reshape(rb.shape[1:])
        pltpu.make_async_copy(rb.at[b, seat], yr.at[b, seat], yrecv.at[b]).start()
        for k in range(1, SEATS):
            return_copy(b, k).start()

    def combine(b):
        slots, loads = selectors(b)
        pltpu.make_async_copy(rb.at[b], yr.at[b], yrecv.at[b]).wait()
        rows = yr[b].reshape(SEATS * 16, yr.shape[-1])
        scale = jnp.concatenate([jnp.where(s, w, 0.0) for s, w in zip(slots, loads)], axis=0)
        high = scale.astype(BF16)
        low = (scale - high.astype(F32)).astype(BF16)
        total = jnp.dot(high, rows, preferred_element_type=F32) + jnp.dot(low, rows, preferred_element_type=F32)
        part[b] = total.astype(BF16).reshape(part.shape[1:])

    small[2].wait()
    tight = cap < WIDE
    relay(1)
    relay(2)
    spread(0)
    relay(3)
    relay(4)
    spread(1)
    for w in weights:
        w.wait()
    if tight:
        expert(0)
    relay(5)
    relay(6)
    spread(2)
    if tight:
        expert(1)
        combine(0)
    relay(7)
    relay(8)
    relay(9)
    spread(3)

    def early(d, hop, rel):
        if rel or hop > 6:
            return None
        if hop == 6:
            return off[d] == SPAN - 1
        return off[d] >= SPAN - 2

    def hand_back(hop, when):
        for rel in reversed(kinds_at(hop)):
            for unit in (0, 1):
                for d in (0, 1):
                    fine = valid(off[d], hop, rel)
                    if unit == 1 and rel == 0:
                        fine = fine & (off[d] < SPAN - 1)
                    ahead = early(d, hop, rel)
                    if when == "end":
                        if ahead is None or unit == 1:
                            continue
                        fine = fine & (off[d] == SPAN - 1)
                    elif when == "middle":
                        if ahead is None or hop == 6:
                            continue
                        fine = fine & (off[d] == SPAN - 2)
                    elif when == "rest" and ahead is not None:
                        fine = fine & jnp.logical_not(ahead)
                    index = first_block(hop) + rel
                    b, k = where_part(d, hop) if rel == 0 else (0, 0)

                    @pl.when(fine)
                    def _():
                        if rel == 0:
                            if hop < HOPS and when != "end":
                                later = first_block(hop + 1)

                                @pl.when(off[d] < SPAN - 1 - unit)
                                def _():
                                    backward(d, back.at[d, later, pieces[unit]], later, unit).wait_recv()
                                    part[b, k, pieces[unit]] = (
                                        part[b, k, pieces[unit]].astype(F32) + back[d, later, pieces[unit]].astype(F32)
                                    ).astype(BF16)

                            backward(d, part.at[b, k, pieces[unit]], index, unit).start()
                        else:
                            later = first_block(hop + 1) + rel - last[d]
                            backward(d, back.at[d, later, pieces[unit]], later, unit).wait_recv()
                            backward(d, back.at[d, later, pieces[unit]], index, unit).start()

    if tight:
        expert(2)
        combine(1)
        combine(2)
        for hop in range(6, 0, -1):
            hand_back(hop, "end")
        expert(3)
        for hop in range(5, 0, -1):
            hand_back(hop, "middle")
    else:

        @pl.loop(0, len(batches))
        def _(b):
            expert(b)

        for b in range(len(batches) - 1):
            combine(b)
    combine(3)
    for hop in range(HOPS, 0, -1):
        hand_back(hop, "rest" if tight else "all")

    first_hop(lambda copy, d, rel, unit: backward(d, back.at[d, rel, pieces[unit]], rel, unit).wait_recv())
    group, up_rank, down_rank = r["gc"], r["Pc"], r["Mc"]
    far = jnp.where(zo >= 2, 0, 1)
    far_rank = jnp.where(zo >= 2, up_rank, down_rank)
    plan = [
        ((group == g0) & (r["mxc"] > zo), up_rank, back.at[0, 0]),
        ((group == g0) & (r["mnc"] < zo), down_rank, back.at[1, 0]),
        (group == lax.rem(g0 + 1, GROUPS), up_rank, back.at[0, 1 - last[0]]),
        (group == lax.rem(g0 + GROUPS - 1, GROUPS), down_rank, back.at[1, 1 - last[1]]),
        (group == lax.rem(g0 + 2, GROUPS), far_rank, back.at[far, 2 - jnp.where(zo >= 2, last[0], last[1])]),
        (group == g0, up_rank, part.at[3, 0]),
    ]
    lanes = iota((tokens, len(plan) * cap), 1)
    pick = jnp.zeros(lanes.shape, F32)
    for i, (mask, rank, _) in enumerate(plan):
        pick = pick + jnp.where(jnp.where(mask, rank + i * cap, -1) == lanes, 1.0, 0.0)
    blocks = jnp.concatenate([ref[...] for _, _, ref in plan], axis=0)
    out_ref[...] = jnp.dot(pick.astype(BF16), blocks, preferred_element_type=F32)

    first_hop(lambda copy, *_: copy.wait_send())
    for hop in range(1, HOPS + 1):
        def done(d, rel, unit):
            index = first_block(hop) + rel
            if hop < HOPS:
                ok, there = goes_on(d, hop, rel, unit)

                @pl.when(ok)
                def _():
                    forward(d, came.at[d, index, pieces[unit]], hop + 1, there, unit).wait_send()

            backward(d, back.at[d, index, pieces[unit]], index, unit).wait_send()

        arrivals(hop, done)
    for b in range(len(batches)):
        for k in range(1, SEATS):
            spread_copy(b, k).wait_send()
            return_copy(b, k).wait_send()


def experts_kernel(cap, normed, ids, meta, w_gate, w_up, w_down):
    rows, width = normed.shape
    inner = w_gate.shape[2]
    far = pl.BlockSpec(memory_space=pltpu.HBM)
    seats = pltpu.VMEM((4, SEATS, 16, width), BF16)
    dma = pltpu.SemaphoreType.DMA
    return pl.pallas_call(
        functools.partial(moe_body, cap),
        out_shape=jax.ShapeDtypeStruct((rows, width), F32),
        in_specs=[far] * 6,
        out_specs=pl.BlockSpec(memory_space=pltpu.VMEM),
        scratch_shapes=[
            pltpu.VMEM((rows, width), BF16),
            pltpu.VMEM(ids.shape, jnp.int32),
            pltpu.VMEM(meta.shape, F32),
            pltpu.VMEM((width, inner), BF16),
            pltpu.VMEM((width, inner), BF16),
            pltpu.VMEM((inner, width), BF16),
            pltpu.VMEM((2, GROUPS, cap, width), BF16),
            pltpu.VMEM((2, BLOCKS, cap, width), BF16),
            pltpu.VMEM((2, BLOCKS, cap, width), BF16),
            pltpu.VMEM((4, 4, cap, width), BF16),
            seats, seats, seats, seats,
            dma((3,)), dma((3,)),
            dma((2, BLOCKS, 2)), dma((2, BLOCKS, 2)), dma((2, BLOCKS, 2)), dma((2, BLOCKS, 2)),
            dma((4, SEATS)), dma((4,)), dma((4, SEATS)), dma((4,)),
        ],
        compiler_params=pltpu.CompilerParams(
            collective_id=1 if cap == WIDE else 3, has_side_effects=True, vmem_limit_bytes=60 << 20
        ),
    )(normed, ids, meta, w_gate, w_up, w_down)


def front_body(
    value_hbm, gate_hbm, taps_hbm, bias_hbm, scale_hbm, shift_hbm, branch_hbm, gain_hbm, row_hbm, load_hbm,
    weight_hbm, residual_hbm,
    hidden_ref, normed_ref, meta_ref, crowd_ref,
    value_ref, gate_ref, taps_ref, vectors, gain_ref, row_ref, load_ref, weight, residual, gated, grown, packs, conv,
    tables, flags, heard,
    lsem, csend, crecv, gsend, grecv, hsend, hrecv, psend, precv, tsend, trecv,
):
    sp, tp = lax.axis_index("sp"), lax.axis_index("tp")
    steps, teams = lax.axis_size("sp"), lax.axis_size("tp")
    zed, core = lax.div(sp, 2), lax.rem(sp, 2)
    rows = hidden_ref.shape[0]
    pieces = rows // UNIT
    channels = value_ref.shape[1]
    parts = lax.axis_size("grp")
    other = zed * 2 + 1 - core
    loads = [
        (row_hbm, row_ref), (load_hbm, load_ref),
        (value_hbm, value_ref), (gate_hbm, gate_ref), (taps_hbm, taps_ref),
        (bias_hbm, vectors.at[0]), (scale_hbm, vectors.at[1]), (shift_hbm, vectors.at[2]), (branch_hbm, vectors.at[3]),
        (residual_hbm, residual), (gain_hbm, gain_ref), (weight_hbm, weight),
    ]
    copies = [pltpu.make_async_copy(a, b, lsem.at[i]) for i, (a, b) in enumerate(loads)]
    for copy in copies:
        copy.start()
    fetch, first, late = copies[:2], copies[2:9], copies[9:]

    def part_of(k):
        return lax.rem(lax.axis_index("grp") + k, parts)

    def team(k):
        return lax.rem(tp + k, teams)

    def column(k):
        return lax.rem(zed + k, PLANES) * 2 + core

    barrier = pltpu.get_barrier_semaphore()
    for k in range(1, teams):
        pl.semaphore_signal(barrier, inc=1, device_id={"tp": team(k)}, device_id_type=MESH)

    @pl.when((sp > 0) & (tp == 0))
    def _():
        for k in range(teams):
            pl.semaphore_signal(barrier, inc=1, device_id={"sp": sp - 1, "tp": k}, device_id_type=MESH)

    for k in range(1, PLANES):
        pl.semaphore_signal(barrier, inc=1, device_id={"sp": column(k)}, device_id_type=MESH)
    for k in range(teams):
        pl.semaphore_signal(barrier, inc=1, device_id={"sp": other, "tp": k}, device_id_type=MESH)
    for k in range(1, parts):
        pl.semaphore_signal(barrier, inc=1, device_id={"grp": part_of(k)}, device_id_type=MESH)

    for copy in fetch:
        copy.wait()
    crowd = route_tables(row_ref[...], load_ref[...], tables, zed)
    flags[0] = crowd
    for copy in first:
        copy.wait()
    passed = (value_ref[...].astype(F32) * jax.nn.sigmoid(gate_ref[...].astype(F32))).astype(BF16)
    gated[...] = passed.reshape(gated.shape)
    packs[tp, 0 : taps_ref.shape[0]] = taps_ref[...].astype(F32)
    for i in range(4):
        packs[tp, 32 + i : 33 + i] = vectors[i]

    @pl.when((sp == 0) & (tp == 0))
    def _():
        grown[:, 0] = jnp.zeros((teams, UNIT, channels), BF16)

    pl.semaphore_wait(barrier, 2 * teams + PLANES + parts - 3 + jnp.where(sp < steps - 1, 1, 0))

    def whole(to, k):
        return pltpu.make_async_remote_copy(
            src_ref=gated.at[pl.ds(jnp.maximum(to * pieces - 1, 0), pieces + 1)], dst_ref=grown.at[tp],
            send_sem=gsend.at[k], recv_sem=grecv.at[tp], device_id={"tp": to}, device_id_type=MESH,
        )

    def short(to, k):
        return pltpu.make_async_remote_copy(
            src_ref=gated.at[pl.ds(0, pieces)], dst_ref=grown.at[tp, pl.ds(1, pieces)],
            send_sem=gsend.at[k], recv_sem=grecv.at[tp], device_id={"tp": to}, device_id_type=MESH,
        )

    def got(source, first):
        size = pieces if first else pieces + 1
        return pltpu.make_async_remote_copy(
            src_ref=gated.at[pl.ds(0, size)], dst_ref=grown.at[source, pl.ds(1 if first else 0, size)],
            send_sem=gsend.at[0], recv_sem=grecv.at[source], device_id={"tp": source}, device_id_type=MESH,
        )

    def pack_copy(k):
        return pltpu.make_async_remote_copy(
            src_ref=packs.at[tp], dst_ref=packs.at[tp], send_sem=psend.at[k], recv_sem=precv.at[tp],
            device_id={"tp": team(k)}, device_id_type=MESH,
        )

    def halo(source):
        return pltpu.make_async_remote_copy(
            src_ref=gated.at[gated.shape[0] - 1], dst_ref=grown.at[source, 0],
            send_sem=hsend.at[0], recv_sem=hrecv.at[source],
            device_id={"sp": lax.rem(sp + 1, steps), "tp": 0}, device_id_type=MESH,
        )

    def table_copy(k):
        return pltpu.make_async_remote_copy(
            src_ref=tables.at[column(k)  // 2], dst_ref=meta_land(k), send_sem=tsend.at[k], recv_sem=trecv.at[k],
            device_id={"sp": column(k)}, device_id_type=MESH,
        )

    def meta_land(k):
        return tables.at[PLANES + k]

    for k in (2, 1, 3):
        pack_copy(k).start()
        for test, copy in ((team(k) == 0, short), (team(k) > 0, whole)):

            @pl.when(test)
            def _():
                copy(team(k), k).start()

    @pl.when(sp < steps - 1)
    def _():
        halo(tp).start()

    for k in range(1, PLANES):
        table_copy(k).start()

    plane_mates = [{"tp": team(k)} for k in range(1, teams)] + [{"sp": other, "tp": k} for k in range(teams)]
    rounds = [
        [(to, i) for i, to in enumerate(plane_mates)],
        [({"grp": part_of(k)}, k) for k in range(1, parts)],
        [({"sp": column(k)}, k) for k in range(1, PLANES)],
    ]

    def flag_copies(stage):
        base = (0, 16, 16 + parts)[stage]
        return [
            pltpu.make_async_remote_copy(
                src_ref=flags.at[stage], dst_ref=heard.at[land(stage, base, i)], send_sem=csend.at[base + i],
                recv_sem=crecv.at[land(stage, base, i)], device_id=to, device_id_type=MESH,
            )
            for to, i in rounds[stage]
        ]

    def land(stage, base, i):
        if stage == 0 and i >= teams - 1:
            return base + teams - 1 + tp
        return base + i

    def hear(stage):
        base = (0, 16, 16 + parts)[stage]
        seen = flags[stage]
        for (to, i) in rounds[stage]:
            pltpu.make_async_remote_copy(
                src_ref=flags.at[stage], dst_ref=heard.at[base + i], send_sem=csend.at[base + i],
                recv_sem=crecv.at[base + i], device_id=to, device_id_type=MESH,
            ).wait_recv()
            seen = jnp.maximum(seen, heard[base + i])
        flags[stage + 1] = seen
        if stage < 2:
            for copy in flag_copies(stage + 1):
                copy.start()

    for copy in flag_copies(0):
        copy.start()

    for test, size in ((tp == 0, 0), (tp > 0, 1)):

        @pl.when(test)
        def _():
            low = jnp.maximum(tp * pieces - 1, 0) if size else 0
            grown[tp, 1 - size : pieces + 1] = gated[pl.ds(low, pieces + size)]

    def wait_part(k):
        source = team(k)
        if k:
            for test, first in ((tp == 0, True), (tp > 0, False)):

                @pl.when(test)
                def _():
                    got(source, first).wait_recv()

            pltpu.make_async_remote_copy(
                src_ref=packs.at[tp], dst_ref=packs.at[source], send_sem=psend.at[k], recv_sem=precv.at[source],
                device_id={"tp": source}, device_id_type=MESH,
            ).wait_recv()

        @pl.when((tp == 0) & (sp > 0))
        def _():
            halo(source).wait_recv()

    reach = taps_ref.shape[0] - 1
    shift0 = UNIT - reach
    for k in (0, 1, 3, 2):
        wait_part(k)
        if k in (1, 2):
            hear(0 if k == 1 else 1)
        source = team(k)
        for half in range(channels // 128):
            lanes = pl.ds(half * 128, 128)
            x = grown[source, :, :, lanes].reshape((pieces + 1) * UNIT, 128).astype(F32)
            total = jnp.broadcast_to(packs[source, 32:33, lanes], (rows, 128))
            for r in range(8):
                span = rows if r == 0 else rows + 8
                acc = None
                for q in range(0, (UNIT - r) // 8 + 1):
                    tap = 8 * q + r - shift0
                    if not 0 <= tap <= reach:
                        continue
                    term = x[8 * q : 8 * q + span] * packs[source, tap : tap + 1, lanes]
                    acc = term if acc is None else acc + term
                total = total + (acc if r == 0 else acc[r : r + rows])
            conv[source, :, lanes] = total

    full = channels * teams
    pieces_of = [conv[s] for s in range(teams)]
    average = sum(jnp.sum(p, axis=1, keepdims=True) for p in pieces_of) / full
    spread = sum(jnp.sum(p * p, axis=1, keepdims=True) for p in pieces_of) / full - average * average
    scale = lax.rsqrt(spread + EPSILON)
    energy = jnp.zeros((rows, 1), F32)
    for s in range(teams):
        v = jax.nn.silu((conv[s] - average) * scale * packs[s, 33:34] + packs[s, 34:35])
        conv[s] = v
        energy = energy + jnp.sum(v * v, axis=1, keepdims=True)
    scale = lax.rsqrt(energy / full + EPSILON)
    branch = jnp.concatenate([(conv[s] * scale * packs[s, 35:36]).astype(BF16) for s in range(teams)], axis=1)
    for copy in late:
        copy.wait()
    projected = jnp.dot(branch, weight[...], preferred_element_type=F32)
    hidden = (residual[...].astype(F32) + projected).astype(BF16)
    hidden_ref[...] = hidden
    wide = hidden.astype(F32)
    scale = lax.rsqrt(jnp.mean(wide * wide, axis=1, keepdims=True) + EPSILON)
    normed_ref[...] = (wide * scale * gain_ref[...]).astype(BF16)

    meta_ref[zed] = tables[zed]
    for k in range(1, PLANES):
        table_copy(k).wait_recv()
        meta_ref[lax.rem(zed + PLANES - k, PLANES)] = tables[PLANES + k]

    hear(2)
    crowd_ref[0] = jnp.max(flags[3]).astype(jnp.int32)
    for stage in range(3):
        for copy in flag_copies(stage):
            copy.wait_send()

    for k in range(1, teams):
        pack_copy(k).wait_send()
        for test, copy in ((team(k) == 0, short), (team(k) > 0, whole)):

            @pl.when(test)
            def _():
                copy(team(k), k).wait_send()

    @pl.when(sp < steps - 1)
    def _():
        halo(tp).wait_send()

    for k in range(1, PLANES):
        table_copy(k).wait_send()


def front_kernel(value, gate, taps, vectors, moe_gain, ids, loads, out_weight, residual):
    rows, width = residual.shape
    tok_rows, channels = value.shape
    teams = lax.axis_size("tp")
    vmem = pl.BlockSpec(memory_space=pltpu.VMEM)
    far = pl.BlockSpec(memory_space=pltpu.HBM)
    dma = pltpu.SemaphoreType.DMA
    voices = 16 + lax.axis_size("grp") + PLANES
    return pl.pallas_call(
        front_body,
        out_shape=(
            jax.ShapeDtypeStruct((rows, width), BF16),
            jax.ShapeDtypeStruct((rows, width), BF16),
            jax.ShapeDtypeStruct((PLANES, 8, 128), F32),
            jax.ShapeDtypeStruct((1,), jnp.int32),
        ),
        in_specs=[far] * 12,
        out_specs=[vmem] * 3 + [pl.BlockSpec(memory_space=pltpu.SMEM)],
        scratch_shapes=[
            pltpu.VMEM(value.shape, BF16),
            pltpu.VMEM(value.shape, BF16),
            pltpu.VMEM(taps.shape, BF16),
            pltpu.VMEM((4, 1, channels), F32),
            pltpu.VMEM(moe_gain.shape, F32),
            pltpu.VMEM(ids.shape, jnp.int32),
            pltpu.VMEM(loads.shape, F32),
            pltpu.VMEM(out_weight.shape, BF16),
            pltpu.VMEM((rows, width), BF16),
            pltpu.VMEM((tok_rows // UNIT, UNIT, channels), BF16),
            pltpu.VMEM((teams, rows // UNIT + 1, UNIT, channels), BF16),
            pltpu.VMEM((teams, 40, channels), F32),
            pltpu.VMEM((teams, rows, channels), F32),
            pltpu.VMEM((2 * PLANES, 8, 128), F32),
            pltpu.VMEM((4, 8, 128), F32),
            pltpu.VMEM((voices, 8, 128), F32),
            dma((12,)), dma((voices,)), dma((voices,)),
            dma((teams,)), dma((teams,)), dma((1,)), dma((teams,)), dma((teams,)), dma((teams,)),
            dma((PLANES,)), dma((PLANES,)),
        ],
        compiler_params=pltpu.CompilerParams(
            collective_id=2, has_side_effects=True, vmem_limit_bytes=60 << 20
        ),
    )(value, gate, taps, *vectors, moe_gain, ids, loads, out_weight, residual)


def per_device(
    conv_value,
    conv_gate,
    kernel,
    conv_bias,
    ln_gain,
    ln_bias,
    out_gain,
    out_weight,
    residual,
    moe_gain,
    expert_ids,
    expert_weights,
    w_gate,
    w_up,
    w_down,
):
    ids = expert_ids.T
    vectors = [v[None] for v in (conv_bias, ln_gain, ln_bias, out_gain)]
    hidden, normed, meta, crowd = front_kernel(
        conv_value, conv_gate, kernel, vectors, moe_gain[None], ids, expert_weights.T, out_weight, residual
    )
    added = lax.cond(
        crowd[0] > 0,
        functools.partial(experts_kernel, WIDE),
        functools.partial(experts_kernel, NARROW),
        normed, ids, meta, w_gate, w_up, w_down,
    )
    return (hidden.astype(F32) + added).astype(BF16)


def solution(mesh):
    in_specs = (
        P(("grp", "sp"), "tp"),
        P(("grp", "sp"), "tp"),
        P(None, "tp"),
        P("tp"),
        P("tp"),
        P("tp"),
        P("tp"),
        P(),
        P(("grp", "sp", "tp"), None),
        P(),
        P(("grp", "sp", "tp"), None),
        P(("grp", "sp", "tp"), None),
        P(("sp", "tp"), None, None),
        P(("sp", "tp"), None, None),
        P(("sp", "tp"), None, None),
    )
    out_specs = P(("grp", "sp", "tp"), None)
    return jax.shard_map(
        per_device, mesh=mesh, in_specs=in_specs, out_specs=out_specs, check_vma=False
    )
```

```python
import functools

import jax
import jax.numpy as jnp
from jax import lax
from jax.experimental import pallas as pl
from jax.experimental.pallas import tpu as pltpu
from jax.sharding import PartitionSpec as P

EPSILON = 1e-06
MESH = pl.DeviceIdType.MESH
F32 = jnp.float32
BF16 = jnp.bfloat16

SPAN = 4
PLANES = 16
GROUPS = 4
HOPS = 9
SEATS = 8
UNIT = 32
NARROW, WIDE = 48, 64
BLOCKS = 3 + 2 * (HOPS - 1)
BATCHES = 8
FAR = (
    ((1, 7), (0, 7), (0, 7), (0, 7)),
    ((1, 8), (1, 7), (1, 7), (0, 8)),
    ((1, 9), (1, 8), (0, 8), (0, 9)),
)
ORDER = (
    ("r", 1), ("s", 0), ("r", 2), ("s", 1), ("e", 0), ("r", 3), ("s", 2), ("e", 1),
    ("r", 4), ("s", 3), ("e", 2), ("r", 5), ("s", 4), ("e", 3), ("c", 2), ("r", 6),
    ("s", 5), ("e", 4), ("r", 7), ("c", 3), ("e", 5), ("w", 0, 4), ("r", 8), ("s", 6),
    ("c", 4), ("w", 0, 5), ("w", 0, 3), ("r", 9), ("s", 7), ("w", 1, 4), ("c", 5), ("e", 6),
    ("w", 0, 6), ("w", 1, 5), ("e", 7), ("c", 1), ("w", 0, 2), ("w", 2, 4), ("w", 1, 6), ("c", 6),
    ("w", 1, 3), ("w", 2, 6), ("c", 7), ("w", 2, 5), ("w", 0, 9), ("w", 0, 8), ("w", 1, 9), ("w", 1, 8),
    ("c", 0), ("w", 0, 7), ("w", 3, 6), ("w", 2, 9), ("w", 3, 5), ("w", 1, 7), ("w", 1, 2), ("w", 2, 8),
    ("w", 2, 7), ("w", 4, 6), ("w", 3, 9), ("w", 3, 8), ("w", 2, 3), ("w", 4, 9), ("w", 3, 7), ("w", 5, 9),
    ("w", 4, 8), ("w", 5, 8), ("w", 6, 9), ("w", 3, 4), ("w", 4, 7), ("w", 0, 1), ("w", 4, 5), ("w", 6, 8),
    ("w", 5, 7), ("w", 7, 9), ("w", 5, 6), ("w", 7, 8), ("w", 8, 9), ("w", 6, 7),
)


def first_block(hop):
    return 0 if hop == 1 else 3 + 2 * (hop - 2)


def kinds_at(hop):
    found = []
    for rel in (2, 1, 0):
        if rel == 2 and hop > 1:
            continue
        if any(static_valid(on, hop, rel) for on in range(SPAN)):
            found.append(rel)
    return found


def static_valid(on, hop, rel):
    start = (on - hop) % SPAN
    kind = (start + hop) // SPAN + rel
    return kind <= 1 or (kind == 2 and start >= 2)


def real(wave, end):
    hop, rel = end - wave, wave // SPAN
    return (rel < 2 or hop == 1) and static_valid(SPAN - 1 - wave % SPAN, hop, rel)


def where_part(d, hop, place):
    if hop <= 6:
        return hop - 1, d
    return ((6, 1), (7, 0), (7, 1))[[FAR[i][place] for i in range(3)].index((d, hop))]


def valid(on, hop, rel):
    start = lax.rem(on + 12 - hop, SPAN)
    kind = lax.div(start + hop, SPAN) + rel
    return (kind <= 1) | ((kind == 2) & (start >= 2))


def iota(shape, dim):
    return lax.broadcasted_iota(jnp.int32, shape, dim)


def ranks(col, row):
    size = col.shape[0]
    out = {}
    e1c, e2c = col[:, 0:1], col[:, 1:2]
    e1r, e2r = row[0:1, :], row[1:2, :]
    gc, gr = e1c >> 5, e1r >> 5
    o1c, o2c = (e1c >> 3) & 3, (e2c >> 3) & 3
    o1r, o2r = (e1r >> 3) & 3, (e2r >> 3) & 3
    mxc, mnc = jnp.maximum(o1c, o2c), jnp.minimum(o1c, o2c)
    mxr, mnr = jnp.maximum(o1r, o2r), jnp.minimum(o1r, o2r)
    sub = iota((size, size), 0)
    lane = iota((size, size), 1)
    same = gc == gr
    for name, kc, kr in (("P", 3 - mxc, 3 - mxr), ("M", mnc, mnr)):
        kc = kc * size + iota((size, 1), 0)
        kr = kr * size + iota((1, size), 1)
        out[name + "r"] = jnp.sum((same & (kc < kr)).astype(F32), axis=0, keepdims=True).astype(jnp.int32)
        out[name + "c"] = jnp.sum((same & (kr < kc)).astype(F32), axis=1, keepdims=True).astype(jnp.int32)
    out.update(gc=gc, gr=gr, mxc=mxc, mnc=mnc, sub=sub, lane=lane)
    return out


def route_tables(row, loads, meta_ref, zed):
    size = row.shape[1]
    cols = columns_of(row, loads)
    col = cols[:, 0:2].astype(jnp.int32)
    zo, g0 = lax.rem(zed, SPAN), lax.div(zed, SPAN)
    r = ranks(col, row)
    e1c, e2c = col[:, 0:1], col[:, 1:2]
    e1r, e2r = row[0:1, :], row[1:2, :]
    earlier = r["lane"] < r["sub"]
    place = []
    for e in (e1c, e2c):
        hit = ((e == e1r) | (e == e2r)) & earlier
        place.append(jnp.sum(hit.astype(F32), axis=1, keepdims=True).astype(jnp.int32))
    group = r["gc"]
    ahead = group - g0
    ahead = jnp.where(ahead < 0, ahead + GROUPS, ahead)
    far_up = jnp.where(zo >= 2, 1, 0)
    lanes = iota((size, 128), 1)
    for plane in range(PLANES):
        slot_row = jnp.full((1, 128), -1.0, F32)
        weight_row = jnp.zeros((1, 128), F32)
        for k, e in enumerate((e1c, e2c)):
            po = plane % SPAN
            own_up = jnp.where(po >= zo, 1, 0)
            up = jnp.where(ahead == 0, own_up, jnp.where(ahead == 1, 1, jnp.where(ahead == 2, far_up, 0)))
            slot = jnp.where(up == 1, r["Pc"], r["Mc"]).astype(F32)
            lane = jnp.where((e >> 3) == plane, (e & 7) * 8 + place[k], -1)
            hit = lane == lanes
            slot_row = slot_row + jnp.sum(jnp.where(hit, slot + 1.0, 0.0), axis=0, keepdims=True)
            weight_row = weight_row + jnp.sum(jnp.where(hit, cols[:, 2 + k : 3 + k], 0.0), axis=0, keepdims=True)
        meta_ref[plane] = jnp.concatenate([slot_row, weight_row, jnp.zeros((6, 128), F32)], axis=0)
    return jnp.broadcast_to(jnp.where(r["Pr"] >= NARROW, 1.0, 0.0), (8, size))


def columns_of(*rows):
    stack = jnp.concatenate([r.astype(F32) for r in rows], axis=0)
    stack = jnp.concatenate([stack, jnp.zeros((8 - stack.shape[0], stack.shape[1]), F32)], axis=0)
    return jnp.transpose(stack, (1, 0))


def moe_body(
    cap, normed_hbm, row_hbm, meta_hbm, wg_hbm, wu_hbm, wd_hbm, out_ref,
    normed_ref, row_ref, meta_ref, wg, wu, wd, active, own, came, back, part, xs, xr, rb, yr,
    isem, wsem, fsend, frecv, bsend, brecv, xsend, xrecv, ysend, yrecv,
):
    sp, tp = lax.axis_index("sp"), lax.axis_index("tp")
    zed, core = lax.div(sp, 2), lax.rem(sp, 2)
    zo, g0 = lax.rem(zed, SPAN), lax.div(zed, SPAN)
    seat = core * 4 + tp
    off = (zo, SPAN - 1 - zo)
    last = tuple(jnp.where(o == SPAN - 1, 1, 0) for o in off)
    following = tuple(lax.rem(o + 1, SPAN) for o in off)
    ring_to = ({"sp": lax.rem(zed + 1, PLANES) * 2 + core}, {"sp": lax.rem(zed + PLANES - 1, PLANES) * 2 + core})
    ring_from = (ring_to[1], ring_to[0])

    def seat_device(s):
        return {"sp": zed * 2 + lax.div(s, 4), "tp": lax.rem(s, 4)}

    small = [
        pltpu.make_async_copy(row_hbm, row_ref, isem.at[0]),
        pltpu.make_async_copy(normed_hbm, normed_ref, isem.at[1]),
        pltpu.make_async_copy(meta_hbm, meta_ref, isem.at[2]),
    ]
    for w in small:
        w.start()
    pieces = (pl.ds(0, UNIT), pl.ds(UNIT, cap - UNIT))
    weights = [
        pltpu.make_async_copy(wg_hbm.at[0], wg, wsem.at[0]),
        pltpu.make_async_copy(wu_hbm.at[0], wu, wsem.at[1]),
        pltpu.make_async_copy(wd_hbm.at[0], wd, wsem.at[2]),
    ]
    for w in weights:
        w.start()

    for d in (0, 1):
        for i in range(3):
            back[d, i] = jnp.zeros(back.shape[2:], BF16)

        @pl.when(off[d] == SPAN - 1)
        def _():
            for hop in range(1, HOPS + 1):
                came[d, first_block(hop), UNIT:cap] = jnp.zeros((cap - UNIT, came.shape[3]), BF16)

    barrier = pltpu.get_barrier_semaphore()
    for to in ring_to:
        pl.semaphore_signal(barrier, inc=1, device_id=to, device_id_type=MESH)
    for k in range(1, SEATS):
        pl.semaphore_signal(barrier, inc=1, device_id=seat_device(lax.rem(seat + k, SEATS)), device_id_type=MESH)

    small[0].wait()
    row = row_ref[...]
    tokens = row.shape[1]
    r = ranks(columns_of(row)[:, 0:2].astype(jnp.int32), row)
    small[1].wait()
    for d, name in ((0, "P"), (1, "M")):
        slot = r["gr"] * cap + r[name + "r"]
        onehot = jnp.where(iota((GROUPS * cap, tokens), 0) == slot, 1.0, 0.0).astype(BF16)

        @pl.loop(0, own.shape[-1] // 512)
        def _(i):
            cols = pl.ds(pl.multiple_of(i * 512, 512), 512)
            rows = jnp.dot(onehot, normed_ref[:, cols], preferred_element_type=F32).astype(BF16)
            own[d, :, :, cols] = rows.reshape(GROUPS, cap, 512)

    pl.semaphore_wait(barrier, SEATS + 1)

    def forward(d, src, hop, index, unit):
        return pltpu.make_async_remote_copy(
            src_ref=src, dst_ref=came.at[d, index, pieces[unit]],
            send_sem=fsend.at[d, index, unit], recv_sem=frecv.at[d, index, unit],
            device_id=ring_to[d], device_id_type=MESH,
        )

    def backward(d, src, index, unit):
        return pltpu.make_async_remote_copy(
            src_ref=src, dst_ref=back.at[d, index, pieces[unit]],
            send_sem=bsend.at[d, index, unit], recv_sem=brecv.at[d, index, unit],
            device_id=ring_from[d], device_id_type=MESH,
        )

    def first_hop(act):
        for rel in kinds_at(1):
            for unit in (0, 1):
                for d in (0, 1):
                    kind = rel + last[d]
                    group = lax.rem(g0 + kind, GROUPS) if d == 0 else lax.rem(g0 + GROUPS - kind, GROUPS)
                    fine = valid(following[d], 1, rel)
                    if unit == 1 and rel == 0:
                        fine = fine & (following[d] < SPAN - 1)

                    @pl.when(fine)
                    def _():
                        act(forward(d, own.at[d, group, pieces[unit]], 1, rel, unit), d, rel, unit)

    first_hop(lambda copy, *_: copy.start())

    def arrivals(hop, act):
        for rel in kinds_at(hop):
            for unit in (0, 1):
                for d in (0, 1):
                    fine = valid(off[d], hop, rel)
                    if unit == 1 and rel == 0:
                        fine = fine & (off[d] < SPAN - 1)

                    @pl.when(fine)
                    def _():
                        act(d, rel, unit)

    def goes_on(d, hop, rel, unit):
        there = rel - last[d]
        ok = there >= 0
        if unit == 1:
            ok = ok & ((there > 0) | (following[d] < SPAN - 1))
        return ok, first_block(hop + 1) + jnp.maximum(there, 0)

    def relay(hop):
        def act(d, rel, unit):
            index = first_block(hop) + rel
            forward(d, came.at[d, index, pieces[unit]], hop, index, unit).wait_recv()
            if hop < HOPS:
                ok, there = goes_on(d, hop, rel, unit)

                @pl.when(ok)
                def _():
                    forward(d, came.at[d, index, pieces[unit]], hop + 1, there, unit).start()

        arrivals(hop, act)

    def near(b):
        hop = b + 1
        index = jnp.where(b == 0, 0, 2 * b + 1)
        return [(0, index, zed + PLANES - hop), (1, index, zed + hop)]

    def by_place(options):
        out = []
        for values in zip(*[(d, first_block(h), PLANES - h if d == 0 else h) for d, h in options]):
            pick = jnp.int32(values[0])
            for i in range(1, SPAN):
                pick = jnp.where(zo == i, values[i], pick)
            out.append(pick)
        return out[0], out[1], zed + out[2]

    def sources(b):
        if isinstance(b, int) and b >= 6:
            return ([None] if b == 6 else []) + [by_place(FAR[i]) for i in ((0,) if b == 6 else (1, 2))]
        return near(b)

    def selectors(b):
        slots, loads = [], []
        for k, source in enumerate(sources(b)):
            whose = zed if source is None else lax.rem(source[2], PLANES)
            meta = meta_ref[whose]
            if k:
                meta = pltpu.roll(meta, 4 * k, 1)
            slots.append(iota((cap, SEATS * 8), 0).astype(F32) == meta[0:1, 0 : SEATS * 8])
            loads.append(meta[1:2, 0 : SEATS * 8])
        return slots, loads

    def spread(b):
        slots, _ = selectors(b)
        pick = jnp.concatenate([jnp.where(s, 1.0, 0.0) for s in slots], axis=0)
        pick = jnp.transpose(pick, (1, 0)).astype(BF16)
        refs = [own.at[0, g0] if source is None else came.at[source[0], source[1]] for source in sources(b)]

        @pl.loop(0, xs.shape[-1] // 512)
        def _(i):
            cols = pl.ds(pl.multiple_of(i * 512, 512), 512)
            blocks = jnp.concatenate([ref[:, cols] for ref in refs], axis=0)
            rows = jnp.dot(pick, blocks, preferred_element_type=F32).astype(BF16)
            xs[b, :, :, cols] = rows.reshape(SEATS, 8, 512)

        pltpu.make_async_copy(xs.at[b, seat], xr.at[b, seat], xrecv.at[b]).start()
        for k in range(1, SEATS):
            spread_copy(b, k).start()

    def spread_copy(b, k):
        to = lax.rem(seat + k, SEATS)
        return pltpu.make_async_remote_copy(
            src_ref=xs.at[b, to], dst_ref=xr.at[b, seat], send_sem=xsend.at[b, k], recv_sem=xrecv.at[b],
            device_id=seat_device(to), device_id_type=MESH,
        )

    def return_copy(b, k):
        to = lax.rem(seat + k, SEATS)
        return pltpu.make_async_remote_copy(
            src_ref=rb.at[b, to], dst_ref=yr.at[b, seat], send_sem=ysend.at[b, k], recv_sem=yrecv.at[b],
            device_id=seat_device(to), device_id_type=MESH,
        )

    def expert(b):
        pltpu.make_async_copy(xs.at[b], xr.at[b], xrecv.at[b]).wait()
        rows = xr[b].reshape(SEATS * 8, xr.shape[-1])

        @pl.loop(0, wg.shape[1] // 256)
        def _(i):
            cols = pl.ds(pl.multiple_of(i * 256, 256), 256)
            gate = jnp.dot(rows, wg[:, cols], preferred_element_type=F32)
            up = jnp.dot(rows, wu[:, cols], preferred_element_type=F32)
            active[:, cols] = (jax.nn.silu(gate) * up).astype(BF16)

        @pl.loop(0, wd.shape[1] // 512)
        def _(i):
            cols = pl.ds(pl.multiple_of(i * 512, 512), 512)
            result = jnp.dot(active[...], wd[:, cols], preferred_element_type=F32).astype(BF16)
            rb[b, :, :, cols] = result.reshape(SEATS, 8, 512)

        pltpu.make_async_copy(rb.at[b, seat], yr.at[b, seat], yrecv.at[b]).start()
        for k in range(1, SEATS):
            return_copy(b, k).start()

    def combine(b):
        slots, loads = selectors(b)
        pltpu.make_async_copy(rb.at[b], yr.at[b], yrecv.at[b]).wait()
        scale = jnp.concatenate([jnp.where(s, w, 0.0) for s, w in zip(slots, loads)], axis=0)
        high = scale.astype(BF16)
        low = (scale - high.astype(F32)).astype(BF16)

        @pl.loop(0, yr.shape[-1] // 512)
        def _(i):
            cols = pl.ds(pl.multiple_of(i * 512, 512), 512)
            rows = yr[b, :, :, cols].reshape(SEATS * 8, 512)
            total = jnp.dot(high, rows, preferred_element_type=F32) + jnp.dot(low, rows, preferred_element_type=F32)
            part[b, :, :, cols] = total.astype(BF16).reshape(2, cap, 512)

    def item(wave, end):
        hop, rel, place = end - wave, wave // SPAN, SPAN - 1 - wave % SPAN
        for d in (0, 1):

            @pl.when(off[d] == place)
            def _():
                index = first_block(hop) + rel
                for unit in (0, 1):
                    if rel:
                        later = first_block(hop + 1) + rel - (place == SPAN - 1)
                        backward(d, back.at[d, later, pieces[unit]], later, unit).wait_recv()
                        backward(d, back.at[d, later, pieces[unit]], index, unit).start()
                    elif unit == 0 or place < SPAN - 1:
                        b, k = where_part(d, hop, place if d == 0 else SPAN - 1 - place)
                        mine = part.at[b, k, pieces[unit]]
                        if place < SPAN - 1 - unit:
                            later = first_block(hop + 1)
                            far = back.at[d, later, pieces[unit]]
                            backward(d, far, later, unit).wait_recv()
                            mine[...] = (mine[...].astype(F32) + far[...].astype(F32)).astype(BF16)
                        backward(d, mine, index, unit).start()

    small[2].wait()
    acts = dict(r=relay, s=spread, e=expert, c=combine, w=item)
    if cap < WIDE:
        fresh = True
        for name, *where in ORDER:
            if name == "e" and fresh:
                for w in weights:
                    w.wait()
                fresh = False
            acts[name](*where)
    else:
        for hop in range(1, HOPS + 1):
            relay(hop)
        for w in weights:
            w.wait()
        for act in (spread, expert, combine):

            @pl.loop(0, 6)
            def _(b):
                act(b)

            act(6)
            act(7)
        for hop in range(HOPS, 0, -1):
            for end in range(hop, HOPS + 1):
                if real(end - hop, end):
                    item(end - hop, end)

    first_hop(lambda copy, d, rel, unit: backward(d, back.at[d, rel, pieces[unit]], rel, unit).wait_recv())
    group, up_rank, down_rank = r["gc"], r["Pc"], r["Mc"]
    far = jnp.where(zo >= 2, 0, 1)
    far_rank = jnp.where(zo >= 2, up_rank, down_rank)
    plan = [
        ((group == g0) & (r["mxc"] > zo), up_rank, back.at[0, 0]),
        ((group == g0) & (r["mnc"] < zo), down_rank, back.at[1, 0]),
        (group == lax.rem(g0 + 1, GROUPS), up_rank, back.at[0, 1 - last[0]]),
        (group == lax.rem(g0 + GROUPS - 1, GROUPS), down_rank, back.at[1, 1 - last[1]]),
        (group == lax.rem(g0 + 2, GROUPS), far_rank, back.at[far, 2 - jnp.where(zo >= 2, last[0], last[1])]),
        (group == g0, up_rank, part.at[6, 0]),
    ]
    lanes = iota((tokens, len(plan) * cap), 1)
    pick = jnp.zeros(lanes.shape, F32)
    for i, (mask, rank, _) in enumerate(plan):
        pick = pick + jnp.where(jnp.where(mask, rank + i * cap, -1) == lanes, 1.0, 0.0)
    pick = pick.astype(BF16)

    @pl.loop(0, out_ref.shape[1] // 512)
    def _(i):
        cols = pl.ds(pl.multiple_of(i * 512, 512), 512)
        blocks = jnp.concatenate([ref[:, cols] for _, _, ref in plan], axis=0)
        out_ref[:, cols] = jnp.dot(pick, blocks, preferred_element_type=F32)

    first_hop(lambda copy, *_: copy.wait_send())
    for hop in range(1, HOPS + 1):
        def done(d, rel, unit):
            index = first_block(hop) + rel
            if hop < HOPS:
                ok, there = goes_on(d, hop, rel, unit)

                @pl.when(ok)
                def _():
                    forward(d, came.at[d, index, pieces[unit]], hop + 1, there, unit).wait_send()

            backward(d, back.at[d, index, pieces[unit]], index, unit).wait_send()

        arrivals(hop, done)
    for b in range(BATCHES):
        for k in range(1, SEATS):
            spread_copy(b, k).wait_send()
            return_copy(b, k).wait_send()


def experts_kernel(cap, normed, ids, meta, w_gate, w_up, w_down):
    rows, width = normed.shape
    inner = w_gate.shape[2]
    far = pl.BlockSpec(memory_space=pltpu.HBM)
    seats = pltpu.VMEM((BATCHES, SEATS, 8, width), BF16)
    dma = pltpu.SemaphoreType.DMA
    return pl.pallas_call(
        functools.partial(moe_body, cap),
        out_shape=jax.ShapeDtypeStruct((rows, width), F32),
        in_specs=[far] * 6,
        out_specs=pl.BlockSpec(memory_space=pltpu.VMEM),
        scratch_shapes=[
            pltpu.VMEM((rows, width), BF16),
            pltpu.VMEM(ids.shape, jnp.int32),
            pltpu.VMEM(meta.shape, F32),
            pltpu.VMEM((width, inner), BF16),
            pltpu.VMEM((width, inner), BF16),
            pltpu.VMEM((inner, width), BF16),
            pltpu.VMEM((SEATS * 8, inner), BF16),
            pltpu.VMEM((2, GROUPS, cap, width), BF16),
            pltpu.VMEM((2, BLOCKS, cap, width), BF16),
            pltpu.VMEM((2, BLOCKS, cap, width), BF16),
            pltpu.VMEM((BATCHES, 2, cap, width), BF16),
            seats, seats, seats, seats,
            dma((3,)), dma((3,)),
            dma((2, BLOCKS, 2)), dma((2, BLOCKS, 2)), dma((2, BLOCKS, 2)), dma((2, BLOCKS, 2)),
            dma((BATCHES, SEATS)), dma((BATCHES,)), dma((BATCHES, SEATS)), dma((BATCHES,)),
        ],
        compiler_params=pltpu.CompilerParams(
            collective_id=1 if cap == WIDE else 3, has_side_effects=True, vmem_limit_bytes=60 << 20
        ),
    )(normed, ids, meta, w_gate, w_up, w_down)


def front_body(
    value_hbm, gate_hbm, taps_hbm, bias_hbm, scale_hbm, shift_hbm, branch_hbm, gain_hbm, row_hbm, load_hbm,
    weight_hbm, residual_hbm,
    hidden_ref, normed_ref, meta_ref, crowd_ref,
    value_ref, gate_ref, taps_ref, vectors, gain_ref, row_ref, load_ref, weight, residual, gated, grown, packs, conv,
    tables, flags, heard,
    lsem, csend, crecv, gsend, grecv, hsend, hrecv, psend, precv, tsend, trecv,
):
    sp, tp = lax.axis_index("sp"), lax.axis_index("tp")
    steps, teams = lax.axis_size("sp"), lax.axis_size("tp")
    zed, core = lax.div(sp, 2), lax.rem(sp, 2)
    rows = hidden_ref.shape[0]
    pieces = rows // UNIT
    channels = value_ref.shape[1]
    parts = lax.axis_size("grp")
    other = zed * 2 + 1 - core
    loads = [
        (row_hbm, row_ref), (load_hbm, load_ref),
        (value_hbm, value_ref), (gate_hbm, gate_ref), (taps_hbm, taps_ref),
        (bias_hbm, vectors.at[0]), (scale_hbm, vectors.at[1]), (shift_hbm, vectors.at[2]), (branch_hbm, vectors.at[3]),
        (residual_hbm, residual), (gain_hbm, gain_ref), (weight_hbm, weight),
    ]
    copies = [pltpu.make_async_copy(a, b, lsem.at[i]) for i, (a, b) in enumerate(loads)]
    for copy in copies:
        copy.start()
    fetch, first, late = copies[:2], copies[2:9], copies[9:]

    def part_of(k):
        return lax.rem(lax.axis_index("grp") + k, parts)

    def team(k):
        return lax.rem(tp + k, teams)

    def column(k):
        return lax.rem(zed + k, PLANES) * 2 + core

    barrier = pltpu.get_barrier_semaphore()
    for k in range(1, teams):
        pl.semaphore_signal(barrier, inc=1, device_id={"tp": team(k)}, device_id_type=MESH)

    @pl.when((sp > 0) & (tp == 0))
    def _():
        for k in range(teams):
            pl.semaphore_signal(barrier, inc=1, device_id={"sp": sp - 1, "tp": k}, device_id_type=MESH)

    for k in range(1, PLANES):
        pl.semaphore_signal(barrier, inc=1, device_id={"sp": column(k)}, device_id_type=MESH)
    for k in range(teams):
        pl.semaphore_signal(barrier, inc=1, device_id={"sp": other, "tp": k}, device_id_type=MESH)
    for k in range(1, parts):
        pl.semaphore_signal(barrier, inc=1, device_id={"grp": part_of(k)}, device_id_type=MESH)

    for copy in fetch:
        copy.wait()
    crowd = route_tables(row_ref[...], load_ref[...], tables, zed)
    flags[0] = crowd
    for copy in first:
        copy.wait()
    passed = (value_ref[...].astype(F32) * jax.nn.sigmoid(gate_ref[...].astype(F32))).astype(BF16)
    gated[...] = passed.reshape(gated.shape)
    packs[tp, 0 : taps_ref.shape[0]] = taps_ref[...].astype(F32)
    for i in range(4):
        packs[tp, 32 + i : 33 + i] = vectors[i]

    @pl.when((sp == 0) & (tp == 0))
    def _():
        grown[:, 0] = jnp.zeros((teams, UNIT, channels), BF16)

    pl.semaphore_wait(barrier, 2 * teams + PLANES + parts - 3 + jnp.where(sp < steps - 1, 1, 0))

    def whole(to, k):
        return pltpu.make_async_remote_copy(
            src_ref=gated.at[pl.ds(jnp.maximum(to * pieces - 1, 0), pieces + 1)], dst_ref=grown.at[tp],
            send_sem=gsend.at[k], recv_sem=grecv.at[tp], device_id={"tp": to}, device_id_type=MESH,
        )

    def short(to, k):
        return pltpu.make_async_remote_copy(
            src_ref=gated.at[pl.ds(0, pieces)], dst_ref=grown.at[tp, pl.ds(1, pieces)],
            send_sem=gsend.at[k], recv_sem=grecv.at[tp], device_id={"tp": to}, device_id_type=MESH,
        )

    def got(source, first):
        size = pieces if first else pieces + 1
        return pltpu.make_async_remote_copy(
            src_ref=gated.at[pl.ds(0, size)], dst_ref=grown.at[source, pl.ds(1 if first else 0, size)],
            send_sem=gsend.at[0], recv_sem=grecv.at[source], device_id={"tp": source}, device_id_type=MESH,
        )

    def pack_copy(k):
        return pltpu.make_async_remote_copy(
            src_ref=packs.at[tp], dst_ref=packs.at[tp], send_sem=psend.at[k], recv_sem=precv.at[tp],
            device_id={"tp": team(k)}, device_id_type=MESH,
        )

    def halo(source):
        return pltpu.make_async_remote_copy(
            src_ref=gated.at[gated.shape[0] - 1], dst_ref=grown.at[source, 0],
            send_sem=hsend.at[0], recv_sem=hrecv.at[source],
            device_id={"sp": lax.rem(sp + 1, steps), "tp": 0}, device_id_type=MESH,
        )

    def table_copy(k):
        return pltpu.make_async_remote_copy(
            src_ref=tables.at[column(k)  // 2], dst_ref=meta_land(k), send_sem=tsend.at[k], recv_sem=trecv.at[k],
            device_id={"sp": column(k)}, device_id_type=MESH,
        )

    def meta_land(k):
        return tables.at[PLANES + k]

    for k in (2, 1, 3):
        pack_copy(k).start()
        for test, copy in ((team(k) == 0, short), (team(k) > 0, whole)):

            @pl.when(test)
            def _():
                copy(team(k), k).start()

    @pl.when(sp < steps - 1)
    def _():
        halo(tp).start()

    for k in range(1, PLANES):
        table_copy(k).start()

    plane_mates = [{"tp": team(k)} for k in range(1, teams)] + [{"sp": other, "tp": k} for k in range(teams)]
    rounds = [
        [(to, i) for i, to in enumerate(plane_mates)],
        [({"grp": part_of(k)}, k) for k in range(1, parts)],
        [({"sp": column(k)}, k) for k in range(1, PLANES)],
    ]

    def flag_copies(stage):
        base = (0, 16, 16 + parts)[stage]
        return [
            pltpu.make_async_remote_copy(
                src_ref=flags.at[stage], dst_ref=heard.at[land(stage, base, i)], send_sem=csend.at[base + i],
                recv_sem=crecv.at[land(stage, base, i)], device_id=to, device_id_type=MESH,
            )
            for to, i in rounds[stage]
        ]

    def land(stage, base, i):
        if stage == 0 and i >= teams - 1:
            return base + teams - 1 + tp
        return base + i

    def hear(stage):
        base = (0, 16, 16 + parts)[stage]
        seen = flags[stage]
        for (to, i) in rounds[stage]:
            pltpu.make_async_remote_copy(
                src_ref=flags.at[stage], dst_ref=heard.at[base + i], send_sem=csend.at[base + i],
                recv_sem=crecv.at[base + i], device_id=to, device_id_type=MESH,
            ).wait_recv()
            seen = jnp.maximum(seen, heard[base + i])
        flags[stage + 1] = seen
        if stage < 2:
            for copy in flag_copies(stage + 1):
                copy.start()

    for copy in flag_copies(0):
        copy.start()

    for test, size in ((tp == 0, 0), (tp > 0, 1)):

        @pl.when(test)
        def _():
            low = jnp.maximum(tp * pieces - 1, 0) if size else 0
            grown[tp, 1 - size : pieces + 1] = gated[pl.ds(low, pieces + size)]

    def wait_part(k):
        source = team(k)
        if k:
            for test, first in ((tp == 0, True), (tp > 0, False)):

                @pl.when(test)
                def _():
                    got(source, first).wait_recv()

            pltpu.make_async_remote_copy(
                src_ref=packs.at[tp], dst_ref=packs.at[source], send_sem=psend.at[k], recv_sem=precv.at[source],
                device_id={"tp": source}, device_id_type=MESH,
            ).wait_recv()

        @pl.when((tp == 0) & (sp > 0))
        def _():
            halo(source).wait_recv()

    reach = taps_ref.shape[0] - 1
    shift0 = UNIT - reach
    for k in (0, 1, 3, 2):
        wait_part(k)
        if k in (1, 2):
            hear(0 if k == 1 else 1)
        source = team(k)
        for half in range(channels // 128):
            lanes = pl.ds(half * 128, 128)
            x = grown[source, :, :, lanes].reshape((pieces + 1) * UNIT, 128).astype(F32)
            total = jnp.broadcast_to(packs[source, 32:33, lanes], (rows, 128))
            for r in range(8):
                span = rows if r == 0 else rows + 8
                acc = None
                for q in range(0, (UNIT - r) // 8 + 1):
                    tap = 8 * q + r - shift0
                    if not 0 <= tap <= reach:
                        continue
                    term = x[8 * q : 8 * q + span] * packs[source, tap : tap + 1, lanes]
                    acc = term if acc is None else acc + term
                total = total + (acc if r == 0 else acc[r : r + rows])
            conv[source, :, lanes] = total

    full = channels * teams
    pieces_of = [conv[s] for s in range(teams)]
    average = sum(jnp.sum(p, axis=1, keepdims=True) for p in pieces_of) / full
    spread = sum(jnp.sum(p * p, axis=1, keepdims=True) for p in pieces_of) / full - average * average
    scale = lax.rsqrt(spread + EPSILON)
    energy = jnp.zeros((rows, 1), F32)
    for s in range(teams):
        v = jax.nn.silu((conv[s] - average) * scale * packs[s, 33:34] + packs[s, 34:35])
        conv[s] = v
        energy = energy + jnp.sum(v * v, axis=1, keepdims=True)
    scale = lax.rsqrt(energy / full + EPSILON)
    branch = jnp.concatenate([(conv[s] * scale * packs[s, 35:36]).astype(BF16) for s in range(teams)], axis=1)
    for copy in late:
        copy.wait()
    projected = jnp.dot(branch, weight[...], preferred_element_type=F32)
    hidden = (residual[...].astype(F32) + projected).astype(BF16)
    hidden_ref[...] = hidden
    wide = hidden.astype(F32)
    scale = lax.rsqrt(jnp.mean(wide * wide, axis=1, keepdims=True) + EPSILON)
    normed_ref[...] = (wide * scale * gain_ref[...]).astype(BF16)

    meta_ref[zed] = tables[zed]
    for k in range(1, PLANES):
        table_copy(k).wait_recv()
        meta_ref[lax.rem(zed + PLANES - k, PLANES)] = tables[PLANES + k]

    hear(2)
    crowd_ref[0] = jnp.max(flags[3]).astype(jnp.int32)
    for stage in range(3):
        for copy in flag_copies(stage):
            copy.wait_send()

    for k in range(1, teams):
        pack_copy(k).wait_send()
        for test, copy in ((team(k) == 0, short), (team(k) > 0, whole)):

            @pl.when(test)
            def _():
                copy(team(k), k).wait_send()

    @pl.when(sp < steps - 1)
    def _():
        halo(tp).wait_send()

    for k in range(1, PLANES):
        table_copy(k).wait_send()


def front_kernel(value, gate, taps, vectors, moe_gain, ids, loads, out_weight, residual):
    rows, width = residual.shape
    tok_rows, channels = value.shape
    teams = lax.axis_size("tp")
    vmem = pl.BlockSpec(memory_space=pltpu.VMEM)
    far = pl.BlockSpec(memory_space=pltpu.HBM)
    dma = pltpu.SemaphoreType.DMA
    voices = 16 + lax.axis_size("grp") + PLANES
    return pl.pallas_call(
        front_body,
        out_shape=(
            jax.ShapeDtypeStruct((rows, width), BF16),
            jax.ShapeDtypeStruct((rows, width), BF16),
            jax.ShapeDtypeStruct((PLANES, 8, 128), F32),
            jax.ShapeDtypeStruct((1,), jnp.int32),
        ),
        in_specs=[far] * 12,
        out_specs=[vmem] * 3 + [pl.BlockSpec(memory_space=pltpu.SMEM)],
        scratch_shapes=[
            pltpu.VMEM(value.shape, BF16),
            pltpu.VMEM(value.shape, BF16),
            pltpu.VMEM(taps.shape, BF16),
            pltpu.VMEM((4, 1, channels), F32),
            pltpu.VMEM(moe_gain.shape, F32),
            pltpu.VMEM(ids.shape, jnp.int32),
            pltpu.VMEM(loads.shape, F32),
            pltpu.VMEM(out_weight.shape, BF16),
            pltpu.VMEM((rows, width), BF16),
            pltpu.VMEM((tok_rows // UNIT, UNIT, channels), BF16),
            pltpu.VMEM((teams, rows // UNIT + 1, UNIT, channels), BF16),
            pltpu.VMEM((teams, 40, channels), F32),
            pltpu.VMEM((teams, rows, channels), F32),
            pltpu.VMEM((2 * PLANES, 8, 128), F32),
            pltpu.VMEM((4, 8, 128), F32),
            pltpu.VMEM((voices, 8, 128), F32),
            dma((12,)), dma((voices,)), dma((voices,)),
            dma((teams,)), dma((teams,)), dma((1,)), dma((teams,)), dma((teams,)), dma((teams,)),
            dma((PLANES,)), dma((PLANES,)),
        ],
        compiler_params=pltpu.CompilerParams(
            collective_id=2, has_side_effects=True, vmem_limit_bytes=60 << 20
        ),
    )(value, gate, taps, *vectors, moe_gain, ids, loads, out_weight, residual)


def per_device(
    conv_value,
    conv_gate,
    kernel,
    conv_bias,
    ln_gain,
    ln_bias,
    out_gain,
    out_weight,
    residual,
    moe_gain,
    expert_ids,
    expert_weights,
    w_gate,
    w_up,
    w_down,
):
    ids = expert_ids.T
    vectors = [v[None] for v in (conv_bias, ln_gain, ln_bias, out_gain)]
    hidden, normed, meta, crowd = front_kernel(
        conv_value, conv_gate, kernel, vectors, moe_gain[None], ids, expert_weights.T, out_weight, residual
    )
    added = lax.cond(
        crowd[0] > 0,
        functools.partial(experts_kernel, WIDE),
        functools.partial(experts_kernel, NARROW),
        normed, ids, meta, w_gate, w_up, w_down,
    )
    return (hidden.astype(F32) + added).astype(BF16)


def solution(mesh):
    in_specs = (
        P(("grp", "sp"), "tp"),
        P(("grp", "sp"), "tp"),
        P(None, "tp"),
        P("tp"),
        P("tp"),
        P("tp"),
        P("tp"),
        P(),
        P(("grp", "sp", "tp"), None),
        P(),
        P(("grp", "sp", "tp"), None),
        P(("grp", "sp", "tp"), None),
        P(("sp", "tp"), None, None),
        P(("sp", "tp"), None, None),
        P(("sp", "tp"), None, None),
    )
    out_specs = P(("grp", "sp", "tp"), None)
    return jax.shard_map(
        per_device, mesh=mesh, in_specs=in_specs, out_specs=out_specs, check_vma=False
    )
```

```python
import functools

import jax
import jax.numpy as jnp
from jax import lax
from jax.experimental import pallas as pl
from jax.experimental.pallas import tpu as pltpu
from jax.sharding import PartitionSpec as P

EPSILON = 1e-06
MESH = pl.DeviceIdType.MESH
F32 = jnp.float32
BF16 = jnp.bfloat16

SPAN = 4
PLANES = 16
GROUPS = 4
HOPS = 9
SEATS = 8
UNIT = 32
NARROW, WIDE = 48, 64
BLOCKS = 3 + 2 * (HOPS - 1)
BATCHES = 8
FAR = (
    ((1, 7), (0, 7), (0, 7), (0, 7)),
    ((1, 8), (1, 7), (1, 7), (0, 8)),
    ((1, 9), (1, 8), (0, 8), (0, 9)),
)
ORDER = (
    ("r", 1), ("s", 0), ("r", 2), ("s", 1), ("e", 0), ("r", 3), ("s", 2), ("e", 1),
    ("r", 4), ("s", 3), ("e", 2), ("r", 5), ("s", 4), ("e", 3), ("c", 2), ("r", 6),
    ("s", 5), ("e", 4), ("r", 7), ("c", 3), ("e", 5), ("w", 0, 4), ("r", 8), ("s", 6),
    ("c", 4), ("w", 0, 5), ("w", 0, 3), ("r", 9), ("s", 7), ("w", 1, 4), ("c", 5), ("e", 6),
    ("w", 0, 6), ("w", 1, 5), ("e", 7), ("c", 1), ("w", 0, 2), ("w", 2, 4), ("w", 1, 6), ("c", 6),
    ("w", 1, 3), ("w", 2, 6), ("c", 7), ("w", 2, 5), ("w", 0, 9), ("w", 0, 8), ("w", 1, 9), ("w", 1, 8),
    ("c", 0), ("w", 0, 7), ("w", 3, 6), ("w", 2, 9), ("w", 3, 5), ("w", 1, 7), ("w", 1, 2), ("w", 2, 8),
    ("w", 2, 7), ("w", 4, 6), ("w", 3, 9), ("w", 3, 8), ("w", 2, 3), ("w", 4, 9), ("w", 3, 7), ("w", 5, 9),
    ("w", 4, 8), ("w", 5, 8), ("w", 6, 9), ("w", 3, 4), ("w", 4, 7), ("w", 0, 1), ("w", 4, 5), ("w", 6, 8),
    ("w", 5, 7), ("w", 7, 9), ("w", 5, 6), ("w", 7, 8), ("w", 8, 9), ("w", 6, 7),
)


def first_block(hop):
    return 0 if hop == 1 else 3 + 2 * (hop - 2)


def kinds_at(hop):
    found = []
    for rel in (2, 1, 0):
        if rel == 2 and hop > 1:
            continue
        if any(static_valid(on, hop, rel) for on in range(SPAN)):
            found.append(rel)
    return found


def static_valid(on, hop, rel):
    start = (on - hop) % SPAN
    kind = (start + hop) // SPAN + rel
    return kind <= 1 or (kind == 2 and start >= 2)


def real(wave, end):
    hop, rel = end - wave, wave // SPAN
    return (rel < 2 or hop == 1) and static_valid(SPAN - 1 - wave % SPAN, hop, rel)


def where_part(d, hop, place):
    if hop <= 6:
        return hop - 1, d
    return ((6, 1), (7, 0), (7, 1))[[FAR[i][place] for i in range(3)].index((d, hop))]


def valid(on, hop, rel):
    start = lax.rem(on + 12 - hop, SPAN)
    kind = lax.div(start + hop, SPAN) + rel
    return (kind <= 1) | ((kind == 2) & (start >= 2))


def iota(shape, dim):
    return lax.broadcasted_iota(jnp.int32, shape, dim)


def ranks(col, row):
    size = col.shape[0]
    out = {}
    e1c, e2c = col[:, 0:1], col[:, 1:2]
    e1r, e2r = row[0:1, :], row[1:2, :]
    gc, gr = e1c >> 5, e1r >> 5
    o1c, o2c = (e1c >> 3) & 3, (e2c >> 3) & 3
    o1r, o2r = (e1r >> 3) & 3, (e2r >> 3) & 3
    mxc, mnc = jnp.maximum(o1c, o2c), jnp.minimum(o1c, o2c)
    mxr, mnr = jnp.maximum(o1r, o2r), jnp.minimum(o1r, o2r)
    sub = iota((size, size), 0)
    lane = iota((size, size), 1)
    same = gc == gr
    for name, kc, kr in (("P", 3 - mxc, 3 - mxr), ("M", mnc, mnr)):
        kc = kc * size + iota((size, 1), 0)
        kr = kr * size + iota((1, size), 1)
        out[name + "r"] = jnp.sum((same & (kc < kr)).astype(F32), axis=0, keepdims=True).astype(jnp.int32)
        out[name + "c"] = jnp.sum((same & (kr < kc)).astype(F32), axis=1, keepdims=True).astype(jnp.int32)
    out.update(gc=gc, gr=gr, mxc=mxc, mnc=mnc, sub=sub, lane=lane)
    return out


def route_tables(r, row, cols, meta_ref, zed):
    size = row.shape[1]
    col = cols[:, 0:2].astype(jnp.int32)
    zo, g0 = lax.rem(zed, SPAN), lax.div(zed, SPAN)
    e1c, e2c = col[:, 0:1], col[:, 1:2]
    e1r, e2r = row[0:1, :], row[1:2, :]
    crowd = jnp.where(r["Pr"] >= NARROW, 1.0, 0.0)
    earlier = r["lane"] < r["sub"]
    place = []
    for e in (e1c, e2c):
        hit = ((e == e1r) | (e == e2r)) & earlier
        place.append(jnp.sum(hit.astype(F32), axis=1, keepdims=True).astype(jnp.int32))
    group = r["gc"]
    ahead = group - g0
    ahead = jnp.where(ahead < 0, ahead + GROUPS, ahead)
    far_up = jnp.where(zo >= 2, 1, 0)
    lanes = iota((size, 128), 1)
    for plane in range(PLANES):
        slot_row = jnp.full((1, 128), -1.0, F32)
        weight_row = jnp.zeros((1, 128), F32)
        for k, e in enumerate((e1c, e2c)):
            po = plane % SPAN
            own_up = jnp.where(po >= zo, 1, 0)
            up = jnp.where(ahead == 0, own_up, jnp.where(ahead == 1, 1, jnp.where(ahead == 2, far_up, 0)))
            slot = jnp.where(up == 1, r["Pc"], r["Mc"]).astype(F32)
            lane = jnp.where((e >> 3) == plane, (e & 7) * 8 + place[k], -1)
            hit = lane == lanes
            slot_row = slot_row + jnp.sum(jnp.where(hit, slot + 1.0, 0.0), axis=0, keepdims=True)
            weight_row = weight_row + jnp.sum(jnp.where(hit, cols[:, 2 + k : 3 + k], 0.0), axis=0, keepdims=True)
        meta_ref[plane] = jnp.concatenate([slot_row, weight_row, crowd, jnp.zeros((5, 128), F32)], axis=0)


def columns_of(*rows):
    stack = jnp.concatenate([r.astype(F32) for r in rows], axis=0)
    stack = jnp.concatenate([stack, jnp.zeros((8 - stack.shape[0], stack.shape[1]), F32)], axis=0)
    return jnp.transpose(stack, (1, 0))


def routing(cap, base, r, normed_ref, meta_ref, wg_hbm, wu_hbm, wd_hbm, out_ref, work):
    (wg, wu, wd, active, own, came, back, part, xs, xr, rb, yr,
     wsem, fsend, frecv, bsend, brecv, xsend, xrecv, ysend, yrecv) = work
    tokens = normed_ref.shape[0]
    sp, tp = lax.axis_index("sp"), lax.axis_index("tp")
    zed, core = lax.div(sp, 2), lax.rem(sp, 2)
    zo, g0 = lax.rem(zed, SPAN), lax.div(zed, SPAN)
    seat = core * 4 + tp
    off = (zo, SPAN - 1 - zo)
    last = tuple(jnp.where(o == SPAN - 1, 1, 0) for o in off)
    following = tuple(lax.rem(o + 1, SPAN) for o in off)
    ring_to = ({"sp": lax.rem(zed + 1, PLANES) * 2 + core}, {"sp": lax.rem(zed + PLANES - 1, PLANES) * 2 + core})
    ring_from = (ring_to[1], ring_to[0])

    def seat_device(s):
        return {"sp": zed * 2 + lax.div(s, 4), "tp": lax.rem(s, 4)}

    pieces = (pl.ds(0, UNIT), pl.ds(UNIT, cap - UNIT)) if cap > UNIT else (pl.ds(0, cap),)
    units = range(len(pieces))
    weights = [
        pltpu.make_async_copy(wg_hbm.at[0], wg, wsem.at[0]),
        pltpu.make_async_copy(wu_hbm.at[0], wu, wsem.at[1]),
        pltpu.make_async_copy(wd_hbm.at[0], wd, wsem.at[2]),
    ]
    def prepare():
        for w in weights:
            w.start()
        for d in (0, 1):
            for i in range(3):
                back[d, i] = jnp.zeros(back.shape[2:], BF16)
            if cap > UNIT:

                @pl.when(off[d] == SPAN - 1)
                def _():
                    for hop in range(1, HOPS + 1):
                        came[d, first_block(hop), UNIT:cap] = jnp.zeros((cap - UNIT, came.shape[3]), BF16)

    def pack_own(d, name):
        slot = jnp.where((r[name + "r"] >= base) & (r[name + "r"] < base + cap), r["gr"] * cap + r[name + "r"] - base, -1)
        onehot = jnp.where(iota((GROUPS * cap, tokens), 0) == slot, 1.0, 0.0).astype(BF16)

        @pl.loop(0, own.shape[-1] // 512)
        def _(i):
            cols = pl.ds(pl.multiple_of(i * 512, 512), 512)
            rows = jnp.dot(onehot, normed_ref[:, cols], preferred_element_type=F32).astype(BF16)
            own[d, :, :, cols] = rows.reshape(GROUPS, cap, 512)

    def forward(d, src, hop, index, unit):
        return pltpu.make_async_remote_copy(
            src_ref=src, dst_ref=came.at[d, index, pieces[unit]],
            send_sem=fsend.at[d, index, unit], recv_sem=frecv.at[d, index, unit],
            device_id=ring_to[d], device_id_type=MESH,
        )

    def backward(d, src, index, unit):
        return pltpu.make_async_remote_copy(
            src_ref=src, dst_ref=back.at[d, index, pieces[unit]],
            send_sem=bsend.at[d, index, unit], recv_sem=brecv.at[d, index, unit],
            device_id=ring_from[d], device_id_type=MESH,
        )

    def first_hop(act):
        for rel in kinds_at(1):
            for unit in units:
                for d in (0, 1):
                    kind = rel + last[d]
                    group = lax.rem(g0 + kind, GROUPS) if d == 0 else lax.rem(g0 + GROUPS - kind, GROUPS)
                    fine = valid(following[d], 1, rel)
                    if unit == 1 and rel == 0:
                        fine = fine & (following[d] < SPAN - 1)

                    @pl.when(fine)
                    def _():
                        act(forward(d, own.at[d, group, pieces[unit]], 1, rel, unit), d, rel, unit)

    def arrivals(hop, act):
        for rel in kinds_at(hop):
            for unit in units:
                for d in (0, 1):
                    fine = valid(off[d], hop, rel)
                    if unit == 1 and rel == 0:
                        fine = fine & (off[d] < SPAN - 1)

                    @pl.when(fine)
                    def _():
                        act(d, rel, unit)

    def goes_on(d, hop, rel, unit):
        there = rel - last[d]
        ok = there >= 0
        if unit == 1:
            ok = ok & ((there > 0) | (following[d] < SPAN - 1))
        return ok, first_block(hop + 1) + jnp.maximum(there, 0)

    def relay(hop):
        def act(d, rel, unit):
            index = first_block(hop) + rel
            forward(d, came.at[d, index, pieces[unit]], hop, index, unit).wait_recv()
            if hop < HOPS:
                ok, there = goes_on(d, hop, rel, unit)

                @pl.when(ok)
                def _():
                    forward(d, came.at[d, index, pieces[unit]], hop + 1, there, unit).start()

        arrivals(hop, act)

    def near(b):
        hop = b + 1
        index = jnp.where(b == 0, 0, 2 * b + 1)
        return [(0, index, zed + PLANES - hop), (1, index, zed + hop)]

    def by_place(options):
        out = []
        for values in zip(*[(d, first_block(h), PLANES - h if d == 0 else h) for d, h in options]):
            pick = jnp.int32(values[0])
            for i in range(1, SPAN):
                pick = jnp.where(zo == i, values[i], pick)
            out.append(pick)
        return out[0], out[1], zed + out[2]

    def sources(b):
        if isinstance(b, int) and b >= 6:
            return ([None] if b == 6 else []) + [by_place(FAR[i]) for i in ((0,) if b == 6 else (1, 2))]
        return near(b)

    def selectors(b):
        slots, loads = [], []
        for k, source in enumerate(sources(b)):
            whose = zed if source is None else lax.rem(source[2], PLANES)
            meta = meta_ref[whose]
            if k:
                meta = pltpu.roll(meta, 4 * k, 1)
            slots.append((iota((cap, SEATS * 8), 0) + base).astype(F32) == meta[0:1, 0 : SEATS * 8])
            loads.append(meta[1:2, 0 : SEATS * 8])
        return slots, loads

    def spread(b):
        slots, _ = selectors(b)
        pick = jnp.concatenate([jnp.where(s, 1.0, 0.0) for s in slots], axis=0)
        pick = jnp.transpose(pick, (1, 0)).astype(BF16)
        refs = [own.at[0, g0] if source is None else came.at[source[0], source[1]] for source in sources(b)]

        @pl.loop(0, xs.shape[-1] // 512)
        def _(i):
            cols = pl.ds(pl.multiple_of(i * 512, 512), 512)
            blocks = jnp.concatenate([ref[:, cols] for ref in refs], axis=0)
            rows = jnp.dot(pick, blocks, preferred_element_type=F32).astype(BF16)
            xs[b, :, :, cols] = rows.reshape(SEATS, 8, 512)

        pltpu.make_async_copy(xs.at[b, seat], xr.at[b, seat], xrecv.at[b]).start()
        for k in range(1, SEATS):
            spread_copy(b, k).start()

    def spread_copy(b, k):
        to = lax.rem(seat + k, SEATS)
        return pltpu.make_async_remote_copy(
            src_ref=xs.at[b, to], dst_ref=xr.at[b, seat], send_sem=xsend.at[b, k], recv_sem=xrecv.at[b],
            device_id=seat_device(to), device_id_type=MESH,
        )

    def return_copy(b, k):
        to = lax.rem(seat + k, SEATS)
        return pltpu.make_async_remote_copy(
            src_ref=rb.at[b, to], dst_ref=yr.at[b, seat], send_sem=ysend.at[b, k], recv_sem=yrecv.at[b],
            device_id=seat_device(to), device_id_type=MESH,
        )

    def expert(b):
        pltpu.make_async_copy(xs.at[b], xr.at[b], xrecv.at[b]).wait()
        rows = xr[b].reshape(SEATS * 8, xr.shape[-1])

        @pl.loop(0, wg.shape[1] // 256)
        def _(i):
            cols = pl.ds(pl.multiple_of(i * 256, 256), 256)
            gate = jnp.dot(rows, wg[:, cols], preferred_element_type=F32)
            up = jnp.dot(rows, wu[:, cols], preferred_element_type=F32)
            active[:, cols] = (jax.nn.silu(gate) * up).astype(BF16)

        @pl.loop(0, wd.shape[1] // 512)
        def _(i):
            cols = pl.ds(pl.multiple_of(i * 512, 512), 512)
            result = jnp.dot(active[...], wd[:, cols], preferred_element_type=F32).astype(BF16)
            rb[b, :, :, cols] = result.reshape(SEATS, 8, 512)

        pltpu.make_async_copy(rb.at[b, seat], yr.at[b, seat], yrecv.at[b]).start()
        for k in range(1, SEATS):
            return_copy(b, k).start()

    def combine(b):
        slots, loads = selectors(b)
        pltpu.make_async_copy(rb.at[b], yr.at[b], yrecv.at[b]).wait()
        scale = jnp.concatenate([jnp.where(s, w, 0.0) for s, w in zip(slots, loads)], axis=0)
        high = scale.astype(BF16)
        low = (scale - high.astype(F32)).astype(BF16)

        @pl.loop(0, yr.shape[-1] // 512)
        def _(i):
            cols = pl.ds(pl.multiple_of(i * 512, 512), 512)
            rows = yr[b, :, :, cols].reshape(SEATS * 8, 512)
            total = jnp.dot(high, rows, preferred_element_type=F32) + jnp.dot(low, rows, preferred_element_type=F32)
            part[b, :, :, cols] = total.astype(BF16).reshape(2, cap, 512)

    def item(wave, end):
        hop, rel, place = end - wave, wave // SPAN, SPAN - 1 - wave % SPAN
        for d in (0, 1):

            @pl.when(off[d] == place)
            def _():
                index = first_block(hop) + rel
                for unit in units:
                    if rel:
                        later = first_block(hop + 1) + rel - (place == SPAN - 1)
                        backward(d, back.at[d, later, pieces[unit]], later, unit).wait_recv()
                        backward(d, back.at[d, later, pieces[unit]], index, unit).start()
                    elif unit == 0 or place < SPAN - 1:
                        b, k = where_part(d, hop, place if d == 0 else SPAN - 1 - place)
                        mine = part.at[b, k, pieces[unit]]
                        if place < SPAN - 1 - unit:
                            later = first_block(hop + 1)
                            far = back.at[d, later, pieces[unit]]
                            backward(d, far, later, unit).wait_recv()
                            mine[...] = (mine[...].astype(F32) + far[...].astype(F32)).astype(BF16)
                        backward(d, mine, index, unit).start()

    acts = dict(r=relay, s=spread, e=expert, c=combine, w=item)

    def send_own():
        pack_own(0, "P")
        pack_own(1, "M")
        first_hop(lambda copy, *_: copy.start())

    def trip(pause):
        if cap == NARROW:
            fresh = True
            for name, *where in ORDER:
                if name == "e" and fresh:
                    for w in weights:
                        w.wait()
                    pause()
                    fresh = False
                acts[name](*where)
            return
        for hop in range(1, HOPS + 1):
            relay(hop)
        for w in weights:
            w.wait()
        for act in (spread, expert, combine):

            @pl.loop(0, 6)
            def _(b):
                act(b)

            act(6)
            act(7)
        for hop in range(HOPS, 0, -1):
            for end in range(hop, HOPS + 1):
                if real(end - hop, end):
                    item(end - hop, end)

    def home():
        first_hop(lambda copy, d, rel, unit: backward(d, back.at[d, rel, pieces[unit]], rel, unit).wait_recv())
        group, up_rank, down_rank = r["gc"], r["Pc"], r["Mc"]
        far = jnp.where(zo >= 2, 0, 1)
        far_rank = jnp.where(zo >= 2, up_rank, down_rank)
        plan = [
            ((group == g0) & (r["mxc"] > zo), up_rank, back.at[0, 0]),
            ((group == g0) & (r["mnc"] < zo), down_rank, back.at[1, 0]),
            (group == lax.rem(g0 + 1, GROUPS), up_rank, back.at[0, 1 - last[0]]),
            (group == lax.rem(g0 + GROUPS - 1, GROUPS), down_rank, back.at[1, 1 - last[1]]),
            (group == lax.rem(g0 + 2, GROUPS), far_rank, back.at[far, 2 - jnp.where(zo >= 2, last[0], last[1])]),
            (group == g0, up_rank, part.at[6, 0]),
        ]
        lanes = iota((tokens, len(plan) * cap), 1)
        pick = jnp.zeros(lanes.shape, F32)
        for i, (mask, rank, _) in enumerate(plan):
            pick = pick + jnp.where(jnp.where(mask & (rank >= base) & (rank < base + cap), rank - base + i * cap, -1) == lanes, 1.0, 0.0)
        pick = pick.astype(BF16)

        @pl.loop(0, out_ref.shape[1] // 512)
        def _(i):
            cols = pl.ds(pl.multiple_of(i * 512, 512), 512)
            blocks = jnp.concatenate([ref[:, cols] for _, _, ref in plan], axis=0)
            out_ref[:, cols] = jnp.dot(pick, blocks, preferred_element_type=F32)

    def settle():
        first_hop(lambda copy, *_: copy.wait_send())
        for hop in range(1, HOPS + 1):
            def done(d, rel, unit):
                index = first_block(hop) + rel
                if hop < HOPS:
                    ok, there = goes_on(d, hop, rel, unit)

                    @pl.when(ok)
                    def _():
                        forward(d, came.at[d, index, pieces[unit]], hop + 1, there, unit).wait_send()

                backward(d, back.at[d, index, pieces[unit]], index, unit).wait_send()

            arrivals(hop, done)
        for b in range(BATCHES):
            for k in range(1, SEATS):
                spread_copy(b, k).wait_send()
                return_copy(b, k).wait_send()

    return prepare, send_own, trip, home, settle


def rest_body(normed_hbm, row_hbm, meta_hbm, wg_hbm, wu_hbm, wd_hbm, out_ref, normed_ref, row_ref, meta_ref, isem, *work):
    small = [
        pltpu.make_async_copy(row_hbm, row_ref, isem.at[0]),
        pltpu.make_async_copy(normed_hbm, normed_ref, isem.at[1]),
        pltpu.make_async_copy(meta_hbm, meta_ref, isem.at[2]),
    ]
    for w in small:
        w.start()
    for w in small:
        w.wait()
    row = row_ref[...]
    r = ranks(columns_of(row)[:, 0:2].astype(jnp.int32), row)
    prepare, send_own, trip, home, settle = routing(
        WIDE - NARROW, NARROW, r, normed_ref, meta_ref, wg_hbm, wu_hbm, wd_hbm, out_ref, work
    )
    prepare()
    sp, tp = lax.axis_index("sp"), lax.axis_index("tp")
    zed, core = lax.div(sp, 2), lax.rem(sp, 2)
    teams = lax.axis_size("tp")
    barrier = pltpu.get_barrier_semaphore()
    for step in (1, PLANES - 1):
        to = {"sp": lax.rem(zed + step, PLANES) * 2 + core}
        pl.semaphore_signal(barrier, inc=1, device_id=to, device_id_type=MESH)
    for k in range(1, teams):
        pl.semaphore_signal(barrier, inc=1, device_id={"tp": lax.rem(tp + k, teams)}, device_id_type=MESH)
    for k in range(teams):
        pl.semaphore_signal(barrier, inc=1, device_id={"sp": zed * 2 + 1 - core, "tp": k}, device_id_type=MESH)
    pl.semaphore_wait(barrier, 2 * teams + 1)
    send_own()
    trip(None)
    home()
    settle()


def work_shapes(cap, width, inner):
    seats = pltpu.VMEM((BATCHES, SEATS, 8, width), BF16)
    dma = pltpu.SemaphoreType.DMA
    return [
        pltpu.VMEM((width, inner), BF16),
        pltpu.VMEM((width, inner), BF16),
        pltpu.VMEM((inner, width), BF16),
        pltpu.VMEM((SEATS * 8, inner), BF16),
        pltpu.VMEM((2, GROUPS, cap, width), BF16),
        pltpu.VMEM((2, BLOCKS, cap, width), BF16),
        pltpu.VMEM((2, BLOCKS, cap, width), BF16),
        pltpu.VMEM((BATCHES, 2, cap, width), BF16),
        seats, seats, seats, seats,
        dma((3,)),
        dma((2, BLOCKS, 2)), dma((2, BLOCKS, 2)), dma((2, BLOCKS, 2)), dma((2, BLOCKS, 2)),
        dma((BATCHES, SEATS)), dma((BATCHES,)), dma((BATCHES, SEATS)), dma((BATCHES,)),
    ]


def rest_kernel(normed, ids, meta, w_gate, w_up, w_down):
    rows, width = normed.shape
    return pl.pallas_call(
        rest_body,
        out_shape=jax.ShapeDtypeStruct((rows, width), F32),
        in_specs=[pl.BlockSpec(memory_space=pltpu.HBM)] * 6,
        out_specs=pl.BlockSpec(memory_space=pltpu.VMEM),
        scratch_shapes=[
            pltpu.VMEM((rows, width), BF16),
            pltpu.VMEM(ids.shape, jnp.int32),
            pltpu.VMEM(meta.shape, F32),
            pltpu.SemaphoreType.DMA((3,)),
        ] + work_shapes(WIDE - NARROW, width, w_gate.shape[2]),
        compiler_params=pltpu.CompilerParams(collective_id=1, has_side_effects=True, vmem_limit_bytes=60 << 20),
    )(normed, ids, meta, w_gate, w_up, w_down)


def main_body(
    value_hbm, gate_hbm, taps_hbm, bias_hbm, scale_hbm, shift_hbm, branch_hbm, gain_hbm, row_hbm, load_hbm,
    weight_hbm, residual_hbm, wg_hbm, wu_hbm, wd_hbm,
    hidden_hbm, normed_hbm, meta_hbm, out_ref, crowd_ref,
    hidden_ref, normed_ref, meta_ref, value_ref, gate_ref, taps_ref, vectors, gain_ref, row_ref, load_ref, weight, residual, gated, grown, packs, conv,
    tables, flags, heard,
    lsem, osem, csend, crecv, gsend, grecv, hsend, hrecv, psend, precv, tsend, trecv, *work,
):
    sp, tp = lax.axis_index("sp"), lax.axis_index("tp")
    steps, teams = lax.axis_size("sp"), lax.axis_size("tp")
    zed, core = lax.div(sp, 2), lax.rem(sp, 2)
    rows = hidden_ref.shape[0]
    pieces = rows // UNIT
    channels = value_ref.shape[1]
    parts = lax.axis_size("grp")
    other = zed * 2 + 1 - core
    loads = [
        (row_hbm, row_ref), (load_hbm, load_ref),
        (value_hbm, value_ref), (gate_hbm, gate_ref), (taps_hbm, taps_ref),
        (bias_hbm, vectors.at[0]), (scale_hbm, vectors.at[1]), (shift_hbm, vectors.at[2]), (branch_hbm, vectors.at[3]),
        (residual_hbm, residual), (gain_hbm, gain_ref), (weight_hbm, weight),
    ]
    copies = [pltpu.make_async_copy(a, b, lsem.at[i]) for i, (a, b) in enumerate(loads)]
    for copy in copies:
        copy.start()
    fetch, first, late = copies[:2], copies[2:9], copies[9:]

    def part_of(k):
        return lax.rem(lax.axis_index("grp") + k, parts)

    def team(k):
        return lax.rem(tp + k, teams)

    def column(k):
        return lax.rem(zed + k, PLANES) * 2 + core

    barrier = pltpu.get_barrier_semaphore()
    for k in range(1, teams):
        pl.semaphore_signal(barrier, inc=1, device_id={"tp": team(k)}, device_id_type=MESH)

    @pl.when((sp > 0) & (tp == 0))
    def _():
        for k in range(teams):
            pl.semaphore_signal(barrier, inc=1, device_id={"sp": sp - 1, "tp": k}, device_id_type=MESH)

    for k in range(1, PLANES):
        pl.semaphore_signal(barrier, inc=1, device_id={"sp": column(k)}, device_id_type=MESH)
    for k in range(teams):
        pl.semaphore_signal(barrier, inc=1, device_id={"sp": other, "tp": k}, device_id_type=MESH)
    for k in range(1, parts):
        pl.semaphore_signal(barrier, inc=1, device_id={"grp": part_of(k)}, device_id_type=MESH)

    for copy in fetch + first:
        copy.wait()
    passed = (value_ref[...].astype(F32) * jax.nn.sigmoid(gate_ref[...].astype(F32))).astype(BF16)
    gated[...] = passed.reshape(gated.shape)
    packs[tp, 0 : taps_ref.shape[0]] = taps_ref[...].astype(F32)
    for i in range(4):
        packs[tp, 32 + i : 33 + i] = vectors[i]

    @pl.when((sp == 0) & (tp == 0))
    def _():
        grown[:, 0] = jnp.zeros((teams, UNIT, channels), BF16)

    row = row_ref[...]
    cols = columns_of(row, load_ref[...])
    r = ranks(cols[:, 0:2].astype(jnp.int32), row)
    prepare, send_own, trip, home, settle = routing(
        NARROW, 0, r, normed_ref, meta_ref, wg_hbm, wu_hbm, wd_hbm, out_ref, work
    )
    prepare()
    pl.semaphore_wait(barrier, 2 * teams + PLANES + parts - 3 + jnp.where(sp < steps - 1, 1, 0))

    def whole(to, k):
        return pltpu.make_async_remote_copy(
            src_ref=gated.at[pl.ds(jnp.maximum(to * pieces - 1, 0), pieces + 1)], dst_ref=grown.at[tp],
            send_sem=gsend.at[k], recv_sem=grecv.at[tp], device_id={"tp": to}, device_id_type=MESH,
        )

    def short(to, k):
        return pltpu.make_async_remote_copy(
            src_ref=gated.at[pl.ds(0, pieces)], dst_ref=grown.at[tp, pl.ds(1, pieces)],
            send_sem=gsend.at[k], recv_sem=grecv.at[tp], device_id={"tp": to}, device_id_type=MESH,
        )

    def got(source, first):
        size = pieces if first else pieces + 1
        return pltpu.make_async_remote_copy(
            src_ref=gated.at[pl.ds(0, size)], dst_ref=grown.at[source, pl.ds(1 if first else 0, size)],
            send_sem=gsend.at[0], recv_sem=grecv.at[source], device_id={"tp": source}, device_id_type=MESH,
        )

    def pack_copy(k):
        return pltpu.make_async_remote_copy(
            src_ref=packs.at[tp], dst_ref=packs.at[tp], send_sem=psend.at[k], recv_sem=precv.at[tp],
            device_id={"tp": team(k)}, device_id_type=MESH,
        )

    def halo(source):
        return pltpu.make_async_remote_copy(
            src_ref=gated.at[gated.shape[0] - 1], dst_ref=grown.at[source, 0],
            send_sem=hsend.at[0], recv_sem=hrecv.at[source],
            device_id={"sp": lax.rem(sp + 1, steps), "tp": 0}, device_id_type=MESH,
        )

    def table_copy(k):
        return pltpu.make_async_remote_copy(
            src_ref=tables.at[lax.rem(zed + k, PLANES)], dst_ref=meta_ref.at[zed], send_sem=tsend.at[k],
            recv_sem=trecv.at[k], device_id={"sp": column(k)}, device_id_type=MESH,
        )

    for k in (2, 1, 3):
        pack_copy(k).start()
        for test, copy in ((team(k) == 0, short), (team(k) > 0, whole)):

            @pl.when(test)
            def _():
                copy(team(k), k).start()

    @pl.when(sp < steps - 1)
    def _():
        halo(tp).start()

    mates = [{"tp": team(k)} for k in range(1, teams)] + [{"sp": other, "tp": k} for k in range(teams)]
    peers = [{"grp": part_of(k)} for k in range(1, parts)]

    def flag_copies(stage):
        out = []
        for i, to in enumerate(peers if stage else mates):
            at = i + SEATS * stage
            land = teams - 1 + tp if not stage and i >= teams - 1 else at
            out.append(pltpu.make_async_remote_copy(
                src_ref=flags.at[stage], dst_ref=heard.at[land], send_sem=csend.at[at],
                recv_sem=crecv.at[land], device_id=to, device_id_type=MESH,
            ))
        return out

    def hear(stage):
        seen = flags[stage]
        for i, to in enumerate(peers if stage else mates):
            at = i + SEATS * stage
            pltpu.make_async_remote_copy(
                src_ref=flags.at[stage], dst_ref=heard.at[at], send_sem=csend.at[at],
                recv_sem=crecv.at[at], device_id=to, device_id_type=MESH,
            ).wait_recv()
            seen = jnp.maximum(seen, heard[at])
        flags[stage + 1] = seen

    for test, size in ((tp == 0, 0), (tp > 0, 1)):

        @pl.when(test)
        def _():
            low = jnp.maximum(tp * pieces - 1, 0) if size else 0
            grown[tp, 1 - size : pieces + 1] = gated[pl.ds(low, pieces + size)]

    route_tables(r, row, cols, tables, zed)
    meta_ref[zed] = tables[zed]
    for k in range(1, PLANES):
        table_copy(k).start()

    def wait_part(k):
        source = team(k)
        if k:
            for test, first in ((tp == 0, True), (tp > 0, False)):

                @pl.when(test)
                def _():
                    got(source, first).wait_recv()

            pltpu.make_async_remote_copy(
                src_ref=packs.at[tp], dst_ref=packs.at[source], send_sem=psend.at[k], recv_sem=precv.at[source],
                device_id={"tp": source}, device_id_type=MESH,
            ).wait_recv()

        @pl.when((tp == 0) & (sp > 0))
        def _():
            halo(source).wait_recv()

    reach = taps_ref.shape[0] - 1
    shift0 = UNIT - reach
    for k in (0, 1, 3, 2):
        wait_part(k)
        source = team(k)
        for half in range(channels // 128):
            lanes = pl.ds(half * 128, 128)
            x = grown[source, :, :, lanes].reshape((pieces + 1) * UNIT, 128).astype(F32)
            total = jnp.broadcast_to(packs[source, 32:33, lanes], (rows, 128))
            for r in range(8):
                span = rows if r == 0 else rows + 8
                acc = None
                for q in range(0, (UNIT - r) // 8 + 1):
                    tap = 8 * q + r - shift0
                    if not 0 <= tap <= reach:
                        continue
                    term = x[8 * q : 8 * q + span] * packs[source, tap : tap + 1, lanes]
                    acc = term if acc is None else acc + term
                total = total + (acc if r == 0 else acc[r : r + rows])
            conv[source, :, lanes] = total

    full = channels * teams
    pieces_of = [conv[s] for s in range(teams)]
    average = sum(jnp.sum(p, axis=1, keepdims=True) for p in pieces_of) / full
    spread = sum(jnp.sum(p * p, axis=1, keepdims=True) for p in pieces_of) / full - average * average
    scale = lax.rsqrt(spread + EPSILON)
    energy = jnp.zeros((rows, 1), F32)
    for s in range(teams):
        v = jax.nn.silu((conv[s] - average) * scale * packs[s, 33:34] + packs[s, 34:35])
        conv[s] = v
        energy = energy + jnp.sum(v * v, axis=1, keepdims=True)
    scale = lax.rsqrt(energy / full + EPSILON)
    branch = jnp.concatenate([(conv[s] * scale * packs[s, 35:36]).astype(BF16) for s in range(teams)], axis=1)
    for copy in late:
        copy.wait()
    projected = jnp.dot(branch, weight[...], preferred_element_type=F32)
    hidden = (residual[...].astype(F32) + projected).astype(BF16)
    hidden_ref[...] = hidden
    wide = hidden.astype(F32)
    scale = lax.rsqrt(jnp.mean(wide * wide, axis=1, keepdims=True) + EPSILON)
    normed_ref[...] = (wide * scale * gain_ref[...]).astype(BF16)

    send_own()
    results = [
        pltpu.make_async_copy(hidden_ref, hidden_hbm, osem.at[0]),
        pltpu.make_async_copy(normed_ref, normed_hbm, osem.at[1]),
        pltpu.make_async_copy(meta_ref, meta_hbm, osem.at[2]),
    ]
    for k in range(1, PLANES):
        table_copy(k).wait_recv()
    for copy in results:
        copy.start()
    crowd = meta_ref[0]
    for z in range(1, PLANES):
        crowd = jnp.maximum(crowd, meta_ref[z])
    flags[0] = jnp.broadcast_to(crowd[2:3], crowd.shape)
    for copy in flag_copies(0):
        copy.start()

    def pause():
        hear(0)
        for copy in flag_copies(1):
            copy.start()

    trip(pause)
    hear(1)
    crowd_ref[0] = jnp.max(flags[2]).astype(jnp.int32)
    home()
    settle()
    for copy in results:
        copy.wait()
    for stage in (0, 1):
        for copy in flag_copies(stage):
            copy.wait_send()

    for k in range(1, teams):
        pack_copy(k).wait_send()
        for test, copy in ((team(k) == 0, short), (team(k) > 0, whole)):

            @pl.when(test)
            def _():
                copy(team(k), k).wait_send()

    @pl.when(sp < steps - 1)
    def _():
        halo(tp).wait_send()

    for k in range(1, PLANES):
        table_copy(k).wait_send()


def main_kernel(value, gate, taps, vectors, moe_gain, ids, loads, out_weight, residual, w_gate, w_up, w_down):
    rows, width = residual.shape
    tok_rows, channels = value.shape
    teams = lax.axis_size("tp")
    far = pl.BlockSpec(memory_space=pltpu.HBM)
    dma = pltpu.SemaphoreType.DMA
    voices = SEATS + lax.axis_size("grp")
    return pl.pallas_call(
        main_body,
        out_shape=(
            jax.ShapeDtypeStruct((rows, width), BF16),
            jax.ShapeDtypeStruct((rows, width), BF16),
            jax.ShapeDtypeStruct((PLANES, 8, 128), F32),
            jax.ShapeDtypeStruct((rows, width), F32),
            jax.ShapeDtypeStruct((1,), jnp.int32),
        ),
        in_specs=[far] * 15,
        out_specs=[far] * 3 + [pl.BlockSpec(memory_space=pltpu.VMEM), pl.BlockSpec(memory_space=pltpu.SMEM)],
        scratch_shapes=[
            pltpu.VMEM((rows, width), BF16),
            pltpu.VMEM((rows, width), BF16),
            pltpu.VMEM((PLANES, 8, 128), F32),
            pltpu.VMEM(value.shape, BF16),
            pltpu.VMEM(value.shape, BF16),
            pltpu.VMEM(taps.shape, BF16),
            pltpu.VMEM((4, 1, channels), F32),
            pltpu.VMEM(moe_gain.shape, F32),
            pltpu.VMEM(ids.shape, jnp.int32),
            pltpu.VMEM(loads.shape, F32),
            pltpu.VMEM(out_weight.shape, BF16),
            pltpu.VMEM((rows, width), BF16),
            pltpu.VMEM((tok_rows // UNIT, UNIT, channels), BF16),
            pltpu.VMEM((teams, rows // UNIT + 1, UNIT, channels), BF16),
            pltpu.VMEM((teams, 40, channels), F32),
            pltpu.VMEM((teams, rows, channels), F32),
            pltpu.VMEM((PLANES, 8, 128), F32),
            pltpu.VMEM((3, 8, 128), F32),
            pltpu.VMEM((voices, 8, 128), F32),
            dma((12,)), dma((3,)), dma((voices,)), dma((voices,)),
            dma((teams,)), dma((teams,)), dma((1,)), dma((teams,)), dma((teams,)), dma((teams,)),
            dma((PLANES,)), dma((PLANES,)),
        ] + work_shapes(NARROW, width, w_gate.shape[2]),
        compiler_params=pltpu.CompilerParams(
            collective_id=2, has_side_effects=True, vmem_limit_bytes=60 << 20
        ),
    )(value, gate, taps, *vectors, moe_gain, ids, loads, out_weight, residual, w_gate, w_up, w_down)


def per_device(
    conv_value,
    conv_gate,
    kernel,
    conv_bias,
    ln_gain,
    ln_bias,
    out_gain,
    out_weight,
    residual,
    moe_gain,
    expert_ids,
    expert_weights,
    w_gate,
    w_up,
    w_down,
):
    ids = expert_ids.T
    vectors = [v[None] for v in (conv_bias, ln_gain, ln_bias, out_gain)]
    hidden, normed, meta, added, crowd = main_kernel(
        conv_value, conv_gate, kernel, vectors, moe_gain[None], ids, expert_weights.T, out_weight, residual,
        w_gate, w_up, w_down,
    )
    return lax.cond(
        crowd[0] > 0,
        lambda hidden, added, *rest: (hidden.astype(F32) + added + rest_kernel(*rest)).astype(BF16),
        lambda hidden, added, *_: (hidden.astype(F32) + added).astype(BF16),
        hidden, added, normed, ids, meta, w_gate, w_up, w_down,
    )


def solution(mesh):
    in_specs = (
        P(("grp", "sp"), "tp"),
        P(("grp", "sp"), "tp"),
        P(None, "tp"),
        P("tp"),
        P("tp"),
        P("tp"),
        P("tp"),
        P(),
        P(("grp", "sp", "tp"), None),
        P(),
        P(("grp", "sp", "tp"), None),
        P(("grp", "sp", "tp"), None),
        P(("sp", "tp"), None, None),
        P(("sp", "tp"), None, None),
        P(("sp", "tp"), None, None),
    )
    out_specs = P(("grp", "sp", "tp"), None)
    return jax.shard_map(
        per_device, mesh=mesh, in_specs=in_specs, out_specs=out_specs, check_vma=False
    )
```

```python
import functools

import jax
import jax.numpy as jnp
from jax import lax
from jax.experimental import pallas as pl
from jax.experimental.pallas import tpu as pltpu
from jax.sharding import PartitionSpec as P

EPSILON = 1e-06
MESH = pl.DeviceIdType.MESH
F32 = jnp.float32
BF16 = jnp.bfloat16

SPAN = 4
PLANES = 16
GROUPS = 4
HOPS = 9
SEATS = 8
UNIT = 32
NARROW, WIDE = 48, 64
BLOCKS = 3 + 2 * (HOPS - 1)
BATCHES = 8
FAR = (
    ((1, 7), (0, 7), (0, 7), (0, 7)),
    ((1, 8), (1, 7), (1, 7), (0, 8)),
    ((1, 9), (1, 8), (0, 8), (0, 9)),
)
ORDER = (
    ("r", 1), ("s", 0), ("r", 2), ("s", 1), ("e", 0), ("r", 3), ("s", 2), ("e", 1),
    ("r", 4), ("s", 3), ("e", 2), ("r", 5), ("s", 4), ("e", 3), ("c", 2), ("r", 6),
    ("s", 5), ("e", 4), ("r", 7), ("c", 3), ("e", 5), ("w", 0, 4), ("r", 8), ("s", 6),
    ("c", 4), ("w", 0, 5), ("w", 0, 3), ("r", 9), ("s", 7), ("w", 1, 4), ("c", 5), ("e", 6),
    ("w", 0, 6), ("w", 1, 5), ("e", 7), ("c", 1), ("w", 0, 2), ("w", 2, 4), ("w", 1, 6), ("c", 6),
    ("w", 1, 3), ("w", 2, 6), ("c", 7), ("w", 2, 5), ("w", 0, 9), ("w", 0, 8), ("w", 1, 9), ("w", 1, 8),
    ("c", 0), ("w", 0, 7), ("w", 3, 6), ("w", 2, 9), ("w", 3, 5), ("w", 1, 7), ("w", 1, 2), ("w", 2, 8),
    ("w", 2, 7), ("w", 4, 6), ("w", 3, 9), ("w", 3, 8), ("w", 2, 3), ("w", 4, 9), ("w", 3, 7), ("w", 5, 9),
    ("w", 4, 8), ("w", 5, 8), ("w", 6, 9), ("w", 3, 4), ("w", 4, 7), ("w", 0, 1), ("w", 4, 5), ("w", 6, 8),
    ("w", 5, 7), ("w", 7, 9), ("w", 5, 6), ("w", 7, 8), ("w", 8, 9), ("w", 6, 7),
)


def first_block(hop):
    return 0 if hop == 1 else 3 + 2 * (hop - 2)


def kinds_at(hop):
    found = []
    for rel in (2, 1, 0):
        if rel == 2 and hop > 1:
            continue
        if any(static_valid(on, hop, rel) for on in range(SPAN)):
            found.append(rel)
    return found


def static_valid(on, hop, rel):
    start = (on - hop) % SPAN
    kind = (start + hop) // SPAN + rel
    return kind <= 1 or (kind == 2 and start >= 2)


def real(wave, end):
    hop, rel = end - wave, wave // SPAN
    return (rel < 2 or hop == 1) and static_valid(SPAN - 1 - wave % SPAN, hop, rel)


def where_part(d, hop, place):
    if hop <= 6:
        return hop - 1, d
    return ((6, 1), (7, 0), (7, 1))[[FAR[i][place] for i in range(3)].index((d, hop))]


def valid(on, hop, rel):
    start = lax.rem(on + 12 - hop, SPAN)
    kind = lax.div(start + hop, SPAN) + rel
    return (kind <= 1) | ((kind == 2) & (start >= 2))


def iota(shape, dim):
    return lax.broadcasted_iota(jnp.int32, shape, dim)


def ranks(col, row):
    size = col.shape[0]
    out = {}
    e1c, e2c = col[:, 0:1], col[:, 1:2]
    e1r, e2r = row[0:1, :], row[1:2, :]
    gc, gr = e1c >> 5, e1r >> 5
    o1c, o2c = (e1c >> 3) & 3, (e2c >> 3) & 3
    o1r, o2r = (e1r >> 3) & 3, (e2r >> 3) & 3
    mxc, mnc = jnp.maximum(o1c, o2c), jnp.minimum(o1c, o2c)
    mxr, mnr = jnp.maximum(o1r, o2r), jnp.minimum(o1r, o2r)
    sub = iota((size, size), 0)
    lane = iota((size, size), 1)
    same = gc == gr
    for name, kc, kr in (("P", 3 - mxc, 3 - mxr), ("M", mnc, mnr)):
        kc = kc * size + iota((size, 1), 0)
        kr = kr * size + iota((1, size), 1)
        out[name + "r"] = jnp.sum((same & (kc < kr)).astype(F32), axis=0, keepdims=True).astype(jnp.int32)
        out[name + "c"] = jnp.sum((same & (kr < kc)).astype(F32), axis=1, keepdims=True).astype(jnp.int32)
    out.update(gc=gc, gr=gr, mxc=mxc, mnc=mnc, sub=sub, lane=lane)
    return out


def route_tables(r, row, cols, meta_ref, zed):
    size = row.shape[1]
    col = cols[:, 0:2].astype(jnp.int32)
    zo, g0 = lax.rem(zed, SPAN), lax.div(zed, SPAN)
    e1c, e2c = col[:, 0:1], col[:, 1:2]
    e1r, e2r = row[0:1, :], row[1:2, :]
    crowd = jnp.where(r["Pr"] >= NARROW, 1.0, 0.0)
    earlier = r["lane"] < r["sub"]
    place = []
    for e in (e1c, e2c):
        hit = ((e == e1r) | (e == e2r)) & earlier
        place.append(jnp.sum(hit.astype(F32), axis=1, keepdims=True).astype(jnp.int32))
    group = r["gc"]
    ahead = group - g0
    ahead = jnp.where(ahead < 0, ahead + GROUPS, ahead)
    far_up = jnp.where(zo >= 2, 1, 0)
    lanes = iota((size, 128), 1)
    for plane in range(PLANES):
        slot_row = jnp.full((1, 128), -1.0, F32)
        weight_row = jnp.zeros((1, 128), F32)
        for k, e in enumerate((e1c, e2c)):
            po = plane % SPAN
            own_up = jnp.where(po >= zo, 1, 0)
            up = jnp.where(ahead == 0, own_up, jnp.where(ahead == 1, 1, jnp.where(ahead == 2, far_up, 0)))
            slot = jnp.where(up == 1, r["Pc"], r["Mc"]).astype(F32)
            lane = jnp.where((e >> 3) == plane, (e & 7) * 8 + place[k], -1)
            hit = lane == lanes
            slot_row = slot_row + jnp.sum(jnp.where(hit, slot + 1.0, 0.0), axis=0, keepdims=True)
            weight_row = weight_row + jnp.sum(jnp.where(hit, cols[:, 2 + k : 3 + k], 0.0), axis=0, keepdims=True)
        meta_ref[plane] = jnp.concatenate([slot_row, weight_row, crowd, jnp.zeros((5, 128), F32)], axis=0)


def columns_of(*rows):
    stack = jnp.concatenate([r.astype(F32) for r in rows], axis=0)
    stack = jnp.concatenate([stack, jnp.zeros((8 - stack.shape[0], stack.shape[1]), F32)], axis=0)
    return jnp.transpose(stack, (1, 0))


def routing(cap, base, r, normed_ref, meta_ref, wg_hbm, wu_hbm, wd_hbm, out_ref, work):
    (wg, wu, wd, active, own, came, back, part, xs, xr, rb, yr,
     wsem, fsend, frecv, bsend, brecv, xsend, xrecv, ysend, yrecv) = work
    tokens = normed_ref.shape[0]
    sp, tp = lax.axis_index("sp"), lax.axis_index("tp")
    zed, core = lax.div(sp, 2), lax.rem(sp, 2)
    zo, g0 = lax.rem(zed, SPAN), lax.div(zed, SPAN)
    seat = core * 4 + tp
    off = (zo, SPAN - 1 - zo)
    last = tuple(jnp.where(o == SPAN - 1, 1, 0) for o in off)
    following = tuple(lax.rem(o + 1, SPAN) for o in off)
    ring_to = ({"sp": lax.rem(zed + 1, PLANES) * 2 + core}, {"sp": lax.rem(zed + PLANES - 1, PLANES) * 2 + core})
    ring_from = (ring_to[1], ring_to[0])

    def seat_device(s):
        return {"sp": zed * 2 + lax.div(s, 4), "tp": lax.rem(s, 4)}

    pieces = (pl.ds(0, UNIT), pl.ds(UNIT, cap - UNIT)) if cap > UNIT else (pl.ds(0, cap),)
    units = range(len(pieces))
    weights = [
        pltpu.make_async_copy(wg_hbm.at[0], wg, wsem.at[0]),
        pltpu.make_async_copy(wu_hbm.at[0], wu, wsem.at[1]),
        pltpu.make_async_copy(wd_hbm.at[0], wd, wsem.at[2]),
    ]
    def prepare():
        for w in weights:
            w.start()
        for d in (0, 1):
            for i in range(3):
                back[d, i] = jnp.zeros(back.shape[2:], BF16)
            if cap > UNIT:

                @pl.when(off[d] == SPAN - 1)
                def _():
                    for hop in range(1, HOPS + 1):
                        came[d, first_block(hop), UNIT:cap] = jnp.zeros((cap - UNIT, came.shape[3]), BF16)

    def pack_own(d, name):
        slot = jnp.where((r[name + "r"] >= base) & (r[name + "r"] < base + cap), r["gr"] * cap + r[name + "r"] - base, -1)
        onehot = jnp.where(iota((GROUPS * cap, tokens), 0) == slot, 1.0, 0.0).astype(BF16)

        @pl.loop(0, own.shape[-1] // 512)
        def _(i):
            cols = pl.ds(pl.multiple_of(i * 512, 512), 512)
            rows = jnp.dot(onehot, normed_ref[:, cols], preferred_element_type=F32).astype(BF16)
            own[d, :, :, cols] = rows.reshape(GROUPS, cap, 512)

    def forward(d, src, hop, index, unit):
        return pltpu.make_async_remote_copy(
            src_ref=src, dst_ref=came.at[d, index, pieces[unit]],
            send_sem=fsend.at[d, index, unit], recv_sem=frecv.at[d, index, unit],
            device_id=ring_to[d], device_id_type=MESH,
        )

    def backward(d, src, index, unit):
        return pltpu.make_async_remote_copy(
            src_ref=src, dst_ref=back.at[d, index, pieces[unit]],
            send_sem=bsend.at[d, index, unit], recv_sem=brecv.at[d, index, unit],
            device_id=ring_from[d], device_id_type=MESH,
        )

    def first_hop(act, ways=(0, 1)):
        for rel in kinds_at(1):
            for unit in units:
                for d in ways:
                    kind = rel + last[d]
                    group = lax.rem(g0 + kind, GROUPS) if d == 0 else lax.rem(g0 + GROUPS - kind, GROUPS)
                    fine = valid(following[d], 1, rel)
                    if unit == 1 and rel == 0:
                        fine = fine & (following[d] < SPAN - 1)

                    @pl.when(fine)
                    def _():
                        act(forward(d, own.at[d, group, pieces[unit]], 1, rel, unit), d, rel, unit)

    def arrivals(hop, act):
        for rel in kinds_at(hop):
            for unit in units:
                for d in (0, 1):
                    fine = valid(off[d], hop, rel)
                    if unit == 1 and rel == 0:
                        fine = fine & (off[d] < SPAN - 1)

                    @pl.when(fine)
                    def _():
                        act(d, rel, unit)

    def goes_on(d, hop, rel, unit):
        there = rel - last[d]
        ok = there >= 0
        if unit == 1:
            ok = ok & ((there > 0) | (following[d] < SPAN - 1))
        return ok, first_block(hop + 1) + jnp.maximum(there, 0)

    def relay(hop):
        def act(d, rel, unit):
            index = first_block(hop) + rel
            forward(d, came.at[d, index, pieces[unit]], hop, index, unit).wait_recv()
            if hop < HOPS:
                ok, there = goes_on(d, hop, rel, unit)

                @pl.when(ok)
                def _():
                    forward(d, came.at[d, index, pieces[unit]], hop + 1, there, unit).start()

        arrivals(hop, act)

    def near(b):
        hop = b + 1
        index = jnp.where(b == 0, 0, 2 * b + 1)
        return [(0, index, zed + PLANES - hop), (1, index, zed + hop)]

    def by_place(options):
        out = []
        for values in zip(*[(d, first_block(h), PLANES - h if d == 0 else h) for d, h in options]):
            pick = jnp.int32(values[0])
            for i in range(1, SPAN):
                pick = jnp.where(zo == i, values[i], pick)
            out.append(pick)
        return out[0], out[1], zed + out[2]

    def sources(b):
        if isinstance(b, int) and b >= 6:
            return ([None] if b == 6 else []) + [by_place(FAR[i]) for i in ((0,) if b == 6 else (1, 2))]
        return near(b)

    def selectors(b):
        slots, loads = [], []
        for k, source in enumerate(sources(b)):
            whose = zed if source is None else lax.rem(source[2], PLANES)
            meta = meta_ref[whose]
            if k:
                meta = pltpu.roll(meta, 4 * k, 1)
            slots.append((iota((cap, SEATS * 8), 0) + base).astype(F32) == meta[0:1, 0 : SEATS * 8])
            loads.append(meta[1:2, 0 : SEATS * 8])
        return slots, loads

    def spread(b):
        slots, _ = selectors(b)
        pick = jnp.concatenate([jnp.where(s, 1.0, 0.0) for s in slots], axis=0)
        pick = jnp.transpose(pick, (1, 0)).astype(BF16)
        refs = [own.at[0, g0] if source is None else came.at[source[0], source[1]] for source in sources(b)]

        @pl.loop(0, xs.shape[-1] // 512)
        def _(i):
            cols = pl.ds(pl.multiple_of(i * 512, 512), 512)
            blocks = jnp.concatenate([ref[:, cols] for ref in refs], axis=0)
            rows = jnp.dot(pick, blocks, preferred_element_type=F32).astype(BF16)
            xs[b, :, :, cols] = rows.reshape(SEATS, 8, 512)

        pltpu.make_async_copy(xs.at[b, seat], xr.at[b, seat], xrecv.at[b]).start()
        for k in range(1, SEATS):
            spread_copy(b, k).start()

    def spread_copy(b, k):
        to = lax.rem(seat + k, SEATS)
        return pltpu.make_async_remote_copy(
            src_ref=xs.at[b, to], dst_ref=xr.at[b, seat], send_sem=xsend.at[b, k], recv_sem=xrecv.at[b],
            device_id=seat_device(to), device_id_type=MESH,
        )

    def return_copy(b, k):
        to = lax.rem(seat + k, SEATS)
        return pltpu.make_async_remote_copy(
            src_ref=rb.at[b, to], dst_ref=yr.at[b, seat], send_sem=ysend.at[b, k], recv_sem=yrecv.at[b],
            device_id=seat_device(to), device_id_type=MESH,
        )

    def expert(b):
        pltpu.make_async_copy(xs.at[b], xr.at[b], xrecv.at[b]).wait()
        rows = xr[b].reshape(SEATS * 8, xr.shape[-1])

        @pl.loop(0, wg.shape[1] // 256)
        def _(i):
            cols = pl.ds(pl.multiple_of(i * 256, 256), 256)
            gate = jnp.dot(rows, wg[:, cols], preferred_element_type=F32)
            up = jnp.dot(rows, wu[:, cols], preferred_element_type=F32)
            active[:, cols] = (jax.nn.silu(gate) * up).astype(BF16)

        @pl.loop(0, wd.shape[1] // 512)
        def _(i):
            cols = pl.ds(pl.multiple_of(i * 512, 512), 512)
            result = jnp.dot(active[...], wd[:, cols], preferred_element_type=F32).astype(BF16)
            rb[b, :, :, cols] = result.reshape(SEATS, 8, 512)

        pltpu.make_async_copy(rb.at[b, seat], yr.at[b, seat], yrecv.at[b]).start()
        for k in range(1, SEATS):
            return_copy(b, k).start()

    def combine(b):
        slots, loads = selectors(b)
        pltpu.make_async_copy(rb.at[b], yr.at[b], yrecv.at[b]).wait()
        scale = jnp.concatenate([jnp.where(s, w, 0.0) for s, w in zip(slots, loads)], axis=0)
        high = scale.astype(BF16)
        low = (scale - high.astype(F32)).astype(BF16)

        @pl.loop(0, yr.shape[-1] // 512)
        def _(i):
            cols = pl.ds(pl.multiple_of(i * 512, 512), 512)
            rows = yr[b, :, :, cols].reshape(SEATS * 8, 512)
            total = jnp.dot(high, rows, preferred_element_type=F32) + jnp.dot(low, rows, preferred_element_type=F32)
            part[b, :, :, cols] = total.astype(BF16).reshape(2, cap, 512)

    def item(wave, end):
        hop, rel, place = end - wave, wave // SPAN, SPAN - 1 - wave % SPAN
        for d in (0, 1):

            @pl.when(off[d] == place)
            def _():
                index = first_block(hop) + rel
                for unit in units:
                    if rel:
                        later = first_block(hop + 1) + rel - (place == SPAN - 1)
                        backward(d, back.at[d, later, pieces[unit]], later, unit).wait_recv()
                        backward(d, back.at[d, later, pieces[unit]], index, unit).start()
                    elif unit == 0 or place < SPAN - 1:
                        b, k = where_part(d, hop, place if d == 0 else SPAN - 1 - place)
                        mine = part.at[b, k, pieces[unit]]
                        if place < SPAN - 1 - unit:
                            later = first_block(hop + 1)
                            far = back.at[d, later, pieces[unit]]
                            backward(d, far, later, unit).wait_recv()
                            mine[...] = (mine[...].astype(F32) + far[...].astype(F32)).astype(BF16)
                        backward(d, mine, index, unit).start()

    acts = dict(r=relay, s=spread, e=expert, c=combine, w=item)

    def send_own():
        for d in (0, 1):
            pack_own(d, "PM"[d])
            first_hop(lambda copy, *_: copy.start(), (d,))

    def trip(pause):
        if cap == NARROW:
            fresh = True
            for name, *where in ORDER:
                if name == "e" and fresh:
                    for w in weights:
                        w.wait()
                    pause()
                    fresh = False
                acts[name](*where)
            return
        for hop in range(1, HOPS + 1):
            relay(hop)
        for w in weights:
            w.wait()
        for act in (spread, expert, combine):

            @pl.loop(0, 6)
            def _(b):
                act(b)

            act(6)
            act(7)
        for hop in range(HOPS, 0, -1):
            for end in range(hop, HOPS + 1):
                if real(end - hop, end):
                    item(end - hop, end)

    def home():
        first_hop(lambda copy, d, rel, unit: backward(d, back.at[d, rel, pieces[unit]], rel, unit).wait_recv())
        group, up_rank, down_rank = r["gc"], r["Pc"], r["Mc"]
        far = jnp.where(zo >= 2, 0, 1)
        far_rank = jnp.where(zo >= 2, up_rank, down_rank)
        plan = [
            ((group == g0) & (r["mxc"] > zo), up_rank, back.at[0, 0]),
            ((group == g0) & (r["mnc"] < zo), down_rank, back.at[1, 0]),
            (group == lax.rem(g0 + 1, GROUPS), up_rank, back.at[0, 1 - last[0]]),
            (group == lax.rem(g0 + GROUPS - 1, GROUPS), down_rank, back.at[1, 1 - last[1]]),
            (group == lax.rem(g0 + 2, GROUPS), far_rank, back.at[far, 2 - jnp.where(zo >= 2, last[0], last[1])]),
            (group == g0, up_rank, part.at[6, 0]),
        ]
        lanes = iota((tokens, len(plan) * cap), 1)
        pick = jnp.zeros(lanes.shape, F32)
        for i, (mask, rank, _) in enumerate(plan):
            pick = pick + jnp.where(jnp.where(mask & (rank >= base) & (rank < base + cap), rank - base + i * cap, -1) == lanes, 1.0, 0.0)
        pick = pick.astype(BF16)

        @pl.loop(0, out_ref.shape[1] // 512)
        def _(i):
            cols = pl.ds(pl.multiple_of(i * 512, 512), 512)
            blocks = jnp.concatenate([ref[:, cols] for _, _, ref in plan], axis=0)
            out_ref[:, cols] = jnp.dot(pick, blocks, preferred_element_type=F32)

    def settle():
        first_hop(lambda copy, *_: copy.wait_send())
        for hop in range(1, HOPS + 1):
            def done(d, rel, unit):
                index = first_block(hop) + rel
                if hop < HOPS:
                    ok, there = goes_on(d, hop, rel, unit)

                    @pl.when(ok)
                    def _():
                        forward(d, came.at[d, index, pieces[unit]], hop + 1, there, unit).wait_send()

                backward(d, back.at[d, index, pieces[unit]], index, unit).wait_send()

            arrivals(hop, done)
        for b in range(BATCHES):
            for k in range(1, SEATS):
                spread_copy(b, k).wait_send()
                return_copy(b, k).wait_send()

    return prepare, send_own, trip, home, settle


def rest_body(normed_hbm, row_hbm, meta_hbm, wg_hbm, wu_hbm, wd_hbm, out_ref, normed_ref, row_ref, meta_ref, isem, *work):
    small = [
        pltpu.make_async_copy(row_hbm, row_ref, isem.at[0]),
        pltpu.make_async_copy(normed_hbm, normed_ref, isem.at[1]),
        pltpu.make_async_copy(meta_hbm, meta_ref, isem.at[2]),
    ]
    for w in small:
        w.start()
    for w in small:
        w.wait()
    row = row_ref[...]
    r = ranks(columns_of(row)[:, 0:2].astype(jnp.int32), row)
    prepare, send_own, trip, home, settle = routing(
        WIDE - NARROW, NARROW, r, normed_ref, meta_ref, wg_hbm, wu_hbm, wd_hbm, out_ref, work
    )
    prepare()
    sp, tp = lax.axis_index("sp"), lax.axis_index("tp")
    zed, core = lax.div(sp, 2), lax.rem(sp, 2)
    teams = lax.axis_size("tp")
    barrier = pltpu.get_barrier_semaphore()
    for step in (1, PLANES - 1):
        to = {"sp": lax.rem(zed + step, PLANES) * 2 + core}
        pl.semaphore_signal(barrier, inc=1, device_id=to, device_id_type=MESH)
    for k in range(1, teams):
        pl.semaphore_signal(barrier, inc=1, device_id={"tp": lax.rem(tp + k, teams)}, device_id_type=MESH)
    for k in range(teams):
        pl.semaphore_signal(barrier, inc=1, device_id={"sp": zed * 2 + 1 - core, "tp": k}, device_id_type=MESH)
    pl.semaphore_wait(barrier, 2 * teams + 1)
    send_own()
    trip(None)
    home()
    settle()


def work_shapes(cap, width, inner):
    seats = pltpu.VMEM((BATCHES, SEATS, 8, width), BF16)
    dma = pltpu.SemaphoreType.DMA
    return [
        pltpu.VMEM((width, inner), BF16),
        pltpu.VMEM((width, inner), BF16),
        pltpu.VMEM((inner, width), BF16),
        pltpu.VMEM((SEATS * 8, inner), BF16),
        pltpu.VMEM((2, GROUPS, cap, width), BF16),
        pltpu.VMEM((2, BLOCKS, cap, width), BF16),
        pltpu.VMEM((2, BLOCKS, cap, width), BF16),
        pltpu.VMEM((BATCHES, 2, cap, width), BF16),
        seats, seats, seats, seats,
        dma((3,)),
        dma((2, BLOCKS, 2)), dma((2, BLOCKS, 2)), dma((2, BLOCKS, 2)), dma((2, BLOCKS, 2)),
        dma((BATCHES, SEATS)), dma((BATCHES,)), dma((BATCHES, SEATS)), dma((BATCHES,)),
    ]


def rest_kernel(normed, ids, meta, w_gate, w_up, w_down):
    rows, width = normed.shape
    return pl.pallas_call(
        rest_body,
        out_shape=jax.ShapeDtypeStruct((rows, width), F32),
        in_specs=[pl.BlockSpec(memory_space=pltpu.HBM)] * 6,
        out_specs=pl.BlockSpec(memory_space=pltpu.VMEM),
        scratch_shapes=[
            pltpu.VMEM((rows, width), BF16),
            pltpu.VMEM(ids.shape, jnp.int32),
            pltpu.VMEM(meta.shape, F32),
            pltpu.SemaphoreType.DMA((3,)),
        ] + work_shapes(WIDE - NARROW, width, w_gate.shape[2]),
        compiler_params=pltpu.CompilerParams(collective_id=1, has_side_effects=True, vmem_limit_bytes=60 << 20),
    )(normed, ids, meta, w_gate, w_up, w_down)


def main_body(
    value_hbm, gate_hbm, taps_hbm, bias_hbm, scale_hbm, shift_hbm, branch_hbm, gain_hbm, row_hbm, load_hbm,
    weight_hbm, residual_hbm, wg_hbm, wu_hbm, wd_hbm,
    hidden_hbm, normed_hbm, meta_hbm, out_ref, crowd_ref,
    hidden_ref, normed_ref, meta_ref, value_ref, gate_ref, taps_ref, vectors, gain_ref, row_ref, load_ref, weight, residual, gated, grown, packs, conv,
    tables, flags, heard,
    lsem, osem, csend, crecv, gsend, grecv, hsend, hrecv, psend, precv, tsend, trecv, *work,
):
    sp, tp = lax.axis_index("sp"), lax.axis_index("tp")
    steps, teams = lax.axis_size("sp"), lax.axis_size("tp")
    zed, core = lax.div(sp, 2), lax.rem(sp, 2)
    rows = hidden_ref.shape[0]
    pieces = rows // UNIT
    channels = value_ref.shape[1]
    parts = lax.axis_size("grp")
    other = zed * 2 + 1 - core
    loads = [
        (row_hbm, row_ref), (load_hbm, load_ref),
        (value_hbm, value_ref), (gate_hbm, gate_ref), (taps_hbm, taps_ref),
        (bias_hbm, vectors.at[0]), (scale_hbm, vectors.at[1]), (shift_hbm, vectors.at[2]), (branch_hbm, vectors.at[3]),
        (residual_hbm, residual), (gain_hbm, gain_ref), (weight_hbm, weight),
    ]
    copies = [pltpu.make_async_copy(a, b, lsem.at[i]) for i, (a, b) in enumerate(loads)]
    for copy in copies:
        copy.start()
    fetch, first, late = copies[:2], copies[2:9], copies[9:]

    def part_of(k):
        return lax.rem(lax.axis_index("grp") + k, parts)

    def team(k):
        return lax.rem(tp + k, teams)

    def column(k):
        return lax.rem(zed + k, PLANES) * 2 + core

    barrier = pltpu.get_barrier_semaphore()
    for k in range(1, teams):
        pl.semaphore_signal(barrier, inc=1, device_id={"tp": team(k)}, device_id_type=MESH)

    @pl.when((sp > 0) & (tp == 0))
    def _():
        for k in range(teams):
            pl.semaphore_signal(barrier, inc=1, device_id={"sp": sp - 1, "tp": k}, device_id_type=MESH)

    for k in range(1, PLANES):
        pl.semaphore_signal(barrier, inc=1, device_id={"sp": column(k)}, device_id_type=MESH)
    for k in range(teams):
        pl.semaphore_signal(barrier, inc=1, device_id={"sp": other, "tp": k}, device_id_type=MESH)
    for k in range(1, parts):
        pl.semaphore_signal(barrier, inc=1, device_id={"grp": part_of(k)}, device_id_type=MESH)

    for copy in fetch + first:
        copy.wait()
    passed = (value_ref[...].astype(F32) * jax.nn.sigmoid(gate_ref[...].astype(F32))).astype(BF16)
    gated[...] = passed.reshape(gated.shape)
    packs[tp, 0 : taps_ref.shape[0]] = taps_ref[...].astype(F32)
    for i in range(4):
        packs[tp, 32 + i : 33 + i] = vectors[i]

    @pl.when((sp == 0) & (tp == 0))
    def _():
        grown[:, 0] = jnp.zeros((teams, UNIT, channels), BF16)

    row = row_ref[...]
    cols = columns_of(row, load_ref[...])
    r = ranks(cols[:, 0:2].astype(jnp.int32), row)
    prepare, send_own, trip, home, settle = routing(
        NARROW, 0, r, normed_ref, meta_ref, wg_hbm, wu_hbm, wd_hbm, out_ref, work
    )
    prepare()
    pl.semaphore_wait(barrier, 2 * teams + PLANES + parts - 3 + jnp.where(sp < steps - 1, 1, 0))

    def whole(to, k):
        return pltpu.make_async_remote_copy(
            src_ref=gated.at[pl.ds(jnp.maximum(to * pieces - 1, 0), pieces + 1)], dst_ref=grown.at[tp],
            send_sem=gsend.at[k], recv_sem=grecv.at[tp], device_id={"tp": to}, device_id_type=MESH,
        )

    def short(to, k):
        return pltpu.make_async_remote_copy(
            src_ref=gated.at[pl.ds(0, pieces)], dst_ref=grown.at[tp, pl.ds(1, pieces)],
            send_sem=gsend.at[k], recv_sem=grecv.at[tp], device_id={"tp": to}, device_id_type=MESH,
        )

    def got(source, first):
        size = pieces if first else pieces + 1
        return pltpu.make_async_remote_copy(
            src_ref=gated.at[pl.ds(0, size)], dst_ref=grown.at[source, pl.ds(1 if first else 0, size)],
            send_sem=gsend.at[0], recv_sem=grecv.at[source], device_id={"tp": source}, device_id_type=MESH,
        )

    def pack_copy(k):
        return pltpu.make_async_remote_copy(
            src_ref=packs.at[tp], dst_ref=packs.at[tp], send_sem=psend.at[k], recv_sem=precv.at[tp],
            device_id={"tp": team(k)}, device_id_type=MESH,
        )

    def halo(source):
        return pltpu.make_async_remote_copy(
            src_ref=gated.at[gated.shape[0] - 1], dst_ref=grown.at[source, 0],
            send_sem=hsend.at[0], recv_sem=hrecv.at[source],
            device_id={"sp": lax.rem(sp + 1, steps), "tp": 0}, device_id_type=MESH,
        )

    def table_copy(k):
        return pltpu.make_async_remote_copy(
            src_ref=tables.at[lax.rem(zed + k, PLANES)], dst_ref=meta_ref.at[zed], send_sem=tsend.at[k],
            recv_sem=trecv.at[k], device_id={"sp": column(k)}, device_id_type=MESH,
        )

    for k in (2, 1, 3):
        pack_copy(k).start()
        for test, copy in ((team(k) == 0, short), (team(k) > 0, whole)):

            @pl.when(test)
            def _():
                copy(team(k), k).start()

    @pl.when(sp < steps - 1)
    def _():
        halo(tp).start()

    mates = [{"tp": team(k)} for k in range(1, teams)] + [{"sp": other, "tp": k} for k in range(teams)]
    peers = [{"grp": part_of(k)} for k in range(1, parts)]

    def flag_copies(stage):
        out = []
        for i, to in enumerate(peers if stage else mates):
            at = i + SEATS * stage
            land = teams - 1 + tp if not stage and i >= teams - 1 else at
            out.append(pltpu.make_async_remote_copy(
                src_ref=flags.at[stage], dst_ref=heard.at[land], send_sem=csend.at[at],
                recv_sem=crecv.at[land], device_id=to, device_id_type=MESH,
            ))
        return out

    def hear(stage):
        seen = flags[stage]
        for i, to in enumerate(peers if stage else mates):
            at = i + SEATS * stage
            pltpu.make_async_remote_copy(
                src_ref=flags.at[stage], dst_ref=heard.at[at], send_sem=csend.at[at],
                recv_sem=crecv.at[at], device_id=to, device_id_type=MESH,
            ).wait_recv()
            seen = jnp.maximum(seen, heard[at])
        flags[stage + 1] = seen

    for test, size in ((tp == 0, 0), (tp > 0, 1)):

        @pl.when(test)
        def _():
            low = jnp.maximum(tp * pieces - 1, 0) if size else 0
            grown[tp, 1 - size : pieces + 1] = gated[pl.ds(low, pieces + size)]

    route_tables(r, row, cols, tables, zed)
    meta_ref[zed] = tables[zed]
    for k in range(1, PLANES):
        table_copy(k).start()

    def wait_part(k):
        source = team(k)
        if k:
            for test, first in ((tp == 0, True), (tp > 0, False)):

                @pl.when(test)
                def _():
                    got(source, first).wait_recv()

            pltpu.make_async_remote_copy(
                src_ref=packs.at[tp], dst_ref=packs.at[source], send_sem=psend.at[k], recv_sem=precv.at[source],
                device_id={"tp": source}, device_id_type=MESH,
            ).wait_recv()

        @pl.when((tp == 0) & (sp > 0))
        def _():
            halo(source).wait_recv()

    reach = taps_ref.shape[0] - 1
    shift0 = UNIT - reach
    for k in (0, 1, 3, 2):
        wait_part(k)
        source = team(k)
        for half in range(channels // 128):
            lanes = pl.ds(half * 128, 128)
            x = grown[source, :, :, lanes].reshape((pieces + 1) * UNIT, 128).astype(F32)
            total = jnp.broadcast_to(packs[source, 32:33, lanes], (rows, 128))
            for r in range(8):
                span = rows if r == 0 else rows + 8
                acc = None
                for q in range(0, (UNIT - r) // 8 + 1):
                    tap = 8 * q + r - shift0
                    if not 0 <= tap <= reach:
                        continue
                    term = x[8 * q : 8 * q + span] * packs[source, tap : tap + 1, lanes]
                    acc = term if acc is None else acc + term
                total = total + (acc if r == 0 else acc[r : r + rows])
            conv[source, :, lanes] = total

    full = channels * teams
    pieces_of = [conv[s] for s in range(teams)]
    average = sum(jnp.sum(p, axis=1, keepdims=True) for p in pieces_of) / full
    spread = sum(jnp.sum(p * p, axis=1, keepdims=True) for p in pieces_of) / full - average * average
    scale = lax.rsqrt(spread + EPSILON)
    energy = jnp.zeros((rows, 1), F32)
    for s in range(teams):
        v = jax.nn.silu((conv[s] - average) * scale * packs[s, 33:34] + packs[s, 34:35])
        conv[s] = v
        energy = energy + jnp.sum(v * v, axis=1, keepdims=True)
    scale = lax.rsqrt(energy / full + EPSILON)
    branch = jnp.concatenate([(conv[s] * scale * packs[s, 35:36]).astype(BF16) for s in range(teams)], axis=1)
    for copy in late:
        copy.wait()
    projected = jnp.dot(branch, weight[...], preferred_element_type=F32)
    hidden = (residual[...].astype(F32) + projected).astype(BF16)
    hidden_ref[...] = hidden
    wide = hidden.astype(F32)
    scale = lax.rsqrt(jnp.mean(wide * wide, axis=1, keepdims=True) + EPSILON)
    normed_ref[...] = (wide * scale * gain_ref[...]).astype(BF16)

    send_own()
    results = [
        pltpu.make_async_copy(hidden_ref, hidden_hbm, osem.at[0]),
        pltpu.make_async_copy(normed_ref, normed_hbm, osem.at[1]),
        pltpu.make_async_copy(meta_ref, meta_hbm, osem.at[2]),
    ]
    for k in range(1, PLANES):
        table_copy(k).wait_recv()
    for copy in results:
        copy.start()
    crowd = meta_ref[0]
    for z in range(1, PLANES):
        crowd = jnp.maximum(crowd, meta_ref[z])
    flags[0] = jnp.broadcast_to(crowd[2:3], crowd.shape)
    for copy in flag_copies(0):
        copy.start()

    def pause():
        hear(0)
        for copy in flag_copies(1):
            copy.start()

    trip(pause)
    hear(1)
    crowd_ref[0] = jnp.max(flags[2]).astype(jnp.int32)
    home()
    settle()
    for copy in results:
        copy.wait()
    for stage in (0, 1):
        for copy in flag_copies(stage):
            copy.wait_send()

    for k in range(1, teams):
        pack_copy(k).wait_send()
        for test, copy in ((team(k) == 0, short), (team(k) > 0, whole)):

            @pl.when(test)
            def _():
                copy(team(k), k).wait_send()

    @pl.when(sp < steps - 1)
    def _():
        halo(tp).wait_send()

    for k in range(1, PLANES):
        table_copy(k).wait_send()


def main_kernel(value, gate, taps, vectors, moe_gain, ids, loads, out_weight, residual, w_gate, w_up, w_down):
    rows, width = residual.shape
    tok_rows, channels = value.shape
    teams = lax.axis_size("tp")
    far = pl.BlockSpec(memory_space=pltpu.HBM)
    dma = pltpu.SemaphoreType.DMA
    voices = SEATS + lax.axis_size("grp")
    return pl.pallas_call(
        main_body,
        out_shape=(
            jax.ShapeDtypeStruct((rows, width), BF16),
            jax.ShapeDtypeStruct((rows, width), BF16),
            jax.ShapeDtypeStruct((PLANES, 8, 128), F32),
            jax.ShapeDtypeStruct((rows, width), F32),
            jax.ShapeDtypeStruct((1,), jnp.int32),
        ),
        in_specs=[far] * 15,
        out_specs=[far] * 3 + [pl.BlockSpec(memory_space=pltpu.VMEM), pl.BlockSpec(memory_space=pltpu.SMEM)],
        scratch_shapes=[
            pltpu.VMEM((rows, width), BF16),
            pltpu.VMEM((rows, width), BF16),
            pltpu.VMEM((PLANES, 8, 128), F32),
            pltpu.VMEM(value.shape, BF16),
            pltpu.VMEM(value.shape, BF16),
            pltpu.VMEM(taps.shape, BF16),
            pltpu.VMEM((4, 1, channels), F32),
            pltpu.VMEM(moe_gain.shape, F32),
            pltpu.VMEM(ids.shape, jnp.int32),
            pltpu.VMEM(loads.shape, F32),
            pltpu.VMEM(out_weight.shape, BF16),
            pltpu.VMEM((rows, width), BF16),
            pltpu.VMEM((tok_rows // UNIT, UNIT, channels), BF16),
            pltpu.VMEM((teams, rows // UNIT + 1, UNIT, channels), BF16),
            pltpu.VMEM((teams, 40, channels), F32),
            pltpu.VMEM((teams, rows, channels), F32),
            pltpu.VMEM((PLANES, 8, 128), F32),
            pltpu.VMEM((3, 8, 128), F32),
            pltpu.VMEM((voices, 8, 128), F32),
            dma((12,)), dma((3,)), dma((voices,)), dma((voices,)),
            dma((teams,)), dma((teams,)), dma((1,)), dma((teams,)), dma((teams,)), dma((teams,)),
            dma((PLANES,)), dma((PLANES,)),
        ] + work_shapes(NARROW, width, w_gate.shape[2]),
        compiler_params=pltpu.CompilerParams(
            collective_id=2, has_side_effects=True, vmem_limit_bytes=60 << 20
        ),
    )(value, gate, taps, *vectors, moe_gain, ids, loads, out_weight, residual, w_gate, w_up, w_down)


def per_device(
    conv_value,
    conv_gate,
    kernel,
    conv_bias,
    ln_gain,
    ln_bias,
    out_gain,
    out_weight,
    residual,
    moe_gain,
    expert_ids,
    expert_weights,
    w_gate,
    w_up,
    w_down,
):
    ids = expert_ids.T
    vectors = [v[None] for v in (conv_bias, ln_gain, ln_bias, out_gain)]
    hidden, normed, meta, added, crowd = main_kernel(
        conv_value, conv_gate, kernel, vectors, moe_gain[None], ids, expert_weights.T, out_weight, residual,
        w_gate, w_up, w_down,
    )
    return lax.cond(
        crowd[0] > 0,
        lambda hidden, added, *rest: (hidden.astype(F32) + added + rest_kernel(*rest)).astype(BF16),
        lambda hidden, added, *_: (hidden.astype(F32) + added).astype(BF16),
        hidden, added, normed, ids, meta, w_gate, w_up, w_down,
    )


def solution(mesh):
    assert mesh.shape["sp"] == 2 * PLANES and 2 * mesh.shape["tp"] == SEATS
    in_specs = (
        P(("grp", "sp"), "tp"),
        P(("grp", "sp"), "tp"),
        P(None, "tp"),
        P("tp"),
        P("tp"),
        P("tp"),
        P("tp"),
        P(),
        P(("grp", "sp", "tp"), None),
        P(),
        P(("grp", "sp", "tp"), None),
        P(("grp", "sp", "tp"), None),
        P(("sp", "tp"), None, None),
        P(("sp", "tp"), None, None),
        P(("sp", "tp"), None, None),
    )
    out_specs = P(("grp", "sp", "tp"), None)
    return jax.shard_map(
        per_device, mesh=mesh, in_specs=in_specs, out_specs=out_specs, check_vma=False
    )
```

```python
import functools

import jax
import jax.numpy as jnp
from jax import lax
from jax.experimental import pallas as pl
from jax.experimental.pallas import tpu as pltpu
from jax.sharding import PartitionSpec as P

EPSILON = 1e-06
MESH = pl.DeviceIdType.MESH
F32 = jnp.float32
BF16 = jnp.bfloat16

SPAN = 4
PLANES = 16
GROUPS = 4
HOPS = 9
SEATS = 8
UNIT = 32
NARROW, WIDE = 48, 64
BLOCKS = 3 + 2 * (HOPS - 1)
BATCHES = 8
FAR = (
    ((1, 7), (0, 7), (0, 7), (0, 7)),
    ((1, 8), (1, 7), (1, 7), (0, 8)),
    ((1, 9), (1, 8), (0, 8), (0, 9)),
)
ORDER = (
    ("r", 1), ("s", 0), ("r", 2), ("s", 1), ("e", 0), ("r", 3), ("s", 2), ("e", 1),
    ("r", 4), ("s", 3), ("e", 2), ("r", 5), ("s", 4), ("e", 3), ("c", 2), ("r", 6),
    ("s", 5), ("e", 4), ("r", 7), ("c", 3), ("e", 5), ("w", 0, 4), ("r", 8), ("s", 6),
    ("c", 4), ("w", 0, 5), ("w", 0, 3), ("r", 9), ("s", 7), ("w", 1, 4), ("c", 5), ("e", 6),
    ("w", 0, 6), ("w", 1, 5), ("e", 7), ("c", 1), ("w", 0, 2), ("w", 2, 4), ("w", 1, 6), ("c", 6),
    ("w", 1, 3), ("w", 2, 6), ("c", 7), ("w", 2, 5), ("w", 0, 9), ("w", 0, 8), ("w", 1, 9), ("w", 1, 8),
    ("c", 0), ("w", 0, 7), ("w", 3, 6), ("w", 2, 9), ("w", 3, 5), ("w", 1, 7), ("w", 1, 2), ("w", 2, 8),
    ("w", 2, 7), ("w", 4, 6), ("w", 3, 9), ("w", 3, 8), ("w", 2, 3), ("w", 4, 9), ("w", 3, 7), ("w", 5, 9),
    ("w", 4, 8), ("w", 5, 8), ("w", 6, 9), ("w", 3, 4), ("w", 4, 7), ("w", 0, 1), ("w", 4, 5), ("w", 6, 8),
    ("w", 5, 7), ("w", 7, 9), ("w", 5, 6), ("w", 7, 8), ("w", 8, 9), ("w", 6, 7),
)


def first_block(hop):
    return 0 if hop == 1 else 3 + 2 * (hop - 2)


def kinds_at(hop):
    found = []
    for rel in (2, 1, 0):
        if rel == 2 and hop > 1:
            continue
        if any(static_valid(on, hop, rel) for on in range(SPAN)):
            found.append(rel)
    return found


def static_valid(on, hop, rel):
    start = (on - hop) % SPAN
    kind = (start + hop) // SPAN + rel
    return kind <= 1 or (kind == 2 and start >= 2)


def real(wave, end):
    hop, rel = end - wave, wave // SPAN
    return (rel < 2 or hop == 1) and static_valid(SPAN - 1 - wave % SPAN, hop, rel)


def where_part(d, hop, place):
    if hop <= 6:
        return hop - 1, d
    return ((6, 1), (7, 0), (7, 1))[[FAR[i][place] for i in range(3)].index((d, hop))]


def valid(on, hop, rel):
    start = lax.rem(on + 12 - hop, SPAN)
    kind = lax.div(start + hop, SPAN) + rel
    return (kind <= 1) | ((kind == 2) & (start >= 2))


def iota(shape, dim):
    return lax.broadcasted_iota(jnp.int32, shape, dim)


def ranks(col, row):
    size = col.shape[0]
    out = {}
    e1c, e2c = col[:, 0:1], col[:, 1:2]
    e1r, e2r = row[0:1, :], row[1:2, :]
    gc, gr = e1c >> 5, e1r >> 5
    o1c, o2c = (e1c >> 3) & 3, (e2c >> 3) & 3
    o1r, o2r = (e1r >> 3) & 3, (e2r >> 3) & 3
    mxc, mnc = jnp.maximum(o1c, o2c), jnp.minimum(o1c, o2c)
    mxr, mnr = jnp.maximum(o1r, o2r), jnp.minimum(o1r, o2r)
    sub = iota((size, size), 0)
    lane = iota((size, size), 1)
    same = gc == gr
    for name, kc, kr in (("P", 3 - mxc, 3 - mxr), ("M", mnc, mnr)):
        kc = kc * size + iota((size, 1), 0)
        kr = kr * size + iota((1, size), 1)
        out[name + "r"] = jnp.sum((same & (kc < kr)).astype(F32), axis=0, keepdims=True).astype(jnp.int32)
        out[name + "c"] = jnp.sum((same & (kr < kc)).astype(F32), axis=1, keepdims=True).astype(jnp.int32)
    out.update(gc=gc, gr=gr, mxc=mxc, mnc=mnc, sub=sub, lane=lane)
    return out


def route_tables(r, row, cols, meta_ref, zed):
    size = row.shape[1]
    col = cols[:, 0:2].astype(jnp.int32)
    zo, g0 = lax.rem(zed, SPAN), lax.div(zed, SPAN)
    e1c, e2c = col[:, 0:1], col[:, 1:2]
    e1r, e2r = row[0:1, :], row[1:2, :]
    crowd = jnp.where(r["Pr"] >= NARROW, 1.0, 0.0)
    earlier = r["lane"] < r["sub"]
    place = []
    for e in (e1c, e2c):
        hit = ((e == e1r) | (e == e2r)) & earlier
        place.append(jnp.sum(hit.astype(F32), axis=1, keepdims=True).astype(jnp.int32))
    group = r["gc"]
    ahead = group - g0
    ahead = jnp.where(ahead < 0, ahead + GROUPS, ahead)
    far_up = jnp.where(zo >= 2, 1, 0)
    lanes = iota((size, 128), 1)
    for plane in range(PLANES):
        slot_row = jnp.full((1, 128), -1.0, F32)
        weight_row = jnp.zeros((1, 128), F32)
        for k, e in enumerate((e1c, e2c)):
            po = plane % SPAN
            own_up = jnp.where(po >= zo, 1, 0)
            up = jnp.where(ahead == 0, own_up, jnp.where(ahead == 1, 1, jnp.where(ahead == 2, far_up, 0)))
            slot = jnp.where(up == 1, r["Pc"], r["Mc"]).astype(F32)
            lane = jnp.where((e >> 3) == plane, (e & 7) * 8 + place[k], -1)
            hit = lane == lanes
            slot_row = slot_row + jnp.sum(jnp.where(hit, slot + 1.0, 0.0), axis=0, keepdims=True)
            weight_row = weight_row + jnp.sum(jnp.where(hit, cols[:, 2 + k : 3 + k], 0.0), axis=0, keepdims=True)
        meta_ref[plane] = jnp.concatenate([slot_row, weight_row, crowd, jnp.zeros((5, 128), F32)], axis=0)


def columns_of(*rows):
    stack = jnp.concatenate([r.astype(F32) for r in rows], axis=0)
    stack = jnp.concatenate([stack, jnp.zeros((8 - stack.shape[0], stack.shape[1]), F32)], axis=0)
    return jnp.transpose(stack, (1, 0))


def routing(cap, base, r, normed_ref, meta_ref, wg_hbm, wu_hbm, wd_hbm, out_ref, work):
    (wg, wu, wd, active, own, came, back, part, xs, xr, rb, yr,
     wsem, fsend, frecv, bsend, brecv, xsend, xrecv, ysend, yrecv) = work
    tokens = normed_ref.shape[0]
    sp, tp = lax.axis_index("sp"), lax.axis_index("tp")
    zed, core = lax.div(sp, 2), lax.rem(sp, 2)
    zo, g0 = lax.rem(zed, SPAN), lax.div(zed, SPAN)
    seat = core * 4 + tp
    off = (zo, SPAN - 1 - zo)
    last = tuple(jnp.where(o == SPAN - 1, 1, 0) for o in off)
    following = tuple(lax.rem(o + 1, SPAN) for o in off)
    ring_to = ({"sp": lax.rem(zed + 1, PLANES) * 2 + core}, {"sp": lax.rem(zed + PLANES - 1, PLANES) * 2 + core})
    ring_from = (ring_to[1], ring_to[0])

    def seat_device(s):
        return {"sp": zed * 2 + lax.div(s, 4), "tp": lax.rem(s, 4)}

    pieces = (pl.ds(0, UNIT), pl.ds(UNIT, cap - UNIT)) if cap > UNIT else (pl.ds(0, cap),)
    units = range(len(pieces))
    weights = [
        pltpu.make_async_copy(wg_hbm.at[0], wg, wsem.at[0]),
        pltpu.make_async_copy(wu_hbm.at[0], wu, wsem.at[1]),
        pltpu.make_async_copy(wd_hbm.at[0], wd, wsem.at[2]),
    ]
    def prepare():
        for w in weights:
            w.start()
        for d in (0, 1):
            for i in range(3):
                back[d, i] = jnp.zeros(back.shape[2:], BF16)
            if cap > UNIT:

                @pl.when(off[d] == SPAN - 1)
                def _():
                    for hop in range(1, HOPS + 1):
                        came[d, first_block(hop), UNIT:cap] = jnp.zeros((cap - UNIT, came.shape[3]), BF16)

    def pack_own(d, name):
        slot = jnp.where((r[name + "r"] >= base) & (r[name + "r"] < base + cap), r["gr"] * cap + r[name + "r"] - base, -1)
        onehot = jnp.where(iota((GROUPS * cap, tokens), 0) == slot, 1.0, 0.0).astype(BF16)

        @pl.loop(0, own.shape[-1] // 512)
        def _(i):
            cols = pl.ds(pl.multiple_of(i * 512, 512), 512)
            rows = jnp.dot(onehot, normed_ref[:, cols], preferred_element_type=F32).astype(BF16)
            own[d, :, :, cols] = rows.reshape(GROUPS, cap, 512)

    def forward(d, src, hop, index, unit):
        return pltpu.make_async_remote_copy(
            src_ref=src, dst_ref=came.at[d, index, pieces[unit]],
            send_sem=fsend.at[d, index, unit], recv_sem=frecv.at[d, index, unit],
            device_id=ring_to[d], device_id_type=MESH,
        )

    def backward(d, src, index, unit):
        return pltpu.make_async_remote_copy(
            src_ref=src, dst_ref=back.at[d, index, pieces[unit]],
            send_sem=bsend.at[d, index, unit], recv_sem=brecv.at[d, index, unit],
            device_id=ring_from[d], device_id_type=MESH,
        )

    def first_hop(act, ways=(0, 1)):
        for rel in kinds_at(1):
            for unit in units:
                for d in ways:
                    kind = rel + last[d]
                    group = lax.rem(g0 + kind, GROUPS) if d == 0 else lax.rem(g0 + GROUPS - kind, GROUPS)
                    fine = valid(following[d], 1, rel)
                    if unit == 1 and rel == 0:
                        fine = fine & (following[d] < SPAN - 1)

                    @pl.when(fine)
                    def _():
                        act(forward(d, own.at[d, group, pieces[unit]], 1, rel, unit), d, rel, unit)

    def arrivals(hop, act):
        for rel in kinds_at(hop):
            for unit in units:
                for d in (0, 1):
                    fine = valid(off[d], hop, rel)
                    if unit == 1 and rel == 0:
                        fine = fine & (off[d] < SPAN - 1)

                    @pl.when(fine)
                    def _():
                        act(d, rel, unit)

    def goes_on(d, hop, rel, unit):
        there = rel - last[d]
        ok = there >= 0
        if unit == 1:
            ok = ok & ((there > 0) | (following[d] < SPAN - 1))
        return ok, first_block(hop + 1) + jnp.maximum(there, 0)

    def relay(hop):
        def act(d, rel, unit):
            index = first_block(hop) + rel
            forward(d, came.at[d, index, pieces[unit]], hop, index, unit).wait_recv()
            if hop < HOPS:
                ok, there = goes_on(d, hop, rel, unit)

                @pl.when(ok)
                def _():
                    forward(d, came.at[d, index, pieces[unit]], hop + 1, there, unit).start()

        arrivals(hop, act)

    def near(b):
        hop = b + 1
        index = jnp.where(b == 0, 0, 2 * b + 1)
        return [(0, index, zed + PLANES - hop), (1, index, zed + hop)]

    def by_place(options):
        out = []
        for values in zip(*[(d, first_block(h), PLANES - h if d == 0 else h) for d, h in options]):
            pick = jnp.int32(values[0])
            for i in range(1, SPAN):
                pick = jnp.where(zo == i, values[i], pick)
            out.append(pick)
        return out[0], out[1], zed + out[2]

    def sources(b):
        if isinstance(b, int) and b >= 6:
            return ([None] if b == 6 else []) + [by_place(FAR[i]) for i in ((0,) if b == 6 else (1, 2))]
        return near(b)

    def selectors(b):
        slots, loads = [], []
        for k, source in enumerate(sources(b)):
            whose = zed if source is None else lax.rem(source[2], PLANES)
            meta = meta_ref[whose]
            if k:
                meta = pltpu.roll(meta, 4 * k, 1)
            slots.append((iota((cap, SEATS * 8), 0) + base).astype(F32) == meta[0:1, 0 : SEATS * 8])
            loads.append(meta[1:2, 0 : SEATS * 8])
        return slots, loads

    def spread(b):
        slots, _ = selectors(b)
        pick = jnp.concatenate([jnp.where(s, 1.0, 0.0) for s in slots], axis=0)
        pick = jnp.transpose(pick, (1, 0)).astype(BF16)
        refs = [own.at[0, g0] if source is None else came.at[source[0], source[1]] for source in sources(b)]

        @pl.loop(0, xs.shape[-1] // 512)
        def _(i):
            cols = pl.ds(pl.multiple_of(i * 512, 512), 512)
            blocks = jnp.concatenate([ref[:, cols] for ref in refs], axis=0)
            rows = jnp.dot(pick, blocks, preferred_element_type=F32).astype(BF16)
            xs[b, :, :, cols] = rows.reshape(SEATS, 8, 512)

        pltpu.make_async_copy(xs.at[b, seat], xr.at[b, seat], xrecv.at[b]).start()
        for k in range(1, SEATS):
            spread_copy(b, k).start()

    def spread_copy(b, k):
        to = lax.rem(seat + k, SEATS)
        return pltpu.make_async_remote_copy(
            src_ref=xs.at[b, to], dst_ref=xr.at[b, seat], send_sem=xsend.at[b, k], recv_sem=xrecv.at[b],
            device_id=seat_device(to), device_id_type=MESH,
        )

    def return_copy(b, k):
        to = lax.rem(seat + k, SEATS)
        return pltpu.make_async_remote_copy(
            src_ref=rb.at[b, to], dst_ref=yr.at[b, seat], send_sem=ysend.at[b, k], recv_sem=yrecv.at[b],
            device_id=seat_device(to), device_id_type=MESH,
        )

    def expert(b):
        pltpu.make_async_copy(xs.at[b], xr.at[b], xrecv.at[b]).wait()
        rows = xr[b].reshape(SEATS * 8, xr.shape[-1])

        @pl.loop(0, wg.shape[1] // 256)
        def _(i):
            cols = pl.ds(pl.multiple_of(i * 256, 256), 256)
            gate = jnp.dot(rows, wg[:, cols], preferred_element_type=F32)
            up = jnp.dot(rows, wu[:, cols], preferred_element_type=F32)
            active[:, cols] = (jax.nn.silu(gate) * up).astype(BF16)

        @pl.loop(0, wd.shape[1] // 512)
        def _(i):
            cols = pl.ds(pl.multiple_of(i * 512, 512), 512)
            result = jnp.dot(active[...], wd[:, cols], preferred_element_type=F32).astype(BF16)
            rb[b, :, :, cols] = result.reshape(SEATS, 8, 512)

        pltpu.make_async_copy(rb.at[b, seat], yr.at[b, seat], yrecv.at[b]).start()
        for k in range(1, SEATS):
            return_copy(b, k).start()

    def combine(b):
        slots, loads = selectors(b)
        pltpu.make_async_copy(rb.at[b], yr.at[b], yrecv.at[b]).wait()
        scale = jnp.concatenate([jnp.where(s, w, 0.0) for s, w in zip(slots, loads)], axis=0)
        high = scale.astype(BF16)
        low = (scale - high.astype(F32)).astype(BF16)

        @pl.loop(0, yr.shape[-1] // 512)
        def _(i):
            cols = pl.ds(pl.multiple_of(i * 512, 512), 512)
            rows = yr[b, :, :, cols].reshape(SEATS * 8, 512)
            total = jnp.dot(high, rows, preferred_element_type=F32) + jnp.dot(low, rows, preferred_element_type=F32)
            part[b, :, :, cols] = total.astype(BF16).reshape(2, cap, 512)

    def item(wave, end):
        hop, rel, place = end - wave, wave // SPAN, SPAN - 1 - wave % SPAN
        for d in (0, 1):

            @pl.when(off[d] == place)
            def _():
                index = first_block(hop) + rel
                for unit in units:
                    if rel:
                        later = first_block(hop + 1) + rel - (place == SPAN - 1)
                        backward(d, back.at[d, later, pieces[unit]], later, unit).wait_recv()
                        backward(d, back.at[d, later, pieces[unit]], index, unit).start()
                    elif unit == 0 or place < SPAN - 1:
                        b, k = where_part(d, hop, place if d == 0 else SPAN - 1 - place)
                        mine = part.at[b, k, pieces[unit]]
                        if place < SPAN - 1 - unit:
                            later = first_block(hop + 1)
                            far = back.at[d, later, pieces[unit]]
                            backward(d, far, later, unit).wait_recv()
                            mine[...] = (mine[...].astype(F32) + far[...].astype(F32)).astype(BF16)
                        backward(d, mine, index, unit).start()

    acts = dict(r=relay, s=spread, e=expert, c=combine, w=item)

    def send_own():
        for d in (0, 1):
            pack_own(d, "PM"[d])
            first_hop(lambda copy, *_: copy.start(), (d,))

    def trip(pause):
        if cap == NARROW:
            fresh = True
            for name, *where in ORDER:
                if name == "e" and fresh:
                    for w in weights:
                        w.wait()
                    pause()
                    fresh = False
                acts[name](*where)
            return
        for hop in range(1, HOPS + 1):
            relay(hop)
        for w in weights:
            w.wait()
        for act in (spread, expert, combine):

            @pl.loop(0, 6)
            def _(b):
                act(b)

            act(6)
            act(7)
        for hop in range(HOPS, 0, -1):
            for end in range(hop, HOPS + 1):
                if real(end - hop, end):
                    item(end - hop, end)

    def home():
        first_hop(lambda copy, d, rel, unit: backward(d, back.at[d, rel, pieces[unit]], rel, unit).wait_recv())
        group, up_rank, down_rank = r["gc"], r["Pc"], r["Mc"]
        far = jnp.where(zo >= 2, 0, 1)
        far_rank = jnp.where(zo >= 2, up_rank, down_rank)
        plan = [
            ((group == g0) & (r["mxc"] > zo), up_rank, back.at[0, 0]),
            ((group == g0) & (r["mnc"] < zo), down_rank, back.at[1, 0]),
            (group == lax.rem(g0 + 1, GROUPS), up_rank, back.at[0, 1 - last[0]]),
            (group == lax.rem(g0 + GROUPS - 1, GROUPS), down_rank, back.at[1, 1 - last[1]]),
            (group == lax.rem(g0 + 2, GROUPS), far_rank, back.at[far, 2 - jnp.where(zo >= 2, last[0], last[1])]),
            (group == g0, up_rank, part.at[6, 0]),
        ]
        lanes = iota((tokens, len(plan) * cap), 1)
        pick = jnp.zeros(lanes.shape, F32)
        for i, (mask, rank, _) in enumerate(plan):
            pick = pick + jnp.where(jnp.where(mask & (rank >= base) & (rank < base + cap), rank - base + i * cap, -1) == lanes, 1.0, 0.0)
        pick = pick.astype(BF16)

        @pl.loop(0, out_ref.shape[1] // 512)
        def _(i):
            cols = pl.ds(pl.multiple_of(i * 512, 512), 512)
            blocks = jnp.concatenate([ref[:, cols] for _, _, ref in plan], axis=0)
            out_ref[:, cols] = jnp.dot(pick, blocks, preferred_element_type=F32)

    def settle():
        first_hop(lambda copy, *_: copy.wait_send())
        for hop in range(1, HOPS + 1):
            def done(d, rel, unit):
                index = first_block(hop) + rel
                if hop < HOPS:
                    ok, there = goes_on(d, hop, rel, unit)

                    @pl.when(ok)
                    def _():
                        forward(d, came.at[d, index, pieces[unit]], hop + 1, there, unit).wait_send()

                backward(d, back.at[d, index, pieces[unit]], index, unit).wait_send()

            arrivals(hop, done)
        for b in range(BATCHES):
            for k in range(1, SEATS):
                spread_copy(b, k).wait_send()
                return_copy(b, k).wait_send()

    return prepare, send_own, trip, home, settle


def rest_body(normed_hbm, row_hbm, meta_hbm, wg_hbm, wu_hbm, wd_hbm, out_ref, normed_ref, row_ref, meta_ref, isem, *work):
    small = [
        pltpu.make_async_copy(row_hbm, row_ref, isem.at[0]),
        pltpu.make_async_copy(normed_hbm, normed_ref, isem.at[1]),
        pltpu.make_async_copy(meta_hbm, meta_ref, isem.at[2]),
    ]
    for w in small:
        w.start()
    for w in small:
        w.wait()
    row = row_ref[...]
    r = ranks(columns_of(row)[:, 0:2].astype(jnp.int32), row)
    prepare, send_own, trip, home, settle = routing(
        WIDE - NARROW, NARROW, r, normed_ref, meta_ref, wg_hbm, wu_hbm, wd_hbm, out_ref, work
    )
    prepare()
    sp, tp = lax.axis_index("sp"), lax.axis_index("tp")
    zed, core = lax.div(sp, 2), lax.rem(sp, 2)
    teams = lax.axis_size("tp")
    barrier = pltpu.get_barrier_semaphore()
    for step in (1, PLANES - 1):
        to = {"sp": lax.rem(zed + step, PLANES) * 2 + core}
        pl.semaphore_signal(barrier, inc=1, device_id=to, device_id_type=MESH)
    for k in range(1, teams):
        pl.semaphore_signal(barrier, inc=1, device_id={"tp": lax.rem(tp + k, teams)}, device_id_type=MESH)
    for k in range(teams):
        pl.semaphore_signal(barrier, inc=1, device_id={"sp": zed * 2 + 1 - core, "tp": k}, device_id_type=MESH)
    pl.semaphore_wait(barrier, 2 * teams + 1)
    send_own()
    trip(None)
    home()
    settle()


def work_shapes(cap, width, inner):
    seats = pltpu.VMEM((BATCHES, SEATS, 8, width), BF16)
    dma = pltpu.SemaphoreType.DMA
    return [
        pltpu.VMEM((width, inner), BF16),
        pltpu.VMEM((width, inner), BF16),
        pltpu.VMEM((inner, width), BF16),
        pltpu.VMEM((SEATS * 8, inner), BF16),
        pltpu.VMEM((2, GROUPS, cap, width), BF16),
        pltpu.VMEM((2, BLOCKS, cap, width), BF16),
        pltpu.VMEM((2, BLOCKS, cap, width), BF16),
        pltpu.VMEM((BATCHES, 2, cap, width), BF16),
        seats, seats, seats, seats,
        dma((3,)),
        dma((2, BLOCKS, 2)), dma((2, BLOCKS, 2)), dma((2, BLOCKS, 2)), dma((2, BLOCKS, 2)),
        dma((BATCHES, SEATS)), dma((BATCHES,)), dma((BATCHES, SEATS)), dma((BATCHES,)),
    ]


def rest_kernel(normed, ids, meta, w_gate, w_up, w_down):
    rows, width = normed.shape
    return pl.pallas_call(
        rest_body,
        out_shape=jax.ShapeDtypeStruct((rows, width), F32),
        in_specs=[pl.BlockSpec(memory_space=pltpu.HBM)] * 6,
        out_specs=pl.BlockSpec(memory_space=pltpu.VMEM),
        scratch_shapes=[
            pltpu.VMEM((rows, width), BF16),
            pltpu.VMEM(ids.shape, jnp.int32),
            pltpu.VMEM(meta.shape, F32),
            pltpu.SemaphoreType.DMA((3,)),
        ] + work_shapes(WIDE - NARROW, width, w_gate.shape[2]),
        compiler_params=pltpu.CompilerParams(collective_id=1, has_side_effects=True, vmem_limit_bytes=60 << 20),
    )(normed, ids, meta, w_gate, w_up, w_down)


def main_body(
    value_hbm, gate_hbm, taps_hbm, bias_hbm, scale_hbm, shift_hbm, branch_hbm, gain_hbm, row_hbm, load_hbm,
    weight_hbm, residual_hbm, wg_hbm, wu_hbm, wd_hbm,
    hidden_hbm, normed_hbm, meta_hbm, out_ref, crowd_ref,
    hidden_ref, normed_ref, meta_ref, value_ref, gate_ref, taps_ref, vectors, gain_ref, row_ref, load_ref, weight, residual, gated, grown, packs, conv,
    tables, flags, heard,
    lsem, osem, csend, crecv, gsend, grecv, hsend, hrecv, psend, precv, tsend, trecv, *work,
):
    sp, tp = lax.axis_index("sp"), lax.axis_index("tp")
    steps, teams = lax.axis_size("sp"), lax.axis_size("tp")
    zed, core = lax.div(sp, 2), lax.rem(sp, 2)
    rows = hidden_ref.shape[0]
    pieces = rows // UNIT
    channels = value_ref.shape[1]
    parts = lax.axis_size("grp")
    other = zed * 2 + 1 - core
    loads = [
        (row_hbm, row_ref), (load_hbm, load_ref),
        (value_hbm, value_ref), (gate_hbm, gate_ref), (taps_hbm, taps_ref),
        (bias_hbm, vectors.at[0]), (scale_hbm, vectors.at[1]), (shift_hbm, vectors.at[2]), (branch_hbm, vectors.at[3]),
        (residual_hbm, residual), (gain_hbm, gain_ref), (weight_hbm, weight),
    ]
    copies = [pltpu.make_async_copy(a, b, lsem.at[i]) for i, (a, b) in enumerate(loads)]
    for copy in copies:
        copy.start()
    fetch, first, late = copies[:2], copies[2:9], copies[9:]

    def part_of(k):
        return lax.rem(lax.axis_index("grp") + k, parts)

    def team(k):
        return lax.rem(tp + k, teams)

    def column(k):
        return lax.rem(zed + k, PLANES) * 2 + core

    barrier = pltpu.get_barrier_semaphore()
    for k in range(1, teams):
        pl.semaphore_signal(barrier, inc=1, device_id={"tp": team(k)}, device_id_type=MESH)

    @pl.when((sp > 0) & (tp == 0))
    def _():
        for k in range(teams):
            pl.semaphore_signal(barrier, inc=1, device_id={"sp": sp - 1, "tp": k}, device_id_type=MESH)

    for k in range(1, PLANES):
        pl.semaphore_signal(barrier, inc=1, device_id={"sp": column(k)}, device_id_type=MESH)
    for k in range(teams):
        pl.semaphore_signal(barrier, inc=1, device_id={"sp": other, "tp": k}, device_id_type=MESH)
    for k in range(1, parts):
        pl.semaphore_signal(barrier, inc=1, device_id={"grp": part_of(k)}, device_id_type=MESH)

    for copy in first[2:]:
        copy.wait()
    packs[tp, 0 : taps_ref.shape[0]] = taps_ref[...].astype(F32)
    for i in range(4):
        packs[tp, 32 + i : 33 + i] = vectors[i]

    @pl.when((sp == 0) & (tp == 0))
    def _():
        grown[:, 0] = jnp.zeros((teams, UNIT, channels), BF16)

    r = {}
    prepare, send_own, trip, home, settle = routing(
        NARROW, 0, r, normed_ref, meta_ref, wg_hbm, wu_hbm, wd_hbm, out_ref, work
    )
    prepare()
    pl.semaphore_wait(barrier, 2 * teams + PLANES + parts - 3 + jnp.where(sp < steps - 1, 1, 0))

    def whole(to, k):
        return pltpu.make_async_remote_copy(
            src_ref=gated.at[pl.ds(jnp.maximum(to * pieces - 1, 0), pieces + 1)], dst_ref=grown.at[tp],
            send_sem=gsend.at[k], recv_sem=grecv.at[tp], device_id={"tp": to}, device_id_type=MESH,
        )

    def short(to, k):
        return pltpu.make_async_remote_copy(
            src_ref=gated.at[pl.ds(0, pieces)], dst_ref=grown.at[tp, pl.ds(1, pieces)],
            send_sem=gsend.at[k], recv_sem=grecv.at[tp], device_id={"tp": to}, device_id_type=MESH,
        )

    def got(source, first):
        size = pieces if first else pieces + 1
        return pltpu.make_async_remote_copy(
            src_ref=gated.at[pl.ds(0, size)], dst_ref=grown.at[source, pl.ds(1 if first else 0, size)],
            send_sem=gsend.at[0], recv_sem=grecv.at[source], device_id={"tp": source}, device_id_type=MESH,
        )

    def pack_copy(k):
        return pltpu.make_async_remote_copy(
            src_ref=packs.at[tp], dst_ref=packs.at[tp], send_sem=psend.at[k], recv_sem=precv.at[tp],
            device_id={"tp": team(k)}, device_id_type=MESH,
        )

    def halo(source):
        return pltpu.make_async_remote_copy(
            src_ref=gated.at[gated.shape[0] - 1], dst_ref=grown.at[source, 0],
            send_sem=hsend.at[0], recv_sem=hrecv.at[source],
            device_id={"sp": lax.rem(sp + 1, steps), "tp": 0}, device_id_type=MESH,
        )

    def table_copy(k):
        return pltpu.make_async_remote_copy(
            src_ref=tables.at[lax.rem(zed + k, PLANES)], dst_ref=meta_ref.at[zed], send_sem=tsend.at[k],
            recv_sem=trecv.at[k], device_id={"sp": column(k)}, device_id_type=MESH,
        )

    for k in (2, 1, 3):
        pack_copy(k).start()
    for copy in first[:2]:
        copy.wait()
    passed = (value_ref[...].astype(F32) * jax.nn.sigmoid(gate_ref[...].astype(F32))).astype(BF16)
    gated[...] = passed.reshape(gated.shape)
    for k in (2, 1, 3):
        for test, copy in ((team(k) == 0, short), (team(k) > 0, whole)):

            @pl.when(test)
            def _():
                copy(team(k), k).start()

    @pl.when(sp < steps - 1)
    def _():
        halo(tp).start()

    mates = [{"tp": team(k)} for k in range(1, teams)] + [{"sp": other, "tp": k} for k in range(teams)]
    peers = [{"grp": part_of(k)} for k in range(1, parts)]

    def flag_copies(stage):
        out = []
        for i, to in enumerate(peers if stage else mates):
            at = i + SEATS * stage
            land = teams - 1 + tp if not stage and i >= teams - 1 else at
            out.append(pltpu.make_async_remote_copy(
                src_ref=flags.at[stage], dst_ref=heard.at[land], send_sem=csend.at[at],
                recv_sem=crecv.at[land], device_id=to, device_id_type=MESH,
            ))
        return out

    def hear(stage):
        seen = flags[stage]
        for i, to in enumerate(peers if stage else mates):
            at = i + SEATS * stage
            pltpu.make_async_remote_copy(
                src_ref=flags.at[stage], dst_ref=heard.at[at], send_sem=csend.at[at],
                recv_sem=crecv.at[at], device_id=to, device_id_type=MESH,
            ).wait_recv()
            seen = jnp.maximum(seen, heard[at])
        flags[stage + 1] = seen

    for test, size in ((tp == 0, 0), (tp > 0, 1)):

        @pl.when(test)
        def _():
            low = jnp.maximum(tp * pieces - 1, 0) if size else 0
            grown[tp, 1 - size : pieces + 1] = gated[pl.ds(low, pieces + size)]

    for copy in fetch:
        copy.wait()
    row = row_ref[...]
    cols = columns_of(row, load_ref[...])
    r.update(ranks(cols[:, 0:2].astype(jnp.int32), row))
    route_tables(r, row, cols, tables, zed)
    meta_ref[zed] = tables[zed]
    for k in range(1, PLANES):
        table_copy(k).start()

    def wait_part(k):
        source = team(k)
        if k:
            for test, first in ((tp == 0, True), (tp > 0, False)):

                @pl.when(test)
                def _():
                    got(source, first).wait_recv()

            pltpu.make_async_remote_copy(
                src_ref=packs.at[tp], dst_ref=packs.at[source], send_sem=psend.at[k], recv_sem=precv.at[source],
                device_id={"tp": source}, device_id_type=MESH,
            ).wait_recv()

        @pl.when((tp == 0) & (sp > 0))
        def _():
            halo(source).wait_recv()

    reach = taps_ref.shape[0] - 1
    shift0 = UNIT - reach
    for k in (0, 1, 3, 2):
        wait_part(k)
        source = team(k)
        for half in range(channels // 128):
            lanes = pl.ds(half * 128, 128)
            x = grown[source, :, :, lanes].reshape((pieces + 1) * UNIT, 128).astype(F32)
            total = jnp.broadcast_to(packs[source, 32:33, lanes], (rows, 128))
            for r in range(8):
                span = rows if r == 0 else rows + 8
                acc = None
                for q in range(0, (UNIT - r) // 8 + 1):
                    tap = 8 * q + r - shift0
                    if not 0 <= tap <= reach:
                        continue
                    term = x[8 * q : 8 * q + span] * packs[source, tap : tap + 1, lanes]
                    acc = term if acc is None else acc + term
                total = total + (acc if r == 0 else acc[r : r + rows])
            conv[source, :, lanes] = total

    full = channels * teams
    pieces_of = [conv[s] for s in range(teams)]
    average = sum(jnp.sum(p, axis=1, keepdims=True) for p in pieces_of) / full
    spread = sum(jnp.sum(p * p, axis=1, keepdims=True) for p in pieces_of) / full - average * average
    scale = lax.rsqrt(spread + EPSILON)
    energy = jnp.zeros((rows, 1), F32)
    for s in range(teams):
        v = jax.nn.silu((conv[s] - average) * scale * packs[s, 33:34] + packs[s, 34:35])
        conv[s] = v
        energy = energy + jnp.sum(v * v, axis=1, keepdims=True)
    scale = lax.rsqrt(energy / full + EPSILON)
    branch = jnp.concatenate([(conv[s] * scale * packs[s, 35:36]).astype(BF16) for s in range(teams)], axis=1)
    for copy in late:
        copy.wait()
    projected = jnp.dot(branch, weight[...], preferred_element_type=F32)
    hidden = (residual[...].astype(F32) + projected).astype(BF16)
    hidden_ref[...] = hidden
    wide = hidden.astype(F32)
    scale = lax.rsqrt(jnp.mean(wide * wide, axis=1, keepdims=True) + EPSILON)
    normed_ref[...] = (wide * scale * gain_ref[...]).astype(BF16)

    send_own()
    results = [
        pltpu.make_async_copy(hidden_ref, hidden_hbm, osem.at[0]),
        pltpu.make_async_copy(normed_ref, normed_hbm, osem.at[1]),
        pltpu.make_async_copy(meta_ref, meta_hbm, osem.at[2]),
    ]
    for k in range(1, PLANES):
        table_copy(k).wait_recv()
    for copy in results:
        copy.start()
    crowd = meta_ref[0]
    for z in range(1, PLANES):
        crowd = jnp.maximum(crowd, meta_ref[z])
    flags[0] = jnp.broadcast_to(crowd[2:3], crowd.shape)
    for copy in flag_copies(0):
        copy.start()

    def pause():
        hear(0)
        for copy in flag_copies(1):
            copy.start()

    trip(pause)
    hear(1)
    crowd_ref[0] = jnp.max(flags[2]).astype(jnp.int32)
    home()
    settle()
    for copy in results:
        copy.wait()
    for stage in (0, 1):
        for copy in flag_copies(stage):
            copy.wait_send()

    for k in range(1, teams):
        pack_copy(k).wait_send()
        for test, copy in ((team(k) == 0, short), (team(k) > 0, whole)):

            @pl.when(test)
            def _():
                copy(team(k), k).wait_send()

    @pl.when(sp < steps - 1)
    def _():
        halo(tp).wait_send()

    for k in range(1, PLANES):
        table_copy(k).wait_send()


def main_kernel(value, gate, taps, vectors, moe_gain, ids, loads, out_weight, residual, w_gate, w_up, w_down):
    rows, width = residual.shape
    tok_rows, channels = value.shape
    teams = lax.axis_size("tp")
    far = pl.BlockSpec(memory_space=pltpu.HBM)
    dma = pltpu.SemaphoreType.DMA
    voices = SEATS + lax.axis_size("grp")
    return pl.pallas_call(
        main_body,
        out_shape=(
            jax.ShapeDtypeStruct((rows, width), BF16),
            jax.ShapeDtypeStruct((rows, width), BF16),
            jax.ShapeDtypeStruct((PLANES, 8, 128), F32),
            jax.ShapeDtypeStruct((rows, width), F32),
            jax.ShapeDtypeStruct((1,), jnp.int32),
        ),
        in_specs=[far] * 15,
        out_specs=[far] * 3 + [pl.BlockSpec(memory_space=pltpu.VMEM), pl.BlockSpec(memory_space=pltpu.SMEM)],
        scratch_shapes=[
            pltpu.VMEM((rows, width), BF16),
            pltpu.VMEM((rows, width), BF16),
            pltpu.VMEM((PLANES, 8, 128), F32),
            pltpu.VMEM(value.shape, BF16),
            pltpu.VMEM(value.shape, BF16),
            pltpu.VMEM(taps.shape, BF16),
            pltpu.VMEM((4, 1, channels), F32),
            pltpu.VMEM(moe_gain.shape, F32),
            pltpu.VMEM(ids.shape, jnp.int32),
            pltpu.VMEM(loads.shape, F32),
            pltpu.VMEM(out_weight.shape, BF16),
            pltpu.VMEM((rows, width), BF16),
            pltpu.VMEM((tok_rows // UNIT, UNIT, channels), BF16),
            pltpu.VMEM((teams, rows // UNIT + 1, UNIT, channels), BF16),
            pltpu.VMEM((teams, 40, channels), F32),
            pltpu.VMEM((teams, rows, channels), F32),
            pltpu.VMEM((PLANES, 8, 128), F32),
            pltpu.VMEM((3, 8, 128), F32),
            pltpu.VMEM((voices, 8, 128), F32),
            dma((12,)), dma((3,)), dma((voices,)), dma((voices,)),
            dma((teams,)), dma((teams,)), dma((1,)), dma((teams,)), dma((teams,)), dma((teams,)),
            dma((PLANES,)), dma((PLANES,)),
        ] + work_shapes(NARROW, width, w_gate.shape[2]),
        compiler_params=pltpu.CompilerParams(
            collective_id=2, has_side_effects=True, vmem_limit_bytes=60 << 20
        ),
    )(value, gate, taps, *vectors, moe_gain, ids, loads, out_weight, residual, w_gate, w_up, w_down)


def per_device(
    conv_value,
    conv_gate,
    kernel,
    conv_bias,
    ln_gain,
    ln_bias,
    out_gain,
    out_weight,
    residual,
    moe_gain,
    expert_ids,
    expert_weights,
    w_gate,
    w_up,
    w_down,
):
    ids = expert_ids.T
    vectors = [v[None] for v in (conv_bias, ln_gain, ln_bias, out_gain)]
    hidden, normed, meta, added, crowd = main_kernel(
        conv_value, conv_gate, kernel, vectors, moe_gain[None], ids, expert_weights.T, out_weight, residual,
        w_gate, w_up, w_down,
    )
    return lax.cond(
        crowd[0] > 0,
        lambda hidden, added, *rest: (hidden.astype(F32) + added + rest_kernel(*rest)).astype(BF16),
        lambda hidden, added, *_: (hidden.astype(F32) + added).astype(BF16),
        hidden, added, normed, ids, meta, w_gate, w_up, w_down,
    )


def solution(mesh):
    assert mesh.shape["sp"] == 2 * PLANES and 2 * mesh.shape["tp"] == SEATS
    in_specs = (
        P(("grp", "sp"), "tp"),
        P(("grp", "sp"), "tp"),
        P(None, "tp"),
        P("tp"),
        P("tp"),
        P("tp"),
        P("tp"),
        P(),
        P(("grp", "sp", "tp"), None),
        P(),
        P(("grp", "sp", "tp"), None),
        P(("grp", "sp", "tp"), None),
        P(("sp", "tp"), None, None),
        P(("sp", "tp"), None, None),
        P(("sp", "tp"), None, None),
    )
    out_specs = P(("grp", "sp", "tp"), None)
    return jax.shard_map(
        per_device, mesh=mesh, in_specs=in_specs, out_specs=out_specs, check_vma=False
    )
```
